32 devices in a mesh: sp: 4 (over z), fs: 4 (over y, x), tp: 2 (over core).
Axes of the slice: x: 2, y: 2, z: 4, core: 2. Of those that a mesh axis runs over, the one named last changes fastest.
Arguments:
- tokens: bfloat16 [8192, 2048], P(('fs', 'sp')), parts along dimension 0, may hold values from -6 to 6
- norm_gain: float32 [2048], replicated, may hold values from 0.1 to 1.9
- state_gate: bfloat16 [2048, 1024], P('sp', 'tp'), may hold values from -0.125 to 0.125
- state_value: bfloat16 [2048, 1024], P('sp', 'tp'), may hold values from -0.125 to 0.125
- state_keys: bfloat16 [2048, 1024], P('sp', 'tp'), may hold values from -0.125 to 0.125
- state_query: bfloat16 [2048, 1024], P('sp', 'tp'), may hold values from -0.125 to 0.125
- state_step: bfloat16 [2048, 16], replicated, may hold values from -0.125 to 0.125
- state_rate: float32 [16], P('tp'), may hold values from 0 to 1, as said below
- state_jumps: float32 [8192, 16], P(('fs', 'sp'), 'tp'), parts along dimension 0, may hold values from -3 to 0
- state_gain: float32 [1024], P('tp'), may hold values from 0.1 to 1.9
- filter_value: bfloat16 [5, 1024], P(None, 'tp'), may hold values from -2.5 to 2.5
- filter_keys: bfloat16 [5, 1024], P(None, 'tp'), may hold values from -2.5 to 2.5
- filter_query: bfloat16 [5, 1024], P(None, 'tp'), may hold values from -2.5 to 2.5
- window_query: bfloat16 [2048, 2048], P('sp', 'tp'), may hold values from -64 to 64
- window_keys: bfloat16 [2048, 1024], P('sp', 'tp'), may hold values from -1 to 1
- window_values: bfloat16 [2048, 1024], P('sp', 'tp'), may hold values from -0.125 to 0.125
- window_sink: float32 [16], P('tp'), may hold values from 2.5 to 5.5
- state_output: bfloat16 [1024, 2048], P('tp', 'sp'), may hold values from -0.1875 to 0.1875
- window_output: bfloat16 [2048, 2048], P('tp', 'sp'), may hold values from -2 to 2
Outputs:
- mixed: bfloat16 [8192, 2048], P(('fs', 'sp', 'tp')), parts along dimension 0
The draws below stay inside these ranges and needn't reach their ends.
There are 4 independent parts, one for each index of `fs`. The reference program is written for one: setup_inputs(seed, part) draws one part's arguments, and reference() takes and returns one part's arrays. A program takes and returns all parts, laid end to end along the dimension named above; an argument that names none is the same for every part. Nothing has to cross between parts.
Inputs may be any that keep to these rules, and one draw needn't show every extreme that they name: `state_rate`: a positive rate for each head.
All inputs are finite; a program needn't handle non-finite values.
Results may differ from the reference program's by a relative error of at most 0.015.
The reference program's roundings to bfloat16 on the way count: a program that leaves them out, or rounds other values in their place, can miss the bound.
Values may be sent and summed in bfloat16 or wider, within the bound.
A program may use at most 64 MiB of HBM per device.

```python
import math
import jax
import jax.numpy as jnp
from jax import lax

D = 2048
MIXER_STATE_HEADS = 16
STATE_HEAD_DIM = 64
STATE_GROUPS = 8
STATE_SIZE = 128
WINDOW_HEADS = 16
WINDOW_KV_HEADS = 8
HEAD_DIM = 128
CONV_WIDTH = 5
WINDOW = 128
BLOCK = 128
GRID_WIDTH = 64
TOK_DEV = 512
SEQUENCE_LENGTH = 2048
STATE_INNER = 1024
GROUP_WIDTH = 1024
WINDOW_WIDTH = 2048
KV_WIDTH = 1024
N_TP = 2


def draw_state_rate(key, part):
    shuffled = jax.random.permutation(jax.random.fold_in(key, 101), MIXER_STATE_HEADS)
    quick_count = MIXER_STATE_HEADS // 2
    quick_heads = shuffled < quick_count
    quick_rate = jnp.exp(jax.random.uniform(jax.random.fold_in(key, 102), (MIXER_STATE_HEADS,), jnp.float32, math.log(1.0 / 60.0), math.log(1.0 / 20.0)))
    slow_rate = jax.random.uniform(jax.random.fold_in(key, 103), (MIXER_STATE_HEADS,), jnp.float32, 0.1, 0.4) / SEQUENCE_LENGTH
    return jnp.where(quick_heads, quick_rate, slow_rate).astype(jnp.float32)


def draw_state_jumps(key, part):
    block_count = SEQUENCE_LENGTH // TOK_DEV
    factors = jnp.exp(jax.random.uniform(jax.random.fold_in(key, 201), (block_count,), jnp.float32, math.log(0.5), math.log(2.5)))
    token_position = jnp.arange(SEQUENCE_LENGTH)
    baseline_level = -0.3 * jnp.take(factors, token_position // TOK_DEV) / SEQUENCE_LENGTH
    spike_positions = jax.random.randint(jax.random.fold_in(key, 202), (3,), 0, SEQUENCE_LENGTH)
    spike_count = (token_position[None, :] == spike_positions[:, None]).astype(jnp.float32)
    spike_depth = jnp.log(jax.random.uniform(jax.random.fold_in(key, 203), (3, MIXER_STATE_HEADS), jnp.float32, 0.5, 0.8))
    return (baseline_level[:, None] + jnp.dot(spike_count.T, spike_depth)).astype(jnp.float32)


def draw_tokens(key, part):
    rows = jnp.clip(jax.random.normal(jax.random.fold_in(key, 404), (SEQUENCE_LENGTH, D), jnp.float32), -6.0, 6.0)
    return rows.astype(jnp.bfloat16)


def window_pair(key):
    scale = 1.0 / math.sqrt(D)
    keys_all = jnp.clip(jax.random.normal(jax.random.fold_in(key, 306), (D, KV_WIDTH), jnp.float32), -6.0, 6.0) * scale
    query_all = jnp.clip(jax.random.normal(jax.random.fold_in(key, 307), (D, WINDOW_WIDTH), jnp.float32), -6.0, 6.0) * scale
    return (query_all.astype(jnp.float32), keys_all.astype(jnp.float32))


def draw_window_query(key, part):
    return window_pair(key)[0].astype(jnp.bfloat16)


def draw_window_keys(key, part):
    return window_pair(key)[1].astype(jnp.bfloat16)


def levels(rng, shape, split, smallest, top_value):
    def one(dim, parts):
        heights = jax.random.uniform(jax.random.fold_in(jax.random.fold_in(rng, 6), dim), (parts,), jnp.float32, smallest / len(split), top_value / len(split))
        return jnp.repeat(jnp.exp(heights), shape[dim] // parts).reshape((-1,) + (1,) * (len(shape) - dim - 1))

    factor_of = one(*split[0])
    for cut in split[1:]:
        factor_of = factor_of * one(*cut)
    return factor_of


def centred(rng, shape, scale, reach, cuts=(), kind=jnp.bfloat16):
    result = scale * jax.random.normal(rng, shape, jnp.float32)
    if cuts:
        result = result * levels(rng, shape, cuts, -0.22, 0.18)
    return jnp.clip(result, -reach, reach).astype(kind)


def setup_inputs(seed: int = 0, part: int = 0) -> dict:
    key_list = jax.random.split(jax.random.key(seed), 20)
    part_splits = jax.random.split(jax.random.fold_in(key_list[19], part), 20)
    return {
        "tokens": draw_tokens(jax.random.fold_in(jax.random.fold_in(key_list[19], part), 71), part),
        "norm_gain": jnp.clip(1.0 + 0.18 * jax.random.normal(key_list[1], (D,), jnp.float32), 0.1, 1.9),
        "state_gate": centred(key_list[2], (D, STATE_INNER), D ** -0.5, 0.125, ((0, 4), (1, 2))),
        "state_value": centred(key_list[3], (D, STATE_INNER), D ** -0.5, 0.125, ((0, 4), (1, 2))),
        "state_keys": centred(key_list[4], (D, GROUP_WIDTH), D ** -0.5, 0.125, ((0, 4), (1, 2))),
        "state_query": centred(key_list[5], (D, GROUP_WIDTH), D ** -0.5, 0.125, ((0, 4), (1, 2))),
        "state_step": centred(key_list[6], (D, MIXER_STATE_HEADS), D ** -0.5, 0.125),
        "state_rate": draw_state_rate(jax.random.fold_in(key_list[19], 71), part),
        "state_jumps": draw_state_jumps(jax.random.fold_in(jax.random.fold_in(key_list[19], part), 71), part),
        "state_gain": jnp.clip(1.0 + 0.18 * jax.random.normal(key_list[9], (STATE_INNER,), jnp.float32), 0.1, 1.9),
        "filter_value": centred(key_list[10], (CONV_WIDTH, STATE_INNER), CONV_WIDTH ** -0.5, 2.5, ((1, 2),)),
        "filter_keys": centred(key_list[11], (CONV_WIDTH, GROUP_WIDTH), CONV_WIDTH ** -0.5, 2.5, ((1, 2),)),
        "filter_query": centred(key_list[12], (CONV_WIDTH, GROUP_WIDTH), CONV_WIDTH ** -0.5, 2.5, ((1, 2),)),
        "window_query": draw_window_query(jax.random.fold_in(key_list[19], 71), part),
        "window_keys": draw_window_keys(jax.random.fold_in(key_list[19], 71), part),
        "window_values": centred(key_list[15], (D, KV_WIDTH), D ** -0.5, 0.125, ((0, 4), (1, 2))),
        "window_sink": jnp.clip(2.5 + 3.0 * jax.random.uniform(key_list[16], (WINDOW_HEADS,), jnp.float32) ** levels(key_list[16], (WINDOW_HEADS,), ((0, 2),), -0.2, 0.2), 2.5, 5.5),
        "state_output": centred(key_list[17], (STATE_INNER, D), STATE_INNER ** -0.5, 0.1875, ((0, 2), (1, 4))),
        "window_output": centred(key_list[18], (WINDOW_WIDTH, D), (WINDOW_WIDTH // (2 * WINDOW + 1)) ** -0.5, 2.0, ((0, 2), (1, 4))),
    }


def rotate_grid(vectors, positions, grid_width):
    head_dim = vectors.shape[-1]
    quarter = head_dim // 4
    half_dim = head_dim // 2
    inverse = 10000.0 ** (-jnp.arange(quarter, dtype=jnp.float32) / quarter)
    grid_row = (positions // grid_width).astype(jnp.float32)
    grid_col = (positions % grid_width).astype(jnp.float32)
    angle_row = grid_row[:, None] * inverse[None, :]
    angle_col = grid_col[:, None] * inverse[None, :]
    angles = jnp.concatenate([angle_row, angle_row, angle_col, angle_col], axis=-1)[:, None, :]
    first_half = vectors[..., :half_dim]
    second = vectors[..., half_dim:]
    turned = jnp.concatenate([-first_half[..., quarter:], first_half[..., :quarter], -second[..., quarter:], second[..., :quarter]], axis=-1)
    return (vectors.astype(jnp.float32) * jnp.cos(angles) + turned.astype(jnp.float32) * jnp.sin(angles)).astype(jnp.bfloat16)

def window_attend(query_rows, keys_pad, values_pad, sink_logits, key_start, total_len, window):
    row_count, query_heads, head_dim = query_rows.shape
    kv_heads = keys_pad.shape[1]
    group_size = query_heads // kv_heads
    block_count = row_count // window
    query_blocks = query_rows.reshape(block_count, window, kv_heads, group_size, head_dim)
    key_split = keys_pad.reshape(block_count + 2, window, kv_heads, head_dim)
    value_split = values_pad.reshape(block_count + 2, window, kv_heads, head_dim)
    key_band = jnp.concatenate([key_split[:-2], key_split[1:-1], key_split[2:]], axis=1)
    value_band = jnp.concatenate([value_split[:-2], value_split[1:-1], value_split[2:]], axis=1)
    scores = jnp.einsum('kihgd,kjhd->khgij', query_blocks.astype(jnp.float32), key_band.astype(jnp.float32)) * head_dim ** (-0.5)
    query_pos = jnp.arange(window)[:, None]
    band_pos = jnp.arange(3 * window)[None, :]
    within = jnp.abs(band_pos - window - query_pos) <= window
    key_pos = key_start + jnp.arange(block_count)[:, None] * window + jnp.arange(3 * window)[None, :]
    inside = (key_pos >= 0) & (key_pos < total_len)
    valid_pair = (within[None] & inside[:, None, :])[:, None, None]
    sink_logit = sink_logits.reshape(kv_heads, group_size)[None, :, :, None, None]
    masked = jnp.where(valid_pair, scores, -1e+30)
    ceiling = jnp.maximum(lax.optimization_barrier(jnp.max(masked, axis=-1, keepdims=True)), sink_logit)
    weights = jnp.where(valid_pair, jnp.exp(masked - ceiling), 0.0)
    denominator = jnp.exp(sink_logit - ceiling) + lax.optimization_barrier(jnp.sum(weights, axis=-1, keepdims=True))
    weights_bf = (weights / denominator).astype(jnp.bfloat16)
    mixed_rows = jnp.einsum('khgij,kjhd->kihgd', weights_bf.astype(jnp.float32), value_band.astype(jnp.float32))
    return mixed_rows.reshape(row_count, query_heads * head_dim).astype(jnp.bfloat16)

def block_terms(query_rows, key_rows, value_rows, log_rows, block_len):
    row_count, group_count, state_size = query_rows.shape
    head_ratio, head_dim = (value_rows.shape[2], value_rows.shape[3])
    block_count = row_count // block_len
    query_blocks = query_rows.reshape(block_count, block_len, group_count, state_size)
    key_blocks = key_rows.reshape(block_count, block_len, group_count, state_size)
    value_blocks = value_rows.reshape(block_count, block_len, group_count, head_ratio, head_dim)
    decay_cum = jnp.cumsum(log_rows.reshape(block_count, block_len, group_count, head_ratio), axis=1)
    decay_total = decay_cum[:, -1]
    gram_block = jnp.einsum('kign,kjgn->kgij', query_blocks.astype(jnp.float32), key_blocks.astype(jnp.float32))
    cum_heads = jnp.moveaxis(decay_cum, 1, 3)
    distance = jnp.abs(cum_heads[..., :, None] - cum_heads[..., None, :])
    pair_weight = (gram_block[:, :, None] * jnp.exp(-distance)).astype(jnp.bfloat16)
    near_terms = jnp.einsum('kgrij,kjgrp->kigrp', pair_weight.astype(jnp.float32), value_blocks.astype(jnp.float32))
    keys_after = (key_blocks[:, :, :, None, :] * jnp.exp(decay_total[:, None] - decay_cum)[..., None]).astype(jnp.bfloat16)
    keys_before = (key_blocks[:, :, :, None, :] * jnp.exp(decay_cum)[..., None]).astype(jnp.bfloat16)
    state_after = jnp.einsum('kjgrn,kjgrp->kgrnp', keys_after.astype(jnp.float32), value_blocks.astype(jnp.float32))
    state_before = jnp.einsum('kjgrn,kjgrp->kgrnp', keys_before.astype(jnp.float32), value_blocks.astype(jnp.float32))
    before = jnp.cumsum(decay_total, axis=0) - decay_total
    overall = lax.optimization_barrier(jnp.sum(decay_total, axis=0))
    after_sum = overall[None] - before - decay_total
    block_order = jnp.arange(block_count)
    earlier_mask = (block_order[None, :] < block_order[:, None])[:, :, None, None]
    later_mask = (block_order[None, :] > block_order[:, None])[:, :, None, None]
    gap_fwd = before[:, None] - before[None, :] - decay_total[None, :]
    gap_bwd = before[None, :] - before[:, None] - decay_total[:, None]
    weight_fwd = jnp.where(earlier_mask, jnp.exp(jnp.minimum(gap_fwd, 0.0)), 0.0)
    weight_bwd = jnp.where(later_mask, jnp.exp(jnp.minimum(gap_bwd, 0.0)), 0.0)
    carried_fwd = jnp.einsum('abgr,bgrnp->agrnp', weight_fwd, state_after, precision=lax.Precision.HIGHEST)
    carried_bwd = jnp.einsum('abgr,bgrnp->agrnp', weight_bwd, state_before, precision=lax.Precision.HIGHEST)
    summary_fwd = jnp.einsum('agr,agrnp->grnp', jnp.exp(after_sum), state_after, precision=lax.Precision.HIGHEST)
    summary_bwd = jnp.einsum('agr,agrnp->grnp', jnp.exp(before), state_before, precision=lax.Precision.HIGHEST)
    pieces = (near_terms, carried_fwd, carried_bwd, decay_cum, decay_total, before, after_sum, query_blocks)
    return (pieces, (summary_fwd, summary_bwd, overall))

def finish_terms(pieces, incoming_fwd, incoming_bwd):
    near_terms, carried_fwd, carried_bwd, decay_cum, decay_total, before, after_sum, query_blocks = pieces
    total_fwd = carried_fwd + jnp.exp(before)[..., None, None] * incoming_fwd[None]
    total_bwd = carried_bwd + jnp.exp(after_sum)[..., None, None] * incoming_bwd[None]
    query_wide = query_blocks.astype(jnp.float32)
    read_fwd = jnp.einsum('kign,kgrnp->kigrp', query_wide, total_fwd, precision=lax.Precision.HIGHEST)
    read_bwd = jnp.einsum('kign,kgrnp->kigrp', query_wide, total_bwd, precision=lax.Precision.HIGHEST)
    combined = near_terms + jnp.exp(decay_cum)[..., None] * read_fwd + jnp.exp(decay_total[:, None] - decay_cum)[..., None] * read_bwd
    block_count, block_len, group_count, head_ratio, head_dim = combined.shape
    return combined.reshape(block_count * block_len, group_count, head_ratio, head_dim)

def reference(tokens, norm_gain, state_gate, state_value, state_keys, state_query, state_step, state_rate, state_jumps, state_gain, filter_value, filter_keys, filter_query, window_query, window_keys, window_values, window_sink, state_output, window_output):
    length, feat_width = tokens.shape
    rows_wide = tokens.astype(jnp.float32)
    normed = (rows_wide * lax.rsqrt(lax.optimization_barrier(jnp.mean(rows_wide * rows_wide, axis=-1, keepdims=True)) + 1e-06) * norm_gain).astype(jnp.bfloat16)
    gate_rows = jnp.dot(normed, state_gate, preferred_element_type=jnp.float32).astype(jnp.bfloat16)
    value_pre = jnp.dot(normed, state_value, preferred_element_type=jnp.float32).astype(jnp.bfloat16)
    keys_pre = jnp.dot(normed, state_keys, preferred_element_type=jnp.float32).astype(jnp.bfloat16)
    query_pre = jnp.dot(normed, state_query, preferred_element_type=jnp.float32).astype(jnp.bfloat16)
    query_raw = jnp.dot(normed, window_query, preferred_element_type=jnp.float32).astype(jnp.bfloat16)
    keys_raw = jnp.dot(normed, window_keys, preferred_element_type=jnp.float32).astype(jnp.bfloat16)
    values_rows = jnp.dot(normed, window_values, preferred_element_type=jnp.float32).astype(jnp.bfloat16)
    step_rows = jax.nn.softplus(jnp.dot(normed, state_step, preferred_element_type=jnp.float32))
    log_decay = -state_rate[None, :] * step_rows + state_jumps
    half_width = filter_value.shape[0] // 2
    stacked = jnp.concatenate([value_pre, keys_pre, query_pre], axis=-1)
    padded = jnp.pad(stacked, ((half_width, half_width), (0, 0)))
    filters = jnp.concatenate([filter_value, filter_keys, filter_query], axis=-1).astype(jnp.float32)
    filtered = jnp.zeros(stacked.shape, jnp.float32)
    for offset in range(filters.shape[0]):
        filtered = filtered + padded[offset:offset + length].astype(jnp.float32) * filters[offset]
    value_cols = STATE_INNER
    key_cols = GROUP_WIDTH
    head_ratio = MIXER_STATE_HEADS // STATE_GROUPS
    inner_rows = jax.nn.silu(filtered[:, :value_cols]).reshape(length, MIXER_STATE_HEADS, STATE_HEAD_DIM) * step_rows[..., None]
    scan_values = inner_rows.astype(jnp.bfloat16).reshape(length, STATE_GROUPS, head_ratio, STATE_HEAD_DIM)
    scan_keys = filtered[:, value_cols:value_cols + key_cols].astype(jnp.bfloat16).reshape(length, STATE_GROUPS, STATE_SIZE)
    scan_query = filtered[:, value_cols + key_cols:].astype(jnp.bfloat16).reshape(length, STATE_GROUPS, STATE_SIZE)
    group_logs = log_decay.reshape(length, STATE_GROUPS, head_ratio)

    def one_group(group_args):
        group_query, group_keys, group_values, group_decay = group_args
        pieces, summaries = block_terms(group_query[:, None], group_keys[:, None], group_values[:, None], group_decay[:, None], BLOCK)
        zero_state = jnp.zeros((1, head_ratio, STATE_SIZE, STATE_HEAD_DIM), jnp.float32)
        return finish_terms(pieces, zero_state, zero_state)[:, 0]
    per_group = lax.map(one_group, (jnp.moveaxis(scan_query, 1, 0), jnp.moveaxis(scan_keys, 1, 0), jnp.moveaxis(scan_values, 1, 0), jnp.moveaxis(group_logs, 1, 0)))
    scan_out = jnp.moveaxis(per_group, 0, 1).reshape(length, STATE_INNER)
    gated_rows = scan_out * jax.nn.silu(gate_rows.astype(jnp.float32))
    per_head = gated_rows.reshape(length, MIXER_STATE_HEADS, STATE_HEAD_DIM)
    state_mix = (per_head * lax.rsqrt(lax.optimization_barrier(jnp.mean(per_head * per_head, axis=-1, keepdims=True)) + 1e-06) * state_gain.reshape(MIXER_STATE_HEADS, STATE_HEAD_DIM)).astype(jnp.bfloat16).reshape(length, STATE_INNER)
    positions = jnp.arange(length, dtype=jnp.int32)
    query_rot = rotate_grid(query_raw.reshape(length, WINDOW_HEADS, HEAD_DIM), positions, GRID_WIDTH)
    keys_rot = rotate_grid(keys_raw.reshape(length, WINDOW_KV_HEADS, HEAD_DIM), positions, GRID_WIDTH)
    keys_pad = jnp.pad(keys_rot, ((WINDOW, WINDOW), (0, 0), (0, 0)))
    values_pad = jnp.pad(values_rows.reshape(length, WINDOW_KV_HEADS, HEAD_DIM), ((WINDOW, WINDOW), (0, 0), (0, 0)))
    group_size = WINDOW_HEADS // WINDOW_KV_HEADS

    def one_head(head_args):
        head_query, head_keys, head_values, head_sink = head_args
        return window_attend(head_query, head_keys[:, None], head_values[:, None], head_sink, -WINDOW, length, WINDOW)
    per_kv = lax.map(one_head, (jnp.moveaxis(query_rot.reshape(length, WINDOW_KV_HEADS, group_size, HEAD_DIM), 1, 0), jnp.moveaxis(keys_pad, 1, 0), jnp.moveaxis(values_pad, 1, 0), window_sink.reshape(WINDOW_KV_HEADS, group_size)))
    window_mix = jnp.moveaxis(per_kv, 0, 1).reshape(length, WINDOW_WIDTH)
    state_cols = STATE_INNER // N_TP
    window_cols = WINDOW_WIDTH // N_TP

    def add_group(group_index, running):
        state_start = (group_index * state_cols).astype(jnp.int32)
        window_start = (group_index * window_cols).astype(jnp.int32)
        state_part = lax.dynamic_slice_in_dim(state_mix, state_start, state_cols, 1)
        state_weight = lax.dynamic_slice_in_dim(state_output, state_start, state_cols, 0)
        window_part = lax.dynamic_slice_in_dim(window_mix, window_start, window_cols, 1)
        window_weight = lax.dynamic_slice_in_dim(window_output, window_start, window_cols, 0)
        term_rows = jnp.dot(state_part, state_weight, preferred_element_type=jnp.float32) + jnp.dot(window_part, window_weight, preferred_element_type=jnp.float32)
        rounded = lax.optimization_barrier(term_rows.astype(jnp.bfloat16))
        return running + rounded.astype(jnp.float32)
    summed = lax.fori_loop(0, N_TP, add_group, jnp.zeros((length, feat_width), jnp.float32))
    return summed.astype(jnp.bfloat16)
```

```python
import functools
import math

import jax
import jax.numpy as jnp
from jax import lax
from jax.experimental import pallas as pl
from jax.experimental.pallas import tpu as pltpu
from jax.sharding import PartitionSpec as P

STATE_SIZE = 128
HEAD_DIM = 128
WINDOW = 128
BLOCK = 128
GRID_WIDTH = 64


def extended(cells, sides, width):
    for axis, dim in sides:
        count = lax.axis_size(axis)
        ends = count - 1
        head = lax.slice_in_dim(cells, 0, width, axis=dim)
        tail = lax.slice_in_dim(cells, cells.shape[dim] - width, cells.shape[dim], axis=dim)
        cells = jnp.concatenate(
            [
                lax.ppermute(tail, axis, [(i, (i + 1) % count) for i in range(ends)]),
                cells,
                lax.ppermute(head, axis, [((i + 1) % count, i) for i in range(ends)]),
            ],
            axis=dim,
        )
    return cells


def rotate_grid(vectors, positions, grid_width):
    head_dim = vectors.shape[-1]
    quarter = head_dim // 4
    half_dim = head_dim // 2
    inverse = 10000.0 ** (-jnp.arange(quarter, dtype=jnp.float32) / quarter)
    grid_row = (positions // grid_width).astype(jnp.float32)
    grid_col = (positions % grid_width).astype(jnp.float32)
    angle_row = grid_row[:, None] * inverse[None, :]
    angle_col = grid_col[:, None] * inverse[None, :]
    angles = jnp.concatenate([angle_row, angle_row, angle_col, angle_col], axis=-1)[:, None, :]
    first_half = vectors[..., :half_dim]
    second = vectors[..., half_dim:]
    turned = jnp.concatenate(
        [
            -first_half[..., quarter:],
            first_half[..., :quarter],
            -second[..., quarter:],
            second[..., :quarter],
        ],
        axis=-1,
    )
    return (
        vectors.astype(jnp.float32) * jnp.cos(angles) + turned.astype(jnp.float32) * jnp.sin(angles)
    ).astype(jnp.bfloat16)


def window_attend(query_rows, keys_pad, values_pad, sink_logits, key_start, total_len, window):
    row_count, query_heads, head_dim = query_rows.shape
    kv_heads = keys_pad.shape[1]
    group_size = query_heads // kv_heads
    block_count = row_count // window
    query_blocks = query_rows.reshape(block_count, window, kv_heads, group_size, head_dim)
    key_split = keys_pad.reshape(block_count + 2, window, kv_heads, head_dim)
    value_split = values_pad.reshape(block_count + 2, window, kv_heads, head_dim)
    key_band = jnp.concatenate([key_split[:-2], key_split[1:-1], key_split[2:]], axis=1)
    value_band = jnp.concatenate([value_split[:-2], value_split[1:-1], value_split[2:]], axis=1)
    scores = jnp.einsum(
        "kihgd,kjhd->khgij", query_blocks, key_band, preferred_element_type=jnp.float32
    ) * head_dim ** (-0.5)
    query_pos = jnp.arange(window)[:, None]
    band_pos = jnp.arange(3 * window)[None, :]
    within = jnp.abs(band_pos - window - query_pos) <= window
    key_pos = (
        key_start + jnp.arange(block_count)[:, None] * window + jnp.arange(3 * window)[None, :]
    )
    inside = (key_pos >= 0) & (key_pos < total_len)
    valid_pair = (within[None] & inside[:, None, :])[:, None, None]
    sink_logit = sink_logits.reshape(kv_heads, group_size)[None, :, :, None, None]
    masked = jnp.where(valid_pair, scores, -1e30)
    ceiling = jnp.maximum(jnp.max(masked, axis=-1, keepdims=True), sink_logit)
    weights = jnp.where(valid_pair, jnp.exp(masked - ceiling), 0.0)
    denominator = jnp.exp(sink_logit - ceiling) + jnp.sum(weights, axis=-1, keepdims=True)
    weights_bf = (weights / denominator).astype(jnp.bfloat16)
    mixed_rows = jnp.einsum(
        "khgij,kjhd->kihgd", weights_bf, value_band, preferred_element_type=jnp.float32
    )
    return mixed_rows.reshape(row_count, query_heads * head_dim).astype(jnp.bfloat16)


def block_terms(query_rows, key_rows, value_rows, log_rows, block_len):
    row_count, group_count, state_size = query_rows.shape
    head_ratio, head_dim = (value_rows.shape[2], value_rows.shape[3])
    block_count = row_count // block_len
    query_blocks = query_rows.reshape(block_count, block_len, group_count, state_size)
    key_blocks = key_rows.reshape(block_count, block_len, group_count, state_size)
    value_blocks = value_rows.reshape(block_count, block_len, group_count, head_ratio, head_dim)
    decay_cum = jnp.cumsum(
        log_rows.reshape(block_count, block_len, group_count, head_ratio), axis=1
    )
    decay_total = decay_cum[:, -1]
    gram_block = jnp.einsum(
        "kign,kjgn->kgij", query_blocks, key_blocks, preferred_element_type=jnp.float32
    )
    cum_heads = jnp.moveaxis(decay_cum, 1, 3)
    distance = jnp.abs(cum_heads[..., :, None] - cum_heads[..., None, :])
    pair_weight = (gram_block[:, :, None] * jnp.exp(-distance)).astype(jnp.bfloat16)
    near_terms = jnp.einsum(
        "kgrij,kjgrp->kigrp", pair_weight, value_blocks, preferred_element_type=jnp.float32
    )
    keys_after = (
        key_blocks[:, :, :, None, :] * jnp.exp(decay_total[:, None] - decay_cum)[..., None]
    ).astype(jnp.bfloat16)
    keys_before = (key_blocks[:, :, :, None, :] * jnp.exp(decay_cum)[..., None]).astype(
        jnp.bfloat16
    )
    state_after = jnp.einsum(
        "kjgrn,kjgrp->kgrnp", keys_after, value_blocks, preferred_element_type=jnp.float32
    )
    state_before = jnp.einsum(
        "kjgrn,kjgrp->kgrnp", keys_before, value_blocks, preferred_element_type=jnp.float32
    )
    before = jnp.cumsum(decay_total, axis=0) - decay_total
    overall = jnp.sum(decay_total, axis=0)
    after_sum = overall[None] - before - decay_total
    block_order = jnp.arange(block_count)
    earlier_mask = (block_order[None, :] < block_order[:, None])[:, :, None, None]
    later_mask = (block_order[None, :] > block_order[:, None])[:, :, None, None]
    gap_fwd = before[:, None] - before[None, :] - decay_total[None, :]
    gap_bwd = before[None, :] - before[:, None] - decay_total[:, None]
    weight_fwd = jnp.where(earlier_mask, jnp.exp(jnp.minimum(gap_fwd, 0.0)), 0.0)
    weight_bwd = jnp.where(later_mask, jnp.exp(jnp.minimum(gap_bwd, 0.0)), 0.0)
    carried_fwd = jnp.einsum(
        "abgr,bgrnp->agrnp", weight_fwd, state_after, precision=lax.Precision.HIGHEST
    )
    carried_bwd = jnp.einsum(
        "abgr,bgrnp->agrnp", weight_bwd, state_before, precision=lax.Precision.HIGHEST
    )
    summary_fwd = jnp.einsum(
        "agr,agrnp->grnp", jnp.exp(after_sum), state_after, precision=lax.Precision.HIGHEST
    )
    summary_bwd = jnp.einsum(
        "agr,agrnp->grnp", jnp.exp(before), state_before, precision=lax.Precision.HIGHEST
    )
    pieces = (
        near_terms,
        carried_fwd,
        carried_bwd,
        decay_cum,
        decay_total,
        before,
        after_sum,
        query_blocks,
    )
    return (pieces, (summary_fwd, summary_bwd, overall))


def finish_terms(pieces, incoming_fwd, incoming_bwd):
    (
        near_terms,
        carried_fwd,
        carried_bwd,
        decay_cum,
        decay_total,
        before,
        after_sum,
        query_blocks,
    ) = pieces
    total_fwd = carried_fwd + jnp.exp(before)[..., None, None] * incoming_fwd[None]
    total_bwd = carried_bwd + jnp.exp(after_sum)[..., None, None] * incoming_bwd[None]
    query_wide = query_blocks.astype(jnp.float32)
    read_fwd = jnp.einsum(
        "kign,kgrnp->kigrp", query_wide, total_fwd, precision=lax.Precision.HIGHEST
    )
    read_bwd = jnp.einsum(
        "kign,kgrnp->kigrp", query_wide, total_bwd, precision=lax.Precision.HIGHEST
    )
    combined = (
        near_terms
        + jnp.exp(decay_cum)[..., None] * read_fwd
        + jnp.exp(decay_total[:, None] - decay_cum)[..., None] * read_bwd
    )
    block_count, block_len, group_count, head_ratio, head_dim = combined.shape
    return combined.reshape(block_count * block_len, group_count, head_ratio, head_dim)


def combine_all(gathered_states, own_index):
    after_all, before_all, logs_all = gathered_states
    device_count = logs_all.shape[0]
    cum_incl = jnp.cumsum(logs_all, axis=0)
    cum_excl = cum_incl - logs_all
    device_order = jnp.arange(device_count)
    picker = (device_order == own_index).astype(jnp.float32)[:, None, None]
    own_incl = jnp.sum(picker * cum_incl, axis=0)
    own_excl = jnp.sum(picker * cum_excl, axis=0)
    lower_mask = (device_order < own_index)[:, None, None]
    higher_mask = (device_order > own_index)[:, None, None]
    weight_fwd = jnp.where(lower_mask, jnp.exp(jnp.minimum(own_excl[None] - cum_incl, 0.0)), 0.0)
    weight_bwd = jnp.where(higher_mask, jnp.exp(jnp.minimum(cum_excl - own_incl[None], 0.0)), 0.0)
    incoming_fwd = jnp.einsum(
        "dgr,dgrnp->grnp", weight_fwd, after_all, precision=lax.Precision.HIGHEST
    )
    incoming_bwd = jnp.einsum(
        "dgr,dgrnp->grnp", weight_bwd, before_all, precision=lax.Precision.HIGHEST
    )
    return (incoming_fwd, incoming_bwd)


def shards(
    tokens,
    norm_gain,
    state_gate,
    state_value,
    state_keys,
    state_query,
    state_step,
    state_rate,
    state_jumps,
    state_gain,
    filter_value,
    filter_keys,
    filter_query,
    window_query,
    window_keys,
    window_values,
    window_sink,
    state_output,
    window_output,
):
    row_count = tokens.shape[0]
    rows_wide = tokens.astype(jnp.float32)
    normed = (
        rows_wide
        * lax.rsqrt(jnp.mean(rows_wide * rows_wide, axis=-1, keepdims=True) + 1e-06)
        * norm_gain
    ).astype(jnp.bfloat16)
    gathered = (
        lax.all_gather(state_gate, "sp", axis=0, tiled=True),
        lax.all_gather(state_value, "sp", axis=0, tiled=True),
        lax.all_gather(state_keys, "sp", axis=0, tiled=True),
        lax.all_gather(state_query, "sp", axis=0, tiled=True),
        lax.all_gather(window_query, "sp", axis=0, tiled=True),
        lax.all_gather(window_keys, "sp", axis=0, tiled=True),
        lax.all_gather(window_values, "sp", axis=0, tiled=True),
        lax.all_gather(state_output, "sp", axis=1, tiled=True),
        lax.all_gather(window_output, "sp", axis=1, tiled=True),
    )
    projected = [
        jnp.dot(normed, matrix, preferred_element_type=jnp.float32) for matrix in gathered[:7]
    ]
    out_state = gathered[7]
    out_window = gathered[8]
    gate_rows, value_pre, keys_pre, query_pre, query_raw, keys_raw, values_rows = [
        result.astype(jnp.bfloat16) for result in projected
    ]
    head_local = state_rate.shape[0]
    group_local = keys_pre.shape[1] // STATE_SIZE
    head_dim = value_pre.shape[1] // head_local
    head_ratio = head_local // group_local
    step_cols = lax.dynamic_slice_in_dim(
        state_step, lax.axis_index("tp") * head_local, head_local, 1
    )
    step_rows = jax.nn.softplus(jnp.dot(normed, step_cols, preferred_element_type=jnp.float32))
    log_decay = -state_rate[None, :] * step_rows + state_jumps
    half_width = filter_value.shape[0] // 2
    stacked = jnp.concatenate([value_pre, keys_pre, query_pre], axis=-1)
    padded = extended(stacked, (("sp", 0),), half_width)
    filters = jnp.concatenate([filter_value, filter_keys, filter_query], axis=-1).astype(
        jnp.float32
    )
    filtered = jnp.zeros(stacked.shape, jnp.float32)
    for offset in range(filters.shape[0]):
        filtered = (
            filtered + padded[offset : offset + row_count].astype(jnp.float32) * filters[offset]
        )
    value_cols = value_pre.shape[1]
    key_cols = keys_pre.shape[1]
    inner_rows = (
        jax.nn.silu(filtered[:, :value_cols]).reshape(row_count, head_local, head_dim)
        * step_rows[..., None]
    )
    scan_values = inner_rows.astype(jnp.bfloat16).reshape(
        row_count, group_local, head_ratio, head_dim
    )
    scan_keys = (
        filtered[:, value_cols : value_cols + key_cols]
        .astype(jnp.bfloat16)
        .reshape(row_count, group_local, STATE_SIZE)
    )
    scan_query = (
        filtered[:, value_cols + key_cols :]
        .astype(jnp.bfloat16)
        .reshape(row_count, group_local, STATE_SIZE)
    )
    pieces, summaries = block_terms(
        scan_query,
        scan_keys,
        scan_values,
        log_decay.reshape(row_count, group_local, head_ratio),
        BLOCK,
    )
    summary_fwd, summary_bwd, overall = summaries
    gathered_states = (
        lax.all_gather(summary_fwd[None].astype(jnp.bfloat16), "sp", axis=0, tiled=True).astype(
            jnp.float32
        ),
        lax.all_gather(summary_bwd[None].astype(jnp.bfloat16), "sp", axis=0, tiled=True).astype(
            jnp.float32
        ),
        lax.all_gather(overall[None].astype(jnp.bfloat16), "sp", axis=0, tiled=True).astype(
            jnp.float32
        ),
    )
    incoming_fwd, incoming_bwd = combine_all(gathered_states, lax.axis_index("sp"))
    scan_out = finish_terms(pieces, incoming_fwd, incoming_bwd).reshape(
        row_count, head_local * head_dim
    )
    gated_rows = scan_out * jax.nn.silu(gate_rows.astype(jnp.float32))
    per_head = gated_rows.reshape(row_count, head_local, head_dim)
    state_mix = (
        (
            per_head
            * lax.rsqrt(jnp.mean(per_head * per_head, axis=-1, keepdims=True) + 1e-06)
            * state_gain.reshape(head_local, head_dim)
        )
        .astype(jnp.bfloat16)
        .reshape(row_count, head_local * head_dim)
    )
    query_heads = window_sink.shape[0]
    kv_heads = keys_raw.shape[1] // HEAD_DIM
    kv_width = kv_heads * HEAD_DIM
    positions = lax.axis_index("sp") * row_count + jnp.arange(row_count, dtype=jnp.int32)
    query_rot = rotate_grid(
        query_raw.reshape(row_count, query_heads, HEAD_DIM), positions, GRID_WIDTH
    )
    keys_rot = rotate_grid(keys_raw.reshape(row_count, kv_heads, HEAD_DIM), positions, GRID_WIDTH)
    pair_rows = jnp.concatenate([keys_rot.reshape(row_count, kv_width), values_rows], axis=-1)
    padded_pair = extended(pair_rows, (("sp", 0),), WINDOW)
    keys_pad = padded_pair[:, :kv_width].reshape(-1, kv_heads, HEAD_DIM)
    values_pad = padded_pair[:, kv_width:].reshape(-1, kv_heads, HEAD_DIM)
    window_mix = window_attend(
        query_rot,
        keys_pad,
        values_pad,
        window_sink,
        lax.axis_index("sp") * row_count - WINDOW,
        lax.axis_size("sp") * row_count,
        WINDOW,
    )
    return lax.psum_scatter(
        (
            jnp.dot(state_mix, out_state, preferred_element_type=jnp.float32)
            + jnp.dot(window_mix, out_window, preferred_element_type=jnp.float32)
        ).astype(jnp.bfloat16),
        "tp",
        scatter_dimension=0,
        tiled=True,
    )


def fits(*args):
    tokens, state_value, state_keys, state_rate = args[0], args[3], args[4], args[7]
    window_query, window_keys, window_sink = args[13], args[14], args[16]
    parts = lax.axis_size("fs")
    heads = state_rate.shape[0]
    return (
        parts == 4
        and lax.axis_size("tp") == 2
        and lax.axis_size("sp") > 1
        and tokens.shape[0] % (4 * BLOCK) == 0
        and state_keys.shape[1] == parts * STATE_SIZE
        and state_value.shape[1] == parts * STATE_SIZE
        and heads == 2 * parts
        and window_keys.shape[1] == parts * HEAD_DIM
        and window_query.shape[1] == 2 * parts * HEAD_DIM
        and window_sink.shape[0] == 2 * parts
    )


def fused_kernel(
    count,
    tokens,
    w_value,
    w_keys,
    w_query,
    w_gate,
    w_wkeys,
    w_wvalues,
    w_wquery,
    w_sout,
    w_wout,
    norm_gain,
    step_w,
    rate,
    jumps,
    gain,
    tap_value,
    tap_keys,
    tap_query,
    sink,
    out,
    tbuf,
    xbuf,
    wbuf,
    wob,
    stepx,
    cos_t,
    sin_t,
    jbuf,
    cbuf,
    gbuf,
    stbuf,
    nbuf,
    sabuf,
    sbbuf,
    cumbuf,
    edge,
    sqbuf,
    fin,
    gin,
    fout,
    gout,
    kvbuf,
    qbuf,
    mixs,
    mixr,
    psend,
    pown,
    precv,
    loc_sem,
    z_send,
    z_recv,
    x_send,
    x_recv,
    d_send,
    d_recv,
    j_send,
    j_recv,
    h_send,
    h_recv,
    m_send,
    m_recv,
    o_send,
    o_recv,
    p_send,
    p_recv,
):
    f32, bf16 = jnp.float32, jnp.bfloat16
    me, fs, tp = lax.axis_index("sp"), lax.axis_index("fs"), lax.axis_index("tp")
    rows, width = tokens.shape
    depth = w_value.shape[0]
    half = rows // 2
    quarter = half // 2
    blocks = rows // BLOCK
    lanes = STATE_SIZE
    has = [me > 0, me < count - 1]
    beside = [jnp.maximum(me - 1, 0), jnp.minimum(me + 1, count - 1)]
    peers = [fs, fs + 1 - 2 * (fs % 2), fs + 2 - 4 * (fs // 2), 3 - fs]
    other = 1 - tp

    def to(ref_src, ref_dst, send, recv, axis, index):
        return pltpu.make_async_remote_copy(
            src_ref=ref_src,
            dst_ref=ref_dst,
            send_sem=send,
            recv_sem=recv,
            device_id={axis: index},
            device_id_type=pl.DeviceIdType.MESH,
        )

    own_rows = pl.ds(pl.multiple_of(me * depth, depth), depth)
    loads = [pltpu.make_async_copy(tokens, tbuf, loc_sem.at[0])]
    col = 0
    weight_loads = []
    for index, matrix in enumerate(
        (w_value, w_keys, w_query, w_gate, w_wkeys, w_wvalues, w_wquery)
    ):
        size = matrix.shape[1] // 4
        weight_loads.append(
            pltpu.make_async_copy(
                matrix.at[:, pl.ds(pl.multiple_of(fs * size, size), size)],
                wbuf.at[own_rows, pl.ds(col, size)],
                loc_sem.at[1 + index],
            )
        )
        col += size
    out_loads = []
    first_rows = w_sout.shape[0] // 4
    second_rows = w_wout.shape[0] // 4
    for part in range(4):
        out_loads.append(
            pltpu.make_async_copy(
                w_sout.at[pl.ds(part * first_rows, first_rows)],
                wob.at[me, part, pl.ds(0, first_rows)],
                loc_sem.at[8 + 2 * part],
            )
        )
        out_loads.append(
            pltpu.make_async_copy(
                w_wout.at[pl.ds(part * second_rows, second_rows)],
                wob.at[me, part, pl.ds(first_rows, second_rows)],
                loc_sem.at[9 + 2 * part],
            )
        )
    for load in weight_loads + loads:
        load.start()

    barrier = pltpu.get_barrier_semaphore()
    for side in range(2):
        pl.when(has[side])(
            lambda side=side: pl.semaphore_signal(
                barrier,
                inc=1,
                device_id={"sp": beside[side]},
                device_id_type=pl.DeviceIdType.MESH,
            )
        )
    for k in range(1, 4):
        pl.semaphore_signal(
            barrier, inc=1, device_id={"fs": peers[k]}, device_id_type=pl.DeviceIdType.MESH
        )
    pl.semaphore_signal(
        barrier, inc=1, device_id={"tp": other}, device_id_type=pl.DeviceIdType.MESH
    )
    pl.semaphore_wait(barrier, 4 + jnp.minimum(me, 1) + jnp.minimum(count - 1 - me, 1))

    spans = ((0, 4 * lanes), (4 * lanes, 2 * lanes), (6 * lanes, 2 * lanes))

    def line(piece, hop, side):
        origin = me - hop if side == 1 else me + hop
        origin = jnp.clip(origin, 0, count - 1)
        if piece == 3:
            ref = wob.at[origin, fs]
        else:
            start, size = spans[piece]
            ref = wbuf.at[pl.ds(pl.multiple_of(origin * depth, depth), depth), pl.ds(start, size)]
        slot = (side * 4 + piece) * (count - 1) + hop
        return to(ref, ref, z_send.at[slot], z_recv.at[slot], "sp", beside[side])

    def valid(hop, side):
        return me >= hop if side == 1 else me + hop <= count - 1

    def send_line(piece, hop):
        for side in range(2):
            pl.when(has[side] & valid(hop, side))(
                lambda side=side: line(piece, hop, side).start()
            )

    def take_line(piece, hop, then=None):
        for side in range(2):

            def arrive(side=side):
                line_in(piece, hop, side).wait_recv()
                if hop < count - 1:
                    pl.when(has[side])(lambda: line(piece, hop, side).start())
                if then is not None:
                    then(hop, side)

            pl.when(valid(hop, side))(arrive)

    def line_in(piece, hop, side):
        origin = me - hop if side == 1 else me + hop
        origin = jnp.clip(origin, 0, count - 1)
        if piece == 3:
            ref = wob.at[origin, fs]
        else:
            start, size = spans[piece]
            ref = wbuf.at[pl.ds(pl.multiple_of(origin * depth, depth), depth), pl.ds(start, size)]
        slot = (side * 4 + piece) * (count - 1) + hop - 1
        return to(ref, ref, z_send.at[slot], z_recv.at[slot], "sp", beside[side])

    for load in weight_loads:
        load.wait()
    send_line(0, 0)
    send_line(1, 0)

    loads[0].wait()
    norm_rows = 32

    def norm(index, base):
        at = pl.ds(pl.multiple_of(base + index * norm_rows, norm_rows), norm_rows)
        wide = tbuf[at, :].astype(f32)
        scale = lax.rsqrt(jnp.mean(wide * wide, axis=-1, keepdims=True) + 1e-06)
        xbuf[fs, at, :] = (wide * scale * norm_gain[...]).astype(bf16)
        return base

    lax.fori_loop(0, half // norm_rows, norm, tp * half)
    lax.fori_loop(0, half // norm_rows, norm, other * half)
    own_half = pl.ds(pl.multiple_of(tp * half, half), half)
    x_own = [
        to(
            xbuf.at[fs, own_half],
            xbuf.at[fs, own_half],
            x_send.at[k - 1],
            x_recv.at[k - 1],
            "fs",
            peers[k],
        )
        for k in (1, 2)
    ]
    for copy in x_own:
        copy.start()
    j_own = [
        to(jumps, jbuf.at[fs], j_send.at[k], j_recv.at[k], "fs", peers[k]) for k in range(1, 4)
    ]
    for copy in j_own:
        copy.start()
    for load in out_loads:
        load.start()
    jbuf[fs, :, :] = jumps[...]

    lane = lax.broadcasted_iota(jnp.int32, (1, lanes), 1)
    low = lane < lanes // 2
    q4 = HEAD_DIM // 4

    def table(index, carry):
        at = pl.ds(pl.multiple_of(index * BLOCK, BLOCK), BLOCK)
        spot = lax.broadcasted_iota(jnp.int32, (BLOCK, lanes), 0) + me * rows + index * BLOCK
        place = jnp.where(low, spot // GRID_WIDTH, spot % GRID_WIDTH).astype(f32)
        inverse = jnp.exp((lane % q4).astype(f32) * (-math.log(10000.0) / q4))
        angle = place * inverse
        cos_t[at, :] = jnp.cos(angle)
        sin_t[at, :] = jnp.where(lane % (2 * q4) < q4, -1.0, 1.0) * jnp.sin(angle)
        return carry

    lax.fori_loop(0, blocks, table, 0)
    heads_all = step_w.shape[1]
    first_head = (tp * 4 + fs) * 2
    pick = (
        lax.broadcasted_iota(jnp.int32, (heads_all, lanes), 0)
        == first_head + lax.broadcasted_iota(jnp.int32, (heads_all, lanes), 1) // (lanes // 2)
    )
    stepx[...] = jnp.dot(
        step_w[...], pick.astype(f32).astype(bf16), preferred_element_type=f32
    ).astype(bf16)

    take_line(0, 1)
    send_line(2, 0)

    x_first = pl.ds(pl.multiple_of(tp * half, quarter), quarter)
    x_second = pl.ds(pl.multiple_of(tp * half + quarter, quarter), quarter)

    def x_in(k, at, slot):
        return to(xbuf.at[peers[k], at], xbuf.at[peers[k], at], x_send.at[slot], x_recv.at[slot], "fs", peers[k])

    relay = [
        to(xbuf.at[peers[1], x_first], xbuf.at[peers[1], x_first], x_send.at[2], x_recv.at[2], "fs", peers[2]),
        to(xbuf.at[peers[2], x_second], xbuf.at[peers[2], x_second], x_send.at[3], x_recv.at[3], "fs", peers[1]),
    ]
    across = [
        to(xbuf.at[peers[k], own_half], xbuf.at[peers[k], own_half], d_send.at[k - 1], d_recv.at[k - 1], "tp", other)
        for k in range(1, 4)
    ]
    for k in (1, 2):
        x_in(k, own_half, k - 1).wait_recv()
        relay[k - 1].start()
        across[k - 1].start()
    if count > 2:
        take_line(0, 2)
    take_line(1, 1)
    x_in(3, x_first, 2).wait_recv()
    x_in(3, x_second, 3).wait_recv()
    across[2].start()
    for hop in range(3, count):
        take_line(0, hop)
    other_half = pl.ds(pl.multiple_of(other * half, half), half)
    for k in range(1, 4):
        to(xbuf.at[peers[k], other_half], xbuf.at[peers[k], other_half], d_send.at[k - 1], d_recv.at[k - 1], "tp", other).wait_recv()

    def project_state(index, carry):
        seq, at = index // 2, pl.ds(pl.multiple_of((index % 2) * half, half), half)
        x = xbuf[seq, at, :]
        y = jnp.dot(x, wbuf[:, : 4 * lanes], preferred_element_type=f32)
        to_at = pl.ds(pl.multiple_of((index % 2) * half + 8, 8), half)
        cbuf[seq, to_at, :] = y[:, : 3 * lanes].astype(bf16).astype(f32)
        gbuf[seq, at, :] = y[:, 3 * lanes :].astype(bf16)
        z = jnp.dot(x, stepx[...], preferred_element_type=f32)
        stbuf[seq, at, :] = jnp.maximum(z, 0.0) + jnp.log1p(jnp.exp(-jnp.abs(z)))
        return carry

    lax.fori_loop(0, 8, project_state, 0)
    low_edge, high_edge = pl.ds(0, 8), pl.ds(rows + 8, 8)
    halo = [
        to(cbuf.at[:, pl.ds(8, 8)], cbuf.at[:, high_edge], h_send.at[0], h_recv.at[0], "sp", beside[0]),
        to(cbuf.at[:, pl.ds(rows, 8)], cbuf.at[:, low_edge], h_send.at[1], h_recv.at[1], "sp", beside[1]),
    ]
    halo_in = [
        to(cbuf.at[:, low_edge], cbuf.at[:, low_edge], h_send.at[1], h_recv.at[1], "sp", beside[0]),
        to(cbuf.at[:, high_edge], cbuf.at[:, high_edge], h_send.at[0], h_recv.at[0], "sp", beside[1]),
    ]
    for side in range(2):
        pl.when(has[side])(lambda side=side: halo[side].start())
    edges = (low_edge, high_edge)
    for side in range(2):

        def clear(side=side):
            cbuf[:, edges[side], :] = jnp.zeros((4, 8, 3 * lanes), f32)

        pl.when(jnp.logical_not(has[side]))(clear)
    for hop in range(2, count - 1):
        take_line(1, hop)
    for hop in range(1, count - 1):
        take_line(2, hop)
    for load in out_loads:
        load.wait()
    send_line(3, 0)
    for copy in j_own:
        copy.wait_send()
    for k in range(1, 4):
        to(jumps, jbuf.at[peers[k]], j_send.at[k], j_recv.at[k], "fs", peers[k]).wait_recv()
    for side in range(2):
        pl.when(has[side])(lambda side=side: halo_in[side].wait_recv())

    own_cols = pl.ds(pl.multiple_of(fs * lanes, lanes), lanes)
    taps = jnp.concatenate(
        [ref[:, own_cols].astype(f32) for ref in (tap_value, tap_keys, tap_query)], axis=1
    )
    rate_lane = jnp.where(low, rate[2 * fs], rate[2 * fs + 1])
    row_id = lax.broadcasted_iota(jnp.int32, (BLOCK, lanes), 0)
    col_id = lax.broadcasted_iota(jnp.int32, (BLOCK, lanes), 1)
    lower = (col_id <= row_id).astype(f32)
    left = col_id < lanes // 2
    tap_count = taps.shape[0]
    reach = tap_count // 2
    tall = BLOCK + 16
    high = lax.Precision.HIGHEST

    def scan_block(index, carry):
        seq, blk = index // blocks, index % blocks
        at = pl.ds(pl.multiple_of(blk * BLOCK, BLOCK), BLOCK)
        pre = cbuf[seq, pl.ds(pl.multiple_of(blk * BLOCK, BLOCK), tall), :]
        filt = jnp.zeros((BLOCK, 3 * lanes), f32)
        for tap in range(tap_count):
            moved = pre if tap == reach else pltpu.roll(pre, (reach - tap) % tall, 0)
            filt = filt + moved[8 : 8 + BLOCK] * taps[tap : tap + 1, :]
        fv, fk, fq = filt[:, :lanes], filt[:, lanes : 2 * lanes], filt[:, 2 * lanes :]
        step = stbuf[seq, at, :]
        sv = (fv * jax.nn.sigmoid(fv) * step).astype(bf16)
        sk, sq = fk.astype(bf16), fq.astype(bf16)
        sqbuf[seq, at, :] = sq
        jrows = jbuf[seq, :, at]
        jrow_id = lax.broadcasted_iota(jnp.int32, jrows.shape, 0)
        jrow = [
            jnp.sum(jnp.where(jrow_id == 2 * fs + r, jrows, 0.0), axis=0, keepdims=True)
            for r in range(2)
        ]
        jump = jnp.where(row_id < lanes // 2, jrow[0], jrow[1]).T
        logs = jump - rate_lane * step
        cum = jnp.dot(lower, logs, preferred_element_type=f32, precision=high)
        cumbuf[seq, at, :] = cum
        cum_t = cum.T
        gram = lax.dot_general(sq, sk, (((1,), (1,)), ((), ())), preferred_element_type=f32)
        key_t = sk.astype(f32).T
        near, after, before = [], [], []
        for r in range(2):
            spot = r * (lanes // 2)
            down = cum[:, spot : spot + 1]
            across_row = cum_t[spot : spot + 1, :]
            pair = (gram * jnp.exp(-jnp.abs(down - across_row))).astype(bf16)
            near.append(jnp.dot(pair, sv, preferred_element_type=f32))
            last = across_row[:, BLOCK - 1 : BLOCK]
            k_after = (key_t * jnp.exp(last - across_row)).astype(bf16)
            after.append(jnp.dot(k_after, sv, preferred_element_type=f32))
            k_before = (key_t * jnp.exp(across_row)).astype(bf16)
            before.append(jnp.dot(k_before, sv, preferred_element_type=f32))
        nbuf[seq, at, :] = jnp.where(left, near[0], near[1])
        sabuf[index, :, :] = jnp.where(left, after[0], after[1])
        sbbuf[index, :, :] = jnp.where(left, before[0], before[1])
        return carry

    lax.fori_loop(0, 4 * blocks, scan_block, 0)

    zero_state = jnp.zeros((STATE_SIZE, lanes), f32)

    def total_of(seq, blk):
        return cumbuf[seq, blk * BLOCK + BLOCK - 8 : blk * BLOCK + BLOCK, :][7:8, :]

    def carry_states(seq, carry):
        state, so_far = zero_state, jnp.zeros((1, lanes), f32)
        for blk in range(blocks):
            added = sabuf[seq * blocks + blk, :, :]
            sabuf[seq * blocks + blk, :, :] = state
            edge[seq * blocks + blk, 0:1, :] = so_far
            total = total_of(seq, blk)
            state = state * jnp.exp(total) + added
            so_far = so_far + total
        fout[seq, :, :] = state.astype(bf16)
        edge[4 * blocks + seq, 0:1, :] = so_far
        state, so_far = zero_state, jnp.zeros((1, lanes), f32)
        for blk in range(blocks - 1, -1, -1):
            added = sbbuf[seq * blocks + blk, :, :]
            sbbuf[seq * blocks + blk, :, :] = state
            edge[seq * blocks + blk, 1:2, :] = so_far
            total = total_of(seq, blk)
            state = state * jnp.exp(total) + added
            so_far = so_far + total
        gout[seq, :, :] = state.astype(bf16)
        return carry

    lax.fori_loop(0, 4, carry_states, 0)
    chain = [
        to(gout, gin, h_send.at[2], h_recv.at[2], "sp", beside[0]),
        to(fout, fin, h_send.at[3], h_recv.at[3], "sp", beside[1]),
    ]

    def clear_forward():
        fin[...] = jnp.zeros(fin.shape, bf16)

    def clear_backward():
        gin[...] = jnp.zeros(gin.shape, bf16)

    pl.when(me == 0)(clear_forward)
    pl.when(me == count - 1)(clear_backward)
    pl.when(me == 0)(lambda: chain[1].start())
    pl.when(me == count - 1)(lambda: chain[0].start())

    def rotated(vectors, at):
        lane_full = lax.broadcasted_iota(jnp.int32, vectors.shape, 1)
        turned = jnp.where(
            lane_full % (2 * q4) < q4,
            pltpu.roll(vectors, HEAD_DIM - q4, 1),
            pltpu.roll(vectors, q4, 1),
        )
        return (vectors * cos_t[at, :] + turned * sin_t[at, :]).astype(bf16)

    for hop in range(max(2, count - 1), count):
        take_line(1, hop)

    def project_pair(index, carry):
        seq, at = index // 2, pl.ds(pl.multiple_of((index % 2) * half, half), half)
        y = jnp.dot(
            xbuf[seq, at, :], wbuf[:, 4 * lanes : 6 * lanes], preferred_element_type=f32
        ).astype(bf16)
        to_at = pl.ds(pl.multiple_of((index % 2) * half + WINDOW, WINDOW), half)
        kvbuf[seq, to_at, : HEAD_DIM] = rotated(y[:, :HEAD_DIM].astype(f32), at)
        kvbuf[seq, to_at, HEAD_DIM:] = y[:, HEAD_DIM:]
        return carry

    lax.fori_loop(0, 8, project_pair, 0)
    bottom, top = pl.ds(0, WINDOW), pl.ds(rows + WINDOW, WINDOW)
    kv_edge = [
        to(kvbuf.at[:, pl.ds(WINDOW, WINDOW)], kvbuf.at[:, top], h_send.at[4], h_recv.at[4], "sp", beside[0]),
        to(kvbuf.at[:, pl.ds(rows, WINDOW)], kvbuf.at[:, bottom], h_send.at[5], h_recv.at[5], "sp", beside[1]),
    ]
    kv_in = [
        to(kvbuf.at[:, bottom], kvbuf.at[:, bottom], h_send.at[5], h_recv.at[5], "sp", beside[0]),
        to(kvbuf.at[:, top], kvbuf.at[:, top], h_send.at[4], h_recv.at[4], "sp", beside[1]),
    ]
    for side in range(2):
        pl.when(has[side])(lambda side=side: kv_edge[side].start())
    bands = (bottom, top)
    for side in range(2):

        def clear_band(side=side):
            kvbuf[:, bands[side], :] = jnp.zeros((4, WINDOW, 2 * HEAD_DIM), bf16)

        pl.when(jnp.logical_not(has[side]))(clear_band)

    def forward_step():
        to(fin, fin, h_send.at[3], h_recv.at[3], "sp", beside[0]).wait_recv()

        def add(seq, carry):
            passed = jnp.exp(edge[4 * blocks + seq, 0:1, :])
            fout[seq, :, :] = (
                fout[seq, :, :].astype(f32) + passed * fin[seq, :, :].astype(f32)
            ).astype(bf16)
            return carry

        def pass_on():
            lax.fori_loop(0, 4, add, 0)
            chain[1].start()

        pl.when(has[1])(pass_on)

    def backward_step():
        to(gin, gin, h_send.at[2], h_recv.at[2], "sp", beside[1]).wait_recv()

        def add(seq, carry):
            passed = jnp.exp(edge[4 * blocks + seq, 0:1, :])
            gout[seq, :, :] = (
                gout[seq, :, :].astype(f32) + passed * gin[seq, :, :].astype(f32)
            ).astype(bf16)
            return carry

        def pass_on():
            lax.fori_loop(0, 4, add, 0)
            chain[0].start()

        pl.when(has[0])(pass_on)

    pl.when(has[0])(forward_step)
    pl.when(has[1])(backward_step)

    gain_row = gain[:, own_cols]

    def split_dot(a, b):
        top_bits = b.astype(bf16)
        rest = (b - top_bits.astype(f32)).astype(bf16)
        return jnp.dot(a, top_bits, preferred_element_type=f32) + jnp.dot(
            a, rest, preferred_element_type=f32
        )

    def finish_block(index, carry):
        seq, blk = index // blocks, index % blocks
        at = pl.ds(pl.multiple_of(blk * BLOCK, BLOCK), BLOCK)
        ahead = sabuf[index, :, :] + jnp.exp(edge[index, 0:1, :]) * fin[seq, :, :].astype(f32)
        behind = sbbuf[index, :, :] + jnp.exp(edge[index, 1:2, :]) * gin[seq, :, :].astype(f32)
        sq = sqbuf[seq, at, :]
        cum = cumbuf[seq, at, :]
        total = cum[BLOCK - 1 : BLOCK, :]
        mixed = (
            nbuf[seq, at, :]
            + jnp.exp(cum) * split_dot(sq, ahead)
            + jnp.exp(total - cum) * split_dot(sq, behind)
        )
        g = gbuf[seq, at, :].astype(f32)
        gated = mixed * (g * jax.nn.sigmoid(g))
        square = gated * gated
        first = jnp.sum(jnp.where(left, square, 0.0), axis=-1, keepdims=True)
        second = jnp.sum(jnp.where(left, 0.0, square), axis=-1, keepdims=True)
        mean = jnp.where(left, first, second) * (2.0 / lanes)
        mixs[seq, at, :lanes] = (gated * lax.rsqrt(mean + 1e-06) * gain_row).astype(bf16)
        return carry

    lax.fori_loop(0, 4 * blocks, finish_block, 0)
    state_part, window_part = pl.ds(0, lanes), pl.ds(lanes, 2 * HEAD_DIM)

    def swap(k, part, slot):
        return to(
            mixs.at[peers[k], :, part],
            mixr.at[fs, :, part],
            m_send.at[slot * 4 + k],
            m_recv.at[slot * 4 + k],
            "fs",
            peers[k],
        )

    def swap_in(k, part, slot):
        ref = mixr.at[peers[k], :, part]
        return to(ref, ref, m_send.at[slot * 4 + k], m_recv.at[slot * 4 + k], "fs", peers[k])

    for k in (3, 1, 2):
        swap(k, state_part, 0).start()

    def spread(hop, side):
        origin = jnp.clip(me - hop if side == 1 else me + hop, 0, count - 1)
        for k in (3, 1, 2):
            to(
                wob.at[origin, fs],
                wob.at[origin, fs],
                o_send.at[origin * 4 + k],
                o_recv.at[origin * 4 + k],
                "fs",
                peers[k],
            ).start()

    take_line(3, 1, spread)

    for hop in range(count - 1, count):
        take_line(2, hop)

    def project_query(index, carry):
        seq, at = index // 2, pl.ds(pl.multiple_of((index % 2) * half, half), half)
        y = jnp.dot(
            xbuf[seq, at, :], wbuf[:, 6 * lanes :], preferred_element_type=f32
        ).astype(bf16).astype(f32)
        for r in range(2):
            qbuf[seq, at, r * HEAD_DIM : (r + 1) * HEAD_DIM] = rotated(
                y[:, r * HEAD_DIM : (r + 1) * HEAD_DIM], at
            )
        return carry

    lax.fori_loop(0, 8, project_query, 0)
    for side in range(2):
        pl.when(has[side])(lambda side=side: kv_in[side].wait_recv())
    band = 3 * WINDOW
    q_id = lax.broadcasted_iota(jnp.int32, (2 * WINDOW, band), 0)
    b_id = lax.broadcasted_iota(jnp.int32, (2 * WINDOW, band), 1)
    within = jnp.abs(b_id - WINDOW - q_id % WINDOW) <= WINDOW
    sink_col = jnp.where(
        lax.broadcasted_iota(jnp.int32, (2 * WINDOW, 1), 0) < WINDOW,
        sink[2 * fs],
        sink[2 * fs + 1],
    )

    def attend(seq):
        def body(blk, carry):
            at = pl.ds(pl.multiple_of(blk * WINDOW, WINDOW), WINDOW)
            wide = pl.ds(pl.multiple_of(blk * WINDOW, WINDOW), band)
            q = jnp.concatenate([qbuf[seq, at, :HEAD_DIM], qbuf[seq, at, HEAD_DIM:]], axis=0)
            s = lax.dot_general(
                q,
                kvbuf[seq, wide, :HEAD_DIM],
                (((1,), (1,)), ((), ())),
                preferred_element_type=f32,
            ) * (HEAD_DIM ** (-0.5))
            place = me * rows + (blk - 1) * WINDOW + b_id
            ok = within & (place >= 0) & (place < count * rows)
            s = jnp.where(ok, s, -1e30)
            m = jnp.maximum(jnp.max(s, axis=-1, keepdims=True), sink_col)
            w = jnp.where(ok, jnp.exp(s - m), 0.0)
            total = jnp.exp(sink_col - m) + jnp.sum(w, axis=-1, keepdims=True)
            p = (w * (1.0 / total)).astype(bf16)
            o = jnp.dot(p, kvbuf[seq, wide, HEAD_DIM:], preferred_element_type=f32).astype(bf16)
            mixs[seq, at, lanes : lanes + HEAD_DIM] = o[:WINDOW]
            mixs[seq, at, lanes + HEAD_DIM :] = o[WINDOW:]
            return carry

        lax.fori_loop(0, blocks, body, 0)

    def attend_peer(step, carry):
        seq = jnp.where(step == 0, peers[3], jnp.where(step == 1, peers[1], jnp.where(step == 2, peers[2], fs)))
        attend(seq)
        for index, k in enumerate((3, 1, 2)):
            pl.when(step == index)(lambda k=k: swap(k, window_part, 1).start())
        return carry

    lax.fori_loop(0, 4, attend_peer, 0)
    mixr[fs, :, :] = mixs[fs, :, :]
    for hop in range(2, count - 1):
        take_line(3, hop, spread)
    for k in range(1, 4):
        swap_in(k, state_part, 0).wait_recv()
        swap_in(k, window_part, 1).wait_recv()

    cols = w_sout.shape[1]

    def share(origin, at):
        total = jnp.zeros((half, cols), f32)
        for part in range(4):
            total = total + jnp.dot(
                mixr[part, at, :], wob[origin, part, :, :], preferred_element_type=f32
            )
        return total.astype(bf16)

    def trade(origin):
        return to(
            psend.at[origin], precv.at[origin], p_send.at[origin], p_recv.at[origin], "tp", other
        )

    def out_quarter(step, carry):
        hop, side = (step + 1) // 2, (step + 1) % 2
        origin = me + jnp.where(side == 1, -hop, hop)
        there = (origin >= 0) & (origin < count) & ((hop > 0) | (side == 1))
        origin = jnp.clip(origin, 0, count - 1)

        def work():
            def gather():
                for k in range(1, 4):
                    to(
                        wob.at[origin, peers[k]],
                        wob.at[origin, peers[k]],
                        o_send.at[origin * 4 + k],
                        o_recv.at[origin * 4 + k],
                        "fs",
                        peers[k],
                    ).wait_recv()

            pl.when(hop > 0)(gather)
            psend[origin, :, :] = share(origin, other_half)
            trade(origin).start()
            pown[origin, :, :] = share(origin, own_half)

        pl.when(there)(work)
        return carry

    lax.fori_loop(0, 3, out_quarter, 0)
    if count > 2:
        take_line(3, count - 1, spread)
        lax.fori_loop(3, 2 * count - 1, out_quarter, 0)
    for origin in range(count):
        trade(origin).wait_recv()
        at = pl.ds(origin * cols, cols)
        out[:, at] = (
            pown[origin, :, :].astype(f32) + precv[origin, :, :].astype(f32)
        ).astype(bf16)

    for piece in range(4):
        for hop in range(count - 1):
            for side in range(2):
                pl.when(has[side] & valid(hop, side))(
                    lambda piece=piece, hop=hop, side=side: line(piece, hop, side).wait_send()
                )
    for copy in x_own + relay + across:
        copy.wait_send()
    for side in range(2):
        pl.when(has[side])(lambda side=side: halo[side].wait_send())
        pl.when(has[side])(lambda side=side: chain[side].wait_send())
        pl.when(has[side])(lambda side=side: kv_edge[side].wait_send())
    for k in range(1, 4):
        swap(k, state_part, 0).wait_send()
        swap(k, window_part, 1).wait_send()

        def left_plane(origin, carry, k=k):
            ref = wob.at[origin, fs]
            slot = origin * 4 + k
            pl.when(origin != me)(
                lambda: to(ref, ref, o_send.at[slot], o_recv.at[slot], "fs", peers[k]).wait_send()
            )
            return carry

        lax.fori_loop(0, count, left_plane, 0)
    for origin in range(count):
        trade(origin).wait_send()


def fused_shards(
    tokens,
    norm_gain,
    state_gate,
    state_value,
    state_keys,
    state_query,
    state_step,
    state_rate,
    state_jumps,
    state_gain,
    filter_value,
    filter_keys,
    filter_query,
    window_query,
    window_keys,
    window_values,
    window_sink,
    state_output,
    window_output,
):
    count = lax.axis_size("sp")
    rows, width = tokens.shape
    lanes = STATE_SIZE
    blocks = rows // BLOCK
    depth = state_value.shape[0]
    cols = state_output.shape[1]
    out_rows = (state_output.shape[0] + window_output.shape[0]) // 4
    f32, bf16 = jnp.float32, jnp.bfloat16
    vmem = pltpu.VMEM
    dma = pltpu.SemaphoreType.DMA
    hbm = pl.BlockSpec(memory_space=pl.ANY)
    chip = pl.BlockSpec(memory_space=pltpu.VMEM)
    scalar = pl.BlockSpec(memory_space=pltpu.SMEM)
    jumps = state_jumps.T
    half = rows // 2
    return pl.pallas_call(
        functools.partial(fused_kernel, count),
        out_shape=jax.ShapeDtypeStruct((half, width), bf16),
        in_specs=[hbm] * 10
        + [chip, chip, scalar, chip, chip, chip, chip, chip, scalar],
        out_specs=chip,
        scratch_shapes=[
            vmem((rows, width), bf16),
            vmem((4, rows, width), bf16),
            vmem((count * depth, 8 * lanes), bf16),
            vmem((count, 4, out_rows, cols), bf16),
            vmem((width, lanes), bf16),
            vmem((rows, lanes), f32),
            vmem((rows, lanes), f32),
            vmem((4,) + jumps.shape, f32),
            vmem((4, rows + 16, 3 * lanes), f32),
            vmem((4, rows, lanes), bf16),
            vmem((4, rows, lanes), f32),
            vmem((4, rows, lanes), f32),
            vmem((4 * blocks, STATE_SIZE, lanes), f32),
            vmem((4 * blocks, STATE_SIZE, lanes), f32),
            vmem((4, rows, lanes), f32),
            vmem((4 * blocks + 4, 8, lanes), f32),
            vmem((4, rows, lanes), bf16),
            vmem((4, STATE_SIZE, lanes), bf16),
            vmem((4, STATE_SIZE, lanes), bf16),
            vmem((4, STATE_SIZE, lanes), bf16),
            vmem((4, STATE_SIZE, lanes), bf16),
            vmem((4, rows + 2 * WINDOW, 2 * HEAD_DIM), bf16),
            vmem((4, rows, 2 * HEAD_DIM), bf16),
            vmem((4, rows, 3 * lanes), bf16),
            vmem((4, rows, 3 * lanes), bf16),
            vmem((count, half, cols), bf16),
            vmem((count, half, cols), bf16),
            vmem((count, half, cols), bf16),
            dma((16,)),
            dma((8 * (count - 1),)),
            dma((8 * (count - 1),)),
            dma((4,)),
            dma((4,)),
            dma((3,)),
            dma((3,)),
            dma((4,)),
            dma((4,)),
            dma((6,)),
            dma((6,)),
            dma((8,)),
            dma((8,)),
            dma((4 * count,)),
            dma((4 * count,)),
            dma((count,)),
            dma((count,)),
        ],
        compiler_params=pltpu.CompilerParams(
            collective_id=0, has_side_effects=True, vmem_limit_bytes=62 * 1024 * 1024
        ),
        name="fused_layer",
    )(
        tokens,
        state_value,
        state_keys,
        state_query,
        state_gate,
        window_keys,
        window_values,
        window_query,
        state_output,
        window_output,
        norm_gain.reshape(1, -1),
        state_step,
        state_rate,
        jumps,
        state_gain.reshape(1, -1),
        filter_value,
        filter_keys,
        filter_query,
        window_sink,
    )


def solution(mesh):
    placed = (
        P(("fs", "sp"), None),
        P(),
        P("sp", "tp"),
        P("sp", "tp"),
        P("sp", "tp"),
        P("sp", "tp"),
        P(),
        P("tp"),
        P(("fs", "sp"), "tp"),
        P("tp"),
        P(None, "tp"),
        P(None, "tp"),
        P(None, "tp"),
        P("sp", "tp"),
        P("sp", "tp"),
        P("sp", "tp"),
        P("tp"),
        P("tp", "sp"),
        P("tp", "sp"),
    )
    def plan(*args):
        return (fused_shards if fits(*args) else shards)(*args)

    return jax.shard_map(
        plan, mesh=mesh, in_specs=placed, out_specs=P(("fs", "sp", "tp"), None), check_vma=False
    )
```

```python
import functools
import math

import jax
import jax.numpy as jnp
from jax import lax
from jax.experimental import pallas as pl
from jax.experimental.pallas import tpu as pltpu
from jax.sharding import PartitionSpec as P

STATE_SIZE = 128
HEAD_DIM = 128
WINDOW = 128
BLOCK = 128
GRID_WIDTH = 64


def extended(cells, sides, width):
    for axis, dim in sides:
        count = lax.axis_size(axis)
        ends = count - 1
        head = lax.slice_in_dim(cells, 0, width, axis=dim)
        tail = lax.slice_in_dim(cells, cells.shape[dim] - width, cells.shape[dim], axis=dim)
        cells = jnp.concatenate(
            [
                lax.ppermute(tail, axis, [(i, (i + 1) % count) for i in range(ends)]),
                cells,
                lax.ppermute(head, axis, [((i + 1) % count, i) for i in range(ends)]),
            ],
            axis=dim,
        )
    return cells


def rotate_grid(vectors, positions, grid_width):
    head_dim = vectors.shape[-1]
    quarter = head_dim // 4
    half_dim = head_dim // 2
    inverse = 10000.0 ** (-jnp.arange(quarter, dtype=jnp.float32) / quarter)
    grid_row = (positions // grid_width).astype(jnp.float32)
    grid_col = (positions % grid_width).astype(jnp.float32)
    angle_row = grid_row[:, None] * inverse[None, :]
    angle_col = grid_col[:, None] * inverse[None, :]
    angles = jnp.concatenate([angle_row, angle_row, angle_col, angle_col], axis=-1)[:, None, :]
    first_half = vectors[..., :half_dim]
    second = vectors[..., half_dim:]
    turned = jnp.concatenate(
        [
            -first_half[..., quarter:],
            first_half[..., :quarter],
            -second[..., quarter:],
            second[..., :quarter],
        ],
        axis=-1,
    )
    return (
        vectors.astype(jnp.float32) * jnp.cos(angles) + turned.astype(jnp.float32) * jnp.sin(angles)
    ).astype(jnp.bfloat16)


def window_attend(query_rows, keys_pad, values_pad, sink_logits, key_start, total_len, window):
    row_count, query_heads, head_dim = query_rows.shape
    kv_heads = keys_pad.shape[1]
    group_size = query_heads // kv_heads
    block_count = row_count // window
    query_blocks = query_rows.reshape(block_count, window, kv_heads, group_size, head_dim)
    key_split = keys_pad.reshape(block_count + 2, window, kv_heads, head_dim)
    value_split = values_pad.reshape(block_count + 2, window, kv_heads, head_dim)
    key_band = jnp.concatenate([key_split[:-2], key_split[1:-1], key_split[2:]], axis=1)
    value_band = jnp.concatenate([value_split[:-2], value_split[1:-1], value_split[2:]], axis=1)
    scores = jnp.einsum(
        "kihgd,kjhd->khgij", query_blocks, key_band, preferred_element_type=jnp.float32
    ) * head_dim ** (-0.5)
    query_pos = jnp.arange(window)[:, None]
    band_pos = jnp.arange(3 * window)[None, :]
    within = jnp.abs(band_pos - window - query_pos) <= window
    key_pos = (
        key_start + jnp.arange(block_count)[:, None] * window + jnp.arange(3 * window)[None, :]
    )
    inside = (key_pos >= 0) & (key_pos < total_len)
    valid_pair = (within[None] & inside[:, None, :])[:, None, None]
    sink_logit = sink_logits.reshape(kv_heads, group_size)[None, :, :, None, None]
    masked = jnp.where(valid_pair, scores, -1e30)
    ceiling = jnp.maximum(jnp.max(masked, axis=-1, keepdims=True), sink_logit)
    weights = jnp.where(valid_pair, jnp.exp(masked - ceiling), 0.0)
    denominator = jnp.exp(sink_logit - ceiling) + jnp.sum(weights, axis=-1, keepdims=True)
    weights_bf = (weights / denominator).astype(jnp.bfloat16)
    mixed_rows = jnp.einsum(
        "khgij,kjhd->kihgd", weights_bf, value_band, preferred_element_type=jnp.float32
    )
    return mixed_rows.reshape(row_count, query_heads * head_dim).astype(jnp.bfloat16)


def block_terms(query_rows, key_rows, value_rows, log_rows, block_len):
    row_count, group_count, state_size = query_rows.shape
    head_ratio, head_dim = (value_rows.shape[2], value_rows.shape[3])
    block_count = row_count // block_len
    query_blocks = query_rows.reshape(block_count, block_len, group_count, state_size)
    key_blocks = key_rows.reshape(block_count, block_len, group_count, state_size)
    value_blocks = value_rows.reshape(block_count, block_len, group_count, head_ratio, head_dim)
    decay_cum = jnp.cumsum(
        log_rows.reshape(block_count, block_len, group_count, head_ratio), axis=1
    )
    decay_total = decay_cum[:, -1]
    gram_block = jnp.einsum(
        "kign,kjgn->kgij", query_blocks, key_blocks, preferred_element_type=jnp.float32
    )
    cum_heads = jnp.moveaxis(decay_cum, 1, 3)
    distance = jnp.abs(cum_heads[..., :, None] - cum_heads[..., None, :])
    pair_weight = (gram_block[:, :, None] * jnp.exp(-distance)).astype(jnp.bfloat16)
    near_terms = jnp.einsum(
        "kgrij,kjgrp->kigrp", pair_weight, value_blocks, preferred_element_type=jnp.float32
    )
    keys_after = (
        key_blocks[:, :, :, None, :] * jnp.exp(decay_total[:, None] - decay_cum)[..., None]
    ).astype(jnp.bfloat16)
    keys_before = (key_blocks[:, :, :, None, :] * jnp.exp(decay_cum)[..., None]).astype(
        jnp.bfloat16
    )
    state_after = jnp.einsum(
        "kjgrn,kjgrp->kgrnp", keys_after, value_blocks, preferred_element_type=jnp.float32
    )
    state_before = jnp.einsum(
        "kjgrn,kjgrp->kgrnp", keys_before, value_blocks, preferred_element_type=jnp.float32
    )
    before = jnp.cumsum(decay_total, axis=0) - decay_total
    overall = jnp.sum(decay_total, axis=0)
    after_sum = overall[None] - before - decay_total
    block_order = jnp.arange(block_count)
    earlier_mask = (block_order[None, :] < block_order[:, None])[:, :, None, None]
    later_mask = (block_order[None, :] > block_order[:, None])[:, :, None, None]
    gap_fwd = before[:, None] - before[None, :] - decay_total[None, :]
    gap_bwd = before[None, :] - before[:, None] - decay_total[:, None]
    weight_fwd = jnp.where(earlier_mask, jnp.exp(jnp.minimum(gap_fwd, 0.0)), 0.0)
    weight_bwd = jnp.where(later_mask, jnp.exp(jnp.minimum(gap_bwd, 0.0)), 0.0)
    carried_fwd = jnp.einsum(
        "abgr,bgrnp->agrnp", weight_fwd, state_after, precision=lax.Precision.HIGHEST
    )
    carried_bwd = jnp.einsum(
        "abgr,bgrnp->agrnp", weight_bwd, state_before, precision=lax.Precision.HIGHEST
    )
    summary_fwd = jnp.einsum(
        "agr,agrnp->grnp", jnp.exp(after_sum), state_after, precision=lax.Precision.HIGHEST
    )
    summary_bwd = jnp.einsum(
        "agr,agrnp->grnp", jnp.exp(before), state_before, precision=lax.Precision.HIGHEST
    )
    pieces = (
        near_terms,
        carried_fwd,
        carried_bwd,
        decay_cum,
        decay_total,
        before,
        after_sum,
        query_blocks,
    )
    return (pieces, (summary_fwd, summary_bwd, overall))


def finish_terms(pieces, incoming_fwd, incoming_bwd):
    (
        near_terms,
        carried_fwd,
        carried_bwd,
        decay_cum,
        decay_total,
        before,
        after_sum,
        query_blocks,
    ) = pieces
    total_fwd = carried_fwd + jnp.exp(before)[..., None, None] * incoming_fwd[None]
    total_bwd = carried_bwd + jnp.exp(after_sum)[..., None, None] * incoming_bwd[None]
    query_wide = query_blocks.astype(jnp.float32)
    read_fwd = jnp.einsum(
        "kign,kgrnp->kigrp", query_wide, total_fwd, precision=lax.Precision.HIGHEST
    )
    read_bwd = jnp.einsum(
        "kign,kgrnp->kigrp", query_wide, total_bwd, precision=lax.Precision.HIGHEST
    )
    combined = (
        near_terms
        + jnp.exp(decay_cum)[..., None] * read_fwd
        + jnp.exp(decay_total[:, None] - decay_cum)[..., None] * read_bwd
    )
    block_count, block_len, group_count, head_ratio, head_dim = combined.shape
    return combined.reshape(block_count * block_len, group_count, head_ratio, head_dim)


def combine_all(gathered_states, own_index):
    after_all, before_all, logs_all = gathered_states
    device_count = logs_all.shape[0]
    cum_incl = jnp.cumsum(logs_all, axis=0)
    cum_excl = cum_incl - logs_all
    device_order = jnp.arange(device_count)
    picker = (device_order == own_index).astype(jnp.float32)[:, None, None]
    own_incl = jnp.sum(picker * cum_incl, axis=0)
    own_excl = jnp.sum(picker * cum_excl, axis=0)
    lower_mask = (device_order < own_index)[:, None, None]
    higher_mask = (device_order > own_index)[:, None, None]
    weight_fwd = jnp.where(lower_mask, jnp.exp(jnp.minimum(own_excl[None] - cum_incl, 0.0)), 0.0)
    weight_bwd = jnp.where(higher_mask, jnp.exp(jnp.minimum(cum_excl - own_incl[None], 0.0)), 0.0)
    incoming_fwd = jnp.einsum(
        "dgr,dgrnp->grnp", weight_fwd, after_all, precision=lax.Precision.HIGHEST
    )
    incoming_bwd = jnp.einsum(
        "dgr,dgrnp->grnp", weight_bwd, before_all, precision=lax.Precision.HIGHEST
    )
    return (incoming_fwd, incoming_bwd)


def shards(
    tokens,
    norm_gain,
    state_gate,
    state_value,
    state_keys,
    state_query,
    state_step,
    state_rate,
    state_jumps,
    state_gain,
    filter_value,
    filter_keys,
    filter_query,
    window_query,
    window_keys,
    window_values,
    window_sink,
    state_output,
    window_output,
):
    row_count = tokens.shape[0]
    rows_wide = tokens.astype(jnp.float32)
    normed = (
        rows_wide
        * lax.rsqrt(jnp.mean(rows_wide * rows_wide, axis=-1, keepdims=True) + 1e-06)
        * norm_gain
    ).astype(jnp.bfloat16)
    gathered = (
        lax.all_gather(state_gate, "sp", axis=0, tiled=True),
        lax.all_gather(state_value, "sp", axis=0, tiled=True),
        lax.all_gather(state_keys, "sp", axis=0, tiled=True),
        lax.all_gather(state_query, "sp", axis=0, tiled=True),
        lax.all_gather(window_query, "sp", axis=0, tiled=True),
        lax.all_gather(window_keys, "sp", axis=0, tiled=True),
        lax.all_gather(window_values, "sp", axis=0, tiled=True),
        lax.all_gather(state_output, "sp", axis=1, tiled=True),
        lax.all_gather(window_output, "sp", axis=1, tiled=True),
    )
    projected = [
        jnp.dot(normed, matrix, preferred_element_type=jnp.float32) for matrix in gathered[:7]
    ]
    out_state = gathered[7]
    out_window = gathered[8]
    gate_rows, value_pre, keys_pre, query_pre, query_raw, keys_raw, values_rows = [
        result.astype(jnp.bfloat16) for result in projected
    ]
    head_local = state_rate.shape[0]
    group_local = keys_pre.shape[1] // STATE_SIZE
    head_dim = value_pre.shape[1] // head_local
    head_ratio = head_local // group_local
    step_cols = lax.dynamic_slice_in_dim(
        state_step, lax.axis_index("tp") * head_local, head_local, 1
    )
    step_rows = jax.nn.softplus(jnp.dot(normed, step_cols, preferred_element_type=jnp.float32))
    log_decay = -state_rate[None, :] * step_rows + state_jumps
    half_width = filter_value.shape[0] // 2
    stacked = jnp.concatenate([value_pre, keys_pre, query_pre], axis=-1)
    padded = extended(stacked, (("sp", 0),), half_width)
    filters = jnp.concatenate([filter_value, filter_keys, filter_query], axis=-1).astype(
        jnp.float32
    )
    filtered = jnp.zeros(stacked.shape, jnp.float32)
    for offset in range(filters.shape[0]):
        filtered = (
            filtered + padded[offset : offset + row_count].astype(jnp.float32) * filters[offset]
        )
    value_cols = value_pre.shape[1]
    key_cols = keys_pre.shape[1]
    inner_rows = (
        jax.nn.silu(filtered[:, :value_cols]).reshape(row_count, head_local, head_dim)
        * step_rows[..., None]
    )
    scan_values = inner_rows.astype(jnp.bfloat16).reshape(
        row_count, group_local, head_ratio, head_dim
    )
    scan_keys = (
        filtered[:, value_cols : value_cols + key_cols]
        .astype(jnp.bfloat16)
        .reshape(row_count, group_local, STATE_SIZE)
    )
    scan_query = (
        filtered[:, value_cols + key_cols :]
        .astype(jnp.bfloat16)
        .reshape(row_count, group_local, STATE_SIZE)
    )
    pieces, summaries = block_terms(
        scan_query,
        scan_keys,
        scan_values,
        log_decay.reshape(row_count, group_local, head_ratio),
        BLOCK,
    )
    summary_fwd, summary_bwd, overall = summaries
    gathered_states = (
        lax.all_gather(summary_fwd[None].astype(jnp.bfloat16), "sp", axis=0, tiled=True).astype(
            jnp.float32
        ),
        lax.all_gather(summary_bwd[None].astype(jnp.bfloat16), "sp", axis=0, tiled=True).astype(
            jnp.float32
        ),
        lax.all_gather(overall[None].astype(jnp.bfloat16), "sp", axis=0, tiled=True).astype(
            jnp.float32
        ),
    )
    incoming_fwd, incoming_bwd = combine_all(gathered_states, lax.axis_index("sp"))
    scan_out = finish_terms(pieces, incoming_fwd, incoming_bwd).reshape(
        row_count, head_local * head_dim
    )
    gated_rows = scan_out * jax.nn.silu(gate_rows.astype(jnp.float32))
    per_head = gated_rows.reshape(row_count, head_local, head_dim)
    state_mix = (
        (
            per_head
            * lax.rsqrt(jnp.mean(per_head * per_head, axis=-1, keepdims=True) + 1e-06)
            * state_gain.reshape(head_local, head_dim)
        )
        .astype(jnp.bfloat16)
        .reshape(row_count, head_local * head_dim)
    )
    query_heads = window_sink.shape[0]
    kv_heads = keys_raw.shape[1] // HEAD_DIM
    kv_width = kv_heads * HEAD_DIM
    positions = lax.axis_index("sp") * row_count + jnp.arange(row_count, dtype=jnp.int32)
    query_rot = rotate_grid(
        query_raw.reshape(row_count, query_heads, HEAD_DIM), positions, GRID_WIDTH
    )
    keys_rot = rotate_grid(keys_raw.reshape(row_count, kv_heads, HEAD_DIM), positions, GRID_WIDTH)
    pair_rows = jnp.concatenate([keys_rot.reshape(row_count, kv_width), values_rows], axis=-1)
    padded_pair = extended(pair_rows, (("sp", 0),), WINDOW)
    keys_pad = padded_pair[:, :kv_width].reshape(-1, kv_heads, HEAD_DIM)
    values_pad = padded_pair[:, kv_width:].reshape(-1, kv_heads, HEAD_DIM)
    window_mix = window_attend(
        query_rot,
        keys_pad,
        values_pad,
        window_sink,
        lax.axis_index("sp") * row_count - WINDOW,
        lax.axis_size("sp") * row_count,
        WINDOW,
    )
    return lax.psum_scatter(
        (
            jnp.dot(state_mix, out_state, preferred_element_type=jnp.float32)
            + jnp.dot(window_mix, out_window, preferred_element_type=jnp.float32)
        ).astype(jnp.bfloat16),
        "tp",
        scatter_dimension=0,
        tiled=True,
    )


def fits(*args):
    tokens, state_value, state_keys, state_rate = args[0], args[3], args[4], args[7]
    window_query, window_keys, window_sink = args[13], args[14], args[16]
    parts = lax.axis_size("fs")
    heads = state_rate.shape[0]
    return (
        parts == 4
        and lax.axis_size("tp") == 2
        and lax.axis_size("sp") > 1
        and tokens.shape[0] % (4 * BLOCK) == 0
        and state_keys.shape[1] == parts * STATE_SIZE
        and state_value.shape[1] == parts * STATE_SIZE
        and heads == 2 * parts
        and window_keys.shape[1] == parts * HEAD_DIM
        and window_query.shape[1] == 2 * parts * HEAD_DIM
        and window_sink.shape[0] == 2 * parts
    )


def fused_kernel(
    count,
    tokens,
    w_value,
    w_keys,
    w_query,
    w_gate,
    w_wkeys,
    w_wvalues,
    w_wquery,
    w_sout,
    w_wout,
    norm_gain,
    step_w,
    rate,
    jumps,
    gain,
    tap_value,
    tap_keys,
    tap_query,
    sink,
    out,
    tbuf,
    xbuf,
    wbuf,
    wob,
    stepw,
    stepx,
    cos_t,
    sin_t,
    jbuf,
    bias,
    acc,
    oacc,
    cbuf,
    gbuf,
    stbuf,
    nbuf,
    sabuf,
    sbbuf,
    cumbuf,
    edge,
    sqbuf,
    fin,
    gin,
    fout,
    gout,
    kvbuf,
    qbuf,
    mixs,
    mixr,
    psend,
    pown,
    precv,
    sums,
    loc_sem,
    z_send,
    z_recv,
    x_send,
    x_recv,
    d_send,
    d_recv,
    j_send,
    j_recv,
    h_send,
    h_recv,
    m_send,
    m_recv,
    o_send,
    o_recv,
    p_send,
    p_recv,
):
    f32, bf16 = jnp.float32, jnp.bfloat16
    me, fs, tp = lax.axis_index("sp"), lax.axis_index("fs"), lax.axis_index("tp")
    rows, width = tokens.shape
    depth = w_value.shape[0]
    half = rows // 2
    quarter = half // 2
    blocks = rows // BLOCK
    lanes = STATE_SIZE
    has = [me > 0, me < count - 1]
    beside = [jnp.maximum(me - 1, 0), jnp.minimum(me + 1, count - 1)]
    peers = [fs, fs + 1 - 2 * (fs % 2), fs + 2 - 4 * (fs // 2), 3 - fs]
    other = 1 - tp

    def to(ref_src, ref_dst, send, recv, axis, index):
        return pltpu.make_async_remote_copy(
            src_ref=ref_src,
            dst_ref=ref_dst,
            send_sem=send,
            recv_sem=recv,
            device_id={axis: index},
            device_id_type=pl.DeviceIdType.MESH,
        )

    own_rows = pl.ds(pl.multiple_of(me * depth, depth), depth)
    loads = [pltpu.make_async_copy(tokens, tbuf, loc_sem.at[0])]
    col = 0
    weight_loads = []
    for index, matrix in enumerate(
        (w_value, w_keys, w_query, w_gate, w_wkeys, w_wvalues, w_wquery)
    ):
        size = matrix.shape[1] // 4
        weight_loads.append(
            pltpu.make_async_copy(
                matrix.at[:, pl.ds(pl.multiple_of(fs * size, size), size)],
                wbuf.at[own_rows, pl.ds(col, size)],
                loc_sem.at[1 + index],
            )
        )
        col += size
    out_loads = []
    first_rows = w_sout.shape[0] // 4
    second_rows = w_wout.shape[0] // 4
    out_rows = first_rows + second_rows
    for part in range(4):
        out_loads.append(
            pltpu.make_async_copy(
                w_sout.at[pl.ds(part * first_rows, first_rows)],
                wob.at[me, part, pl.ds(0, first_rows)],
                loc_sem.at[8 + 2 * part],
            )
        )
        out_loads.append(
            pltpu.make_async_copy(
                w_wout.at[pl.ds(part * second_rows, second_rows)],
                wob.at[me, part, pl.ds(first_rows, second_rows)],
                loc_sem.at[9 + 2 * part],
            )
        )
    step_load = pltpu.make_async_copy(step_w, stepw, loc_sem.at[16])
    for load in weight_loads + loads + [step_load]:
        load.start()

    barrier = pltpu.get_barrier_semaphore()
    for side in range(2):
        pl.when(has[side])(
            lambda side=side: pl.semaphore_signal(
                barrier,
                inc=1,
                device_id={"sp": beside[side]},
                device_id_type=pl.DeviceIdType.MESH,
            )
        )
    for k in range(1, 4):
        pl.semaphore_signal(
            barrier, inc=1, device_id={"fs": peers[k]}, device_id_type=pl.DeviceIdType.MESH
        )
    pl.semaphore_signal(
        barrier, inc=1, device_id={"tp": other}, device_id_type=pl.DeviceIdType.MESH
    )
    pl.semaphore_wait(barrier, 4 + jnp.minimum(me, 1) + jnp.minimum(count - 1 - me, 1))

    spans = ((0, 4 * lanes), (4 * lanes, 2 * lanes), (6 * lanes, 2 * lanes))

    def line(piece, hop, side):
        origin = me - hop if side == 1 else me + hop
        origin = jnp.clip(origin, 0, count - 1)
        if piece == 3:
            ref = wob.at[origin, fs]
        else:
            start, size = spans[piece]
            ref = wbuf.at[pl.ds(pl.multiple_of(origin * depth, depth), depth), pl.ds(start, size)]
        slot = (side * 4 + piece) * (count - 1) + hop
        return to(ref, ref, z_send.at[slot], z_recv.at[slot], "sp", beside[side])

    def valid(hop, side):
        return me >= hop if side == 1 else me + hop <= count - 1

    def send_line(piece, hop):
        for side in range(2):
            pl.when(has[side] & valid(hop, side))(
                lambda side=side: line(piece, hop, side).start()
            )

    def take_line(piece, hop, then=None, mode=None, hold=False):
        for side in range(2):
            wanted = valid(hop, side)
            if mode == "pass":
                wanted = wanted & has[side]
            elif mode == "pass_end":
                wanted = wanted & has[side] & jnp.logical_not(valid(hop + 1, side))
            elif mode == "pass_rest":
                wanted = wanted & has[side] & valid(hop + 1, side)
            elif mode == "keep":
                wanted = wanted & jnp.logical_not(has[side])

            def arrive(side=side):
                line_in(piece, hop, side).wait_recv()
                if hop < count - 1 and not hold:
                    pl.when(has[side])(lambda: line(piece, hop, side).start())
                if then is not None:
                    then(hop, side)

            pl.when(wanted)(arrive)

    def line_in(piece, hop, side):
        origin = me - hop if side == 1 else me + hop
        origin = jnp.clip(origin, 0, count - 1)
        if piece == 3:
            ref = wob.at[origin, fs]
        else:
            start, size = spans[piece]
            ref = wbuf.at[pl.ds(pl.multiple_of(origin * depth, depth), depth), pl.ds(start, size)]
        slot = (side * 4 + piece) * (count - 1) + hop - 1
        return to(ref, ref, z_send.at[slot], z_recv.at[slot], "sp", beside[side])

    for load in weight_loads:
        load.wait()
    send_line(0, 0)
    send_line(1, 0)

    loads[0].wait()
    norm_rows = 32

    def norm(index, base):
        at = pl.ds(pl.multiple_of(base + index * norm_rows, norm_rows), norm_rows)
        wide = tbuf[at, :].astype(f32)
        scale = lax.rsqrt(jnp.mean(wide * wide, axis=-1, keepdims=True) + 1e-06)
        xbuf[fs, at, :] = (wide * scale * norm_gain[...]).astype(bf16)
        return base

    lax.fori_loop(0, half // norm_rows, norm, tp * half)
    lax.fori_loop(0, half // norm_rows, norm, other * half)
    own_half = pl.ds(pl.multiple_of(tp * half, half), half)
    x_own = [
        to(
            xbuf.at[fs, own_half],
            xbuf.at[fs, own_half],
            x_send.at[k - 1],
            x_recv.at[k - 1],
            "fs",
            peers[k],
        )
        for k in (1, 2)
    ]
    for copy in x_own:
        copy.start()
    j_own = [
        to(jumps, jbuf.at[fs], j_send.at[k], j_recv.at[k], "fs", peers[k]) for k in range(1, 4)
    ]
    for copy in j_own:
        copy.start()
    for load in out_loads:
        load.start()
    jbuf[fs, :, :] = jumps[...]

    lane = lax.broadcasted_iota(jnp.int32, (1, lanes), 1)
    low = lane < lanes // 2
    q4 = HEAD_DIM // 4

    def table(index, carry):
        at = pl.ds(pl.multiple_of(index * BLOCK, BLOCK), BLOCK)
        spot = lax.broadcasted_iota(jnp.int32, (BLOCK, lanes), 0) + me * rows + index * BLOCK
        place = jnp.where(low, spot // GRID_WIDTH, spot % GRID_WIDTH).astype(f32)
        inverse = jnp.exp((lane % q4).astype(f32) * (-math.log(10000.0) / q4))
        angle = place * inverse
        cos_t[at, :] = jnp.cos(angle)
        sin_t[at, :] = jnp.where(lane % (2 * q4) < q4, -1.0, 1.0) * jnp.sin(angle)
        return carry

    lax.fori_loop(0, blocks, table, 0)

    def window_bias(index, carry):
        q_id = lax.broadcasted_iota(jnp.int32, (2 * WINDOW, 3 * WINDOW), 0)
        b_id = lax.broadcasted_iota(jnp.int32, (2 * WINDOW, 3 * WINDOW), 1)
        blk = jnp.where(index == 2, blocks - 1, index)
        place = me * rows + (blk - 1) * WINDOW + b_id
        ok = jnp.abs(b_id - WINDOW - q_id % WINDOW) <= WINDOW
        ok = ok & (place >= 0) & (place < count * rows)
        bias[index, :, :] = jnp.where(ok, 0.0, -1e30)
        return carry

    lax.fori_loop(0, 3, window_bias, 0)
    heads_all = step_w.shape[1]
    first_head = (tp * 4 + fs) * 2
    pick = (
        lax.broadcasted_iota(jnp.int32, (heads_all, lanes), 0)
        == first_head + lax.broadcasted_iota(jnp.int32, (heads_all, lanes), 1) // (lanes // 2)
    )
    step_load.wait()
    stepx[...] = jnp.dot(
        stepw[...], pick.astype(f32).astype(bf16), preferred_element_type=f32
    ).astype(bf16)

    take_line(0, 1)
    for load in out_loads:
        load.wait()
    send_line(3, 0)

    x_first = pl.ds(pl.multiple_of(tp * half, quarter), quarter)
    x_second = pl.ds(pl.multiple_of(tp * half + quarter, quarter), quarter)

    def x_in(k, at, slot):
        return to(xbuf.at[peers[k], at], xbuf.at[peers[k], at], x_send.at[slot], x_recv.at[slot], "fs", peers[k])

    relay = [
        to(xbuf.at[peers[1], x_first], xbuf.at[peers[1], x_first], x_send.at[2], x_recv.at[2], "fs", peers[2]),
        to(xbuf.at[peers[2], x_second], xbuf.at[peers[2], x_second], x_send.at[3], x_recv.at[3], "fs", peers[1]),
    ]
    across = [
        to(xbuf.at[peers[k], own_half], xbuf.at[peers[k], own_half], d_send.at[k - 1], d_recv.at[k - 1], "tp", other)
        for k in range(1, 4)
    ]
    for k in (1, 2):
        x_in(k, own_half, k - 1).wait_recv()
        relay[k - 1].start()
        across[k - 1].start()
    if count > 2:
        take_line(0, 2)
    take_line(1, 1)
    inner = has[0] & has[1]

    out_half = out_rows // 2

    def plane(origin, k, at, slot, target):
        ref = wob.at[origin, peers[k]] if at is None else wob.at[origin, peers[k], at]
        slot = origin * 4 + slot
        return to(ref, ref, o_send.at[slot], o_recv.at[slot], "fs", peers[target])

    halves = (pl.ds(0, out_half), pl.ds(out_half, out_half))

    def spread(hop, side):
        origin = jnp.clip(me - hop if side == 1 else me + hop, 0, count - 1)
        plane(origin, 0, None, 1, 1).start()
        plane(origin, 0, None, 2, 2).start()

    def relay_out(hop):
        for side in range(2):

            def work(side=side):
                origin = jnp.clip(me - hop if side == 1 else me + hop, 0, count - 1)
                plane(origin, 1, None, 1, 1).wait_recv()
                plane(origin, 1, halves[0], 3, 2).start()
                plane(origin, 2, None, 2, 2).wait_recv()
                plane(origin, 2, halves[1], 0, 1).start()

            pl.when(valid(hop, side))(work)

    at_top = jnp.where(me == count - 1, 1, 0)
    most = (count - 1) * depth
    most_at = pl.ds(pl.multiple_of(at_top * depth, depth), most)
    last_at = pl.ds(pl.multiple_of((1 - at_top) * most, depth), depth)
    other_half = pl.ds(pl.multiple_of(other * half, half), half)

    def sequence(step):
        return jnp.where(
            step == 0,
            peers[0],
            jnp.where(step == 1, peers[1], jnp.where(step == 2, peers[2], peers[3])),
        )

    def project_most(index, start):
        seq, at = sequence(index // 2), pl.ds(pl.multiple_of((index % 2) * half, half), half)
        acc[seq, at, :] = jnp.dot(
            xbuf[seq, at, most_at], wbuf[most_at, : 4 * lanes], preferred_element_type=f32
        )
        z = jnp.dot(xbuf[seq, at, :], stepx[...], preferred_element_type=f32)
        stbuf[seq, at, :] = jnp.maximum(z, 0.0) + jnp.log1p(jnp.exp(-jnp.abs(z)))
        return start

    def half_in(k):
        ref = xbuf.at[peers[k], other_half]
        to(ref, ref, d_send.at[k - 1], d_recv.at[k - 1], "tp", other).wait_recv()

    half_in(1)
    half_in(2)
    lax.fori_loop(0, 6, project_most, 0)
    x_in(3, x_first, 2).wait_recv()
    x_in(3, x_second, 3).wait_recv()
    across[2].start()
    take_line(3, 1, spread, hold=True)
    half_in(3)
    lax.fori_loop(6, 8, project_most, 0)
    for hop in range(3, count):
        take_line(0, hop)

    def project_state(index, carry):
        seq, at = index // 2, pl.ds(pl.multiple_of((index % 2) * half, half), half)
        y = acc[seq, at, :] + jnp.dot(
            xbuf[seq, at, last_at], wbuf[last_at, : 4 * lanes], preferred_element_type=f32
        )
        to_at = pl.ds(pl.multiple_of((index % 2) * half + 8, 8), half)
        cbuf[seq, to_at, :] = y[:, : 3 * lanes].astype(bf16).astype(f32)
        gbuf[seq, at, :] = y[:, 3 * lanes :].astype(bf16)
        return carry

    lax.fori_loop(0, 8, project_state, 0)
    low_edge, high_edge = pl.ds(0, 8), pl.ds(rows + 8, 8)
    halo = [
        to(cbuf.at[:, pl.ds(8, 8)], cbuf.at[:, high_edge], h_send.at[0], h_recv.at[0], "sp", beside[0]),
        to(cbuf.at[:, pl.ds(rows, 8)], cbuf.at[:, low_edge], h_send.at[1], h_recv.at[1], "sp", beside[1]),
    ]
    halo_in = [
        to(cbuf.at[:, low_edge], cbuf.at[:, low_edge], h_send.at[1], h_recv.at[1], "sp", beside[0]),
        to(cbuf.at[:, high_edge], cbuf.at[:, high_edge], h_send.at[0], h_recv.at[0], "sp", beside[1]),
    ]
    for side in range(2):
        pl.when(has[side])(lambda side=side: halo[side].start())
    edges = (low_edge, high_edge)
    for side in range(2):

        def clear(side=side):
            cbuf[:, edges[side], :] = jnp.zeros((4, 8, 3 * lanes), f32)

        pl.when(jnp.logical_not(has[side]))(clear)
    if count > 2:
        send_line(3, 1)
    for hop in range(2, count - 1):
        take_line(1, hop, mode="pass")
    send_line(2, 0)
    for copy in j_own:
        copy.wait_send()
    for k in range(1, 4):
        to(jumps, jbuf.at[peers[k]], j_send.at[k], j_recv.at[k], "fs", peers[k]).wait_recv()
    for side in range(2):
        pl.when(has[side])(lambda side=side: halo_in[side].wait_recv())

    own_cols = pl.ds(pl.multiple_of(fs * lanes, lanes), lanes)
    taps = jnp.concatenate(
        [ref[:, own_cols].astype(f32) for ref in (tap_value, tap_keys, tap_query)], axis=1
    )
    rate_lane = jnp.where(low, rate[2 * fs], rate[2 * fs + 1])
    row_id = lax.broadcasted_iota(jnp.int32, (BLOCK, lanes), 0)
    col_id = lax.broadcasted_iota(jnp.int32, (BLOCK, lanes), 1)
    lower = (col_id <= row_id).astype(f32)
    left = col_id < lanes // 2
    tap_count = taps.shape[0]
    reach = tap_count // 2
    tall = BLOCK + 16
    high = lax.Precision.HIGHEST

    def scan_block(index):
        seq, blk = index // blocks, index % blocks
        at = pl.ds(pl.multiple_of(blk * BLOCK, BLOCK), BLOCK)
        pre = cbuf[seq, pl.ds(pl.multiple_of(blk * BLOCK, BLOCK), tall), :]
        filt = jnp.zeros((BLOCK, 3 * lanes), f32)
        for tap in range(tap_count):
            moved = pre if tap == reach else pltpu.roll(pre, (reach - tap) % tall, 0)
            filt = filt + moved[8 : 8 + BLOCK] * taps[tap : tap + 1, :]
        fv, fk, fq = filt[:, :lanes], filt[:, lanes : 2 * lanes], filt[:, 2 * lanes :]
        step = stbuf[seq, at, :]
        sv = (fv * jax.nn.sigmoid(fv) * step).astype(bf16)
        sk, sq = fk.astype(bf16), fq.astype(bf16)
        jrows = jbuf[seq, :, at]
        jrow_id = lax.broadcasted_iota(jnp.int32, jrows.shape, 0)
        jrow = [
            jnp.sum(jnp.where(jrow_id == 2 * fs + r, jrows, 0.0), axis=0, keepdims=True)
            for r in range(2)
        ]
        jump = jnp.where(row_id < lanes // 2, jrow[0], jrow[1]).T
        logs = jump - rate_lane * step
        cum = jnp.dot(lower, logs, preferred_element_type=f32, precision=high)
        cum_t = cum.T
        gram = lax.dot_general(sq, sk, (((1,), (1,)), ((), ())), preferred_element_type=f32)
        key_t = sk.astype(f32).T
        near, after, before = [], [], []
        for r in range(2):
            spot = r * (lanes // 2)
            down = cum[:, spot : spot + 1]
            across_row = cum_t[spot : spot + 1, :]
            pair = (gram * jnp.exp(-jnp.abs(down - across_row))).astype(bf16)
            near.append(jnp.dot(pair, sv, preferred_element_type=f32))
            last = across_row[:, BLOCK - 1 : BLOCK]
            k_after = (key_t * jnp.exp(last - across_row)).astype(bf16)
            after.append(jnp.dot(k_after, sv, preferred_element_type=f32))
            k_before = (key_t * jnp.exp(across_row)).astype(bf16)
            before.append(jnp.dot(k_before, sv, preferred_element_type=f32))

        def store():
            sqbuf[seq, at, :] = sq
            cumbuf[seq, at, :] = cum
            nbuf[seq, at, :] = jnp.where(left, near[0], near[1])
            sabuf[index, :, :] = jnp.where(left, after[0], after[1])
            sbbuf[index, :, :] = jnp.where(left, before[0], before[1])

        return store

    def pairs_of(block):
        def body(index, carry):
            for store in [block(2 * index + k) for k in range(2)]:
                store()
            return carry

        return body

    lax.fori_loop(0, 2 * blocks, pairs_of(scan_block), 0)

    relay_out(1)
    for hop in range(2, count - 1):
        take_line(3, hop, spread, hold=True)
    if count > 2:
        take_line(2, 1, mode="pass_end")

    zero_state = jnp.zeros((STATE_SIZE, lanes), f32)

    def total_of(seq, blk):
        return cumbuf[seq, blk * BLOCK + BLOCK - 8 : blk * BLOCK + BLOCK, :][7:8, :]

    def carry_states(seq, carry):
        state, so_far = zero_state, jnp.zeros((1, lanes), f32)
        for blk in range(blocks):
            added = sabuf[seq * blocks + blk, :, :]
            sabuf[seq * blocks + blk, :, :] = state
            edge[seq * blocks + blk, 0:1, :] = so_far
            total = total_of(seq, blk)
            state = state * jnp.exp(total) + added
            so_far = so_far + total
        fout[seq, :, :] = state.astype(bf16)
        edge[4 * blocks + seq, 0:1, :] = so_far
        state, so_far = zero_state, jnp.zeros((1, lanes), f32)
        for blk in range(blocks - 1, -1, -1):
            added = sbbuf[seq * blocks + blk, :, :]
            sbbuf[seq * blocks + blk, :, :] = state
            edge[seq * blocks + blk, 1:2, :] = so_far
            total = total_of(seq, blk)
            state = state * jnp.exp(total) + added
            so_far = so_far + total
        gout[seq, :, :] = state.astype(bf16)
        return carry

    lax.fori_loop(0, 4, carry_states, 0)
    chain = [
        to(gout, gin, h_send.at[2], h_recv.at[2], "sp", beside[0]),
        to(fout, fin, h_send.at[3], h_recv.at[3], "sp", beside[1]),
    ]

    def clear_forward():
        fin[...] = jnp.zeros(fin.shape, bf16)

    def clear_backward():
        gin[...] = jnp.zeros(gin.shape, bf16)

    pl.when(me == 0)(clear_forward)
    pl.when(me == count - 1)(clear_backward)
    pl.when(me == 0)(lambda: chain[1].start())
    pl.when(me == count - 1)(lambda: chain[0].start())

    def rotated(vectors, at):
        lane_full = lax.broadcasted_iota(jnp.int32, vectors.shape, 1)
        turned = jnp.where(
            lane_full % (2 * q4) < q4,
            pltpu.roll(vectors, HEAD_DIM - q4, 1),
            pltpu.roll(vectors, q4, 1),
        )
        return (vectors * cos_t[at, :] + turned * sin_t[at, :]).astype(bf16)

    for hop in range(2, count):
        take_line(1, hop, mode="keep")

    def project_pair(index, carry):
        seq, at = index // 2, pl.ds(pl.multiple_of((index % 2) * half, half), half)
        y = jnp.dot(
            xbuf[seq, at, :], wbuf[:, 4 * lanes : 6 * lanes], preferred_element_type=f32
        ).astype(bf16)
        to_at = pl.ds(pl.multiple_of((index % 2) * half + WINDOW, WINDOW), half)
        kvbuf[seq, to_at, : HEAD_DIM] = rotated(y[:, :HEAD_DIM].astype(f32), at)
        kvbuf[seq, to_at, HEAD_DIM:] = y[:, HEAD_DIM:]
        return carry

    lax.fori_loop(0, 8, project_pair, 0)
    bottom, top = pl.ds(0, WINDOW), pl.ds(rows + WINDOW, WINDOW)
    kv_edge = [
        to(kvbuf.at[:, pl.ds(WINDOW, WINDOW)], kvbuf.at[:, top], h_send.at[4], h_recv.at[4], "sp", beside[0]),
        to(kvbuf.at[:, pl.ds(rows, WINDOW)], kvbuf.at[:, bottom], h_send.at[5], h_recv.at[5], "sp", beside[1]),
    ]
    kv_in = [
        to(kvbuf.at[:, bottom], kvbuf.at[:, bottom], h_send.at[5], h_recv.at[5], "sp", beside[0]),
        to(kvbuf.at[:, top], kvbuf.at[:, top], h_send.at[4], h_recv.at[4], "sp", beside[1]),
    ]
    bands = (bottom, top)
    for side in range(2):

        def clear_band(side=side):
            kvbuf[:, bands[side], :] = jnp.zeros((4, WINDOW, 2 * HEAD_DIM), bf16)

        pl.when(jnp.logical_not(has[side]))(clear_band)

    def forward_step():
        to(fin, fin, h_send.at[3], h_recv.at[3], "sp", beside[0]).wait_recv()

        def add(seq, carry):
            passed = jnp.exp(edge[4 * blocks + seq, 0:1, :])
            fout[seq, :, :] = (
                fout[seq, :, :].astype(f32) + passed * fin[seq, :, :].astype(f32)
            ).astype(bf16)
            return carry

        def pass_on():
            lax.fori_loop(0, 4, add, 0)
            chain[1].start()

        pl.when(has[1])(pass_on)

    def backward_step():
        to(gin, gin, h_send.at[2], h_recv.at[2], "sp", beside[1]).wait_recv()

        def add(seq, carry):
            passed = jnp.exp(edge[4 * blocks + seq, 0:1, :])
            gout[seq, :, :] = (
                gout[seq, :, :].astype(f32) + passed * gin[seq, :, :].astype(f32)
            ).astype(bf16)
            return carry

        def pass_on():
            lax.fori_loop(0, 4, add, 0)
            chain[0].start()

        pl.when(has[0])(pass_on)

    near_first = 2 * me < count
    pl.when(inner & near_first)(forward_step)
    pl.when(inner)(backward_step)
    pl.when(inner & jnp.logical_not(near_first))(forward_step)
    for hop in range(2, count - 1):
        send_line(3, hop)
    if count > 2:
        take_line(2, 1, mode="pass_rest")
    for hop in range(2, count - 1):
        take_line(2, hop, mode="pass")
    for side in range(2):
        pl.when(has[side])(lambda side=side: kv_edge[side].start())
    for hop in range(2, count - 1):
        relay_out(hop)

    state_part, window_part = pl.ds(0, lanes), pl.ds(lanes, 2 * HEAD_DIM)

    spread_rows = (
        pl.ds(0, rows),
        pl.ds(BLOCK, rows - 2 * BLOCK),
        pl.ds(0, BLOCK),
        pl.ds(rows - BLOCK, BLOCK),
    )

    def swap(k, part, slot):
        return to(
            mixs.at[peers[k], spread_rows[slot], part],
            mixr.at[fs, spread_rows[slot], part],
            m_send.at[slot * 4 + k],
            m_recv.at[slot * 4 + k],
            "fs",
            peers[k],
        )

    def swap_in(k, part, slot):
        ref = mixr.at[peers[k], spread_rows[slot], part]
        return to(ref, ref, m_send.at[slot * 4 + k], m_recv.at[slot * 4 + k], "fs", peers[k])

    pl.when(has[0] & jnp.logical_not(has[1]))(forward_step)
    pl.when(has[1] & jnp.logical_not(has[0]))(backward_step)
    gain_row = gain[:, own_cols]

    def split_dot(a, b):
        top_bits = b.astype(bf16)
        rest = (b - top_bits.astype(f32)).astype(bf16)
        return jnp.dot(a, top_bits, preferred_element_type=f32) + jnp.dot(
            a, rest, preferred_element_type=f32
        )

    def finish_block(index):
        seq, blk = index // blocks, index % blocks
        at = pl.ds(pl.multiple_of(blk * BLOCK, BLOCK), BLOCK)
        ahead = sabuf[index, :, :] + jnp.exp(edge[index, 0:1, :]) * fin[seq, :, :].astype(f32)
        behind = sbbuf[index, :, :] + jnp.exp(edge[index, 1:2, :]) * gin[seq, :, :].astype(f32)
        sq = sqbuf[seq, at, :]
        cum = cumbuf[seq, at, :]
        total = cum[BLOCK - 1 : BLOCK, :]
        mixed = (
            nbuf[seq, at, :]
            + jnp.exp(cum) * split_dot(sq, ahead)
            + jnp.exp(total - cum) * split_dot(sq, behind)
        )
        g = gbuf[seq, at, :].astype(f32)
        gated = mixed * (g * jax.nn.sigmoid(g))
        square = gated * gated
        first = jnp.sum(jnp.where(left, square, 0.0), axis=-1, keepdims=True)
        second = jnp.sum(jnp.where(left, 0.0, square), axis=-1, keepdims=True)
        mean = jnp.where(left, first, second) * (2.0 / lanes)
        mix = (gated * lax.rsqrt(mean + 1e-06) * gain_row).astype(bf16)

        def store():
            mixs[seq, at, :lanes] = mix

        return store

    lax.fori_loop(0, 2 * blocks, pairs_of(finish_block), 0)
    for k in (3, 1, 2):
        swap(k, state_part, 0).start()


    if count > 2:
        take_line(3, count - 1, spread)

    def query_most(index, carry):
        seq, at = index // 2, pl.ds(pl.multiple_of((index % 2) * half, half), half)
        acc[seq, at, : 2 * HEAD_DIM] = jnp.dot(
            xbuf[seq, at, most_at], wbuf[most_at, 6 * lanes :], preferred_element_type=f32
        )
        return carry

    for hop in range(1, count - 1):
        take_line(2, hop, mode="keep")
    lax.fori_loop(0, 8, query_most, 0)
    if count > 2:
        relay_out(count - 1)
    take_line(2, count - 1, mode="keep")

    def project_query(index, carry):
        seq, at = index // 2, pl.ds(pl.multiple_of((index % 2) * half, half), half)
        y = acc[seq, at, : 2 * HEAD_DIM] + jnp.dot(
            xbuf[seq, at, last_at], wbuf[last_at, 6 * lanes :], preferred_element_type=f32
        )
        y = y.astype(bf16).astype(f32)
        for r in range(2):
            qbuf[seq, at, r * HEAD_DIM : (r + 1) * HEAD_DIM] = rotated(
                y[:, r * HEAD_DIM : (r + 1) * HEAD_DIM], at
            )
        return carry

    lax.fori_loop(0, 8, project_query, 0)
    band = 3 * WINDOW
    log2e = math.log2(math.e)
    sink_col = log2e * jnp.where(
        lax.broadcasted_iota(jnp.int32, (2 * WINDOW, 1), 0) < WINDOW,
        sink[2 * fs],
        sink[2 * fs + 1],
    )

    def attend_block(seq, blk):
        at = pl.ds(pl.multiple_of(blk * WINDOW, WINDOW), WINDOW)
        wide = pl.ds(pl.multiple_of(blk * WINDOW, WINDOW), band)
        q = jnp.concatenate([qbuf[seq, at, :HEAD_DIM], qbuf[seq, at, HEAD_DIM:]], axis=0)
        s = lax.dot_general(
            q,
            kvbuf[seq, wide, :HEAD_DIM],
            (((1,), (1,)), ((), ())),
            preferred_element_type=f32,
        )
        kind = jnp.where(blk == 0, 0, jnp.where(blk == blocks - 1, 2, 1))
        s = s * (HEAD_DIM ** (-0.5) * log2e) + bias[kind, :, :]
        m = jnp.maximum(jnp.max(s, axis=-1, keepdims=True), sink_col)
        w = jnp.exp2(s - m)
        total = jnp.exp2(sink_col - m) + jnp.sum(w, axis=-1, keepdims=True)
        p = (w * (1.0 / total)).astype(bf16)
        o = jnp.dot(p, kvbuf[seq, wide, HEAD_DIM:], preferred_element_type=f32).astype(bf16)

        def store():
            mixs[seq, at, lanes : lanes + HEAD_DIM] = o[:WINDOW]
            mixs[seq, at, lanes + HEAD_DIM :] = o[WINDOW:]

        return store

    def far_first(step):
        return jnp.where(
            step == 0,
            peers[3],
            jnp.where(step == 1, peers[1], jnp.where(step == 2, peers[2], peers[0])),
        )

    def attend_inner(step, carry):
        seq = far_first(step)

        def body(index, carry):
            for store in [attend_block(seq, 1 + 2 * index + k) for k in range(2)]:
                store()
            return carry

        lax.fori_loop(0, blocks // 2 - 1, body, 0)
        for index, k in enumerate((3, 1, 2)):
            pl.when(step == index)(lambda k=k: swap(k, window_part, 1).start())
        return carry

    lax.fori_loop(0, 4, attend_inner, 0)
    for side in range(2):
        pl.when(has[side])(lambda side=side: kv_in[side].wait_recv())

    def attend_edges(step, carry):
        seq = far_first(step)
        for store in [attend_block(seq, blk) for blk in (0, blocks - 1)]:
            store()
        for index, k in enumerate((3, 1, 2)):

            def send(k=k):
                swap(k, window_part, 2).start()
                swap(k, window_part, 3).start()

            pl.when(step == index)(send)
        return carry

    lax.fori_loop(0, 4, attend_edges, 0)

    cols = w_sout.shape[1]

    def out_in(origin):
        def work():
            plane(origin, 3, halves[0], 3, 2).wait_recv()
            plane(origin, 3, halves[1], 0, 1).wait_recv()

        pl.when(origin != me)(work)

    def trade(origin):
        return to(
            psend.at[origin], precv.at[origin], p_send.at[origin], p_recv.at[origin], "tp", other
        )

    def product(ref, part, origin, at):
        return jnp.dot(ref[part, at, :], wob[origin, part, :, :], preferred_element_type=f32)

    def hand_over(origin, totals):
        psend[origin, :, :] = totals[0].astype(bf16)
        trade(origin).start()
        pown[origin, :, :] = totals[1].astype(bf16)

    row_halves = (other_half, own_half)

    def add_part(ref, part, first=False, last=False):
        def body(index, carry):
            origin = index
            if first:
                out_in(origin)
            totals = [product(ref, part, origin, at) for at in row_halves]
            if not first:
                totals = [x + oacc[origin, at, :] for x, at in zip(totals, row_halves)]
            if last:
                hand_over(origin, totals)
            else:
                for x, at in zip(totals, row_halves):
                    oacc[origin, at, :] = x
            return carry

        lax.fori_loop(0, count, body, 0)

    def store_out(origin):
        return pltpu.make_async_copy(
            sums.at[origin],
            out.at[:, pl.ds(pl.multiple_of(origin * cols, cols), cols)],
            loc_sem.at[17 + origin],
        )

    def finish_out(origin):
        trade(origin).wait_recv()
        sums[origin, :, :] = (
            pown[origin, :, :].astype(f32) + precv[origin, :, :].astype(f32)
        ).astype(bf16)
        store_out(origin).start()

    add_part(mixs, fs, first=True)
    for k in (3, 1, 2):
        swap_in(k, state_part, 0).wait_recv()
        for slot in range(1, 4):
            swap_in(k, window_part, slot).wait_recv()
        add_part(mixr, peers[k], last=k == 2)

    def finish_each(origin, carry):
        finish_out(origin)
        return carry

    lax.fori_loop(0, count, finish_each, 0)
    for origin in range(count):
        store_out(origin).wait()

    for piece in range(4):
        for hop in range(count - 1):
            for side in range(2):
                pl.when(has[side] & valid(hop, side))(
                    lambda piece=piece, hop=hop, side=side: line(piece, hop, side).wait_send()
                )
    for copy in x_own + relay + across:
        copy.wait_send()
    for side in range(2):
        pl.when(has[side])(lambda side=side: halo[side].wait_send())
        pl.when(has[side])(lambda side=side: chain[side].wait_send())
        pl.when(has[side])(lambda side=side: kv_edge[side].wait_send())
    for k in range(1, 4):
        swap(k, state_part, 0).wait_send()
        for slot in range(1, 4):
            swap(k, window_part, slot).wait_send()

    def left_plane(origin, carry):
        def work():
            plane(origin, 0, None, 1, 1).wait_send()
            plane(origin, 0, None, 2, 2).wait_send()
            plane(origin, 1, halves[0], 3, 2).wait_send()
            plane(origin, 2, halves[1], 0, 1).wait_send()

        pl.when(origin != me)(work)
        return carry

    lax.fori_loop(0, count, left_plane, 0)
    for origin in range(count):
        trade(origin).wait_send()


def fused_shards(
    tokens,
    norm_gain,
    state_gate,
    state_value,
    state_keys,
    state_query,
    state_step,
    state_rate,
    state_jumps,
    state_gain,
    filter_value,
    filter_keys,
    filter_query,
    window_query,
    window_keys,
    window_values,
    window_sink,
    state_output,
    window_output,
):
    count = lax.axis_size("sp")
    rows, width = tokens.shape
    lanes = STATE_SIZE
    blocks = rows // BLOCK
    depth = state_value.shape[0]
    cols = state_output.shape[1]
    out_rows = (state_output.shape[0] + window_output.shape[0]) // 4
    f32, bf16 = jnp.float32, jnp.bfloat16
    vmem = pltpu.VMEM
    dma = pltpu.SemaphoreType.DMA
    hbm = pl.BlockSpec(memory_space=pl.ANY)
    chip = pl.BlockSpec(memory_space=pltpu.VMEM)
    scalar = pl.BlockSpec(memory_space=pltpu.SMEM)
    jumps = state_jumps.T
    half = rows // 2
    return pl.pallas_call(
        functools.partial(fused_kernel, count),
        out_shape=jax.ShapeDtypeStruct((half, width), bf16),
        in_specs=[hbm] * 10
        + [chip, hbm, scalar, chip, chip, chip, chip, chip, scalar],
        out_specs=hbm,
        scratch_shapes=[
            vmem((rows, width), bf16),
            vmem((4, rows, width), bf16),
            vmem((count * depth, 8 * lanes), bf16),
            vmem((count, 4, out_rows, cols), bf16),
            vmem(state_step.shape, bf16),
            vmem((width, lanes), bf16),
            vmem((rows, lanes), f32),
            vmem((rows, lanes), f32),
            vmem((4,) + jumps.shape, f32),
            vmem((3, 2 * WINDOW, 3 * WINDOW), f32),
            vmem((4, rows, 4 * lanes), f32),
            vmem((count, rows, cols), f32),
            vmem((4, rows + 16, 3 * lanes), f32),
            vmem((4, rows, lanes), bf16),
            vmem((4, rows, lanes), f32),
            vmem((4, rows, lanes), f32),
            vmem((4 * blocks, STATE_SIZE, lanes), f32),
            vmem((4 * blocks, STATE_SIZE, lanes), f32),
            vmem((4, rows, lanes), f32),
            vmem((4 * blocks + 4, 8, lanes), f32),
            vmem((4, rows, lanes), bf16),
            vmem((4, STATE_SIZE, lanes), bf16),
            vmem((4, STATE_SIZE, lanes), bf16),
            vmem((4, STATE_SIZE, lanes), bf16),
            vmem((4, STATE_SIZE, lanes), bf16),
            vmem((4, rows + 2 * WINDOW, 2 * HEAD_DIM), bf16),
            vmem((4, rows, 2 * HEAD_DIM), bf16),
            vmem((4, rows, 3 * lanes), bf16),
            vmem((4, rows, 3 * lanes), bf16),
            vmem((count, half, cols), bf16),
            vmem((count, half, cols), bf16),
            vmem((count, half, cols), bf16),
            vmem((count, half, cols), bf16),
            dma((17 + count,)),
            dma((8 * (count - 1),)),
            dma((8 * (count - 1),)),
            dma((4,)),
            dma((4,)),
            dma((3,)),
            dma((3,)),
            dma((4,)),
            dma((4,)),
            dma((6,)),
            dma((6,)),
            dma((16,)),
            dma((16,)),
            dma((4 * count,)),
            dma((4 * count,)),
            dma((count,)),
            dma((count,)),
        ],
        compiler_params=pltpu.CompilerParams(
            collective_id=0, has_side_effects=True, vmem_limit_bytes=62 * 1024 * 1024
        ),
        name="fused_layer",
    )(
        tokens,
        state_value,
        state_keys,
        state_query,
        state_gate,
        window_keys,
        window_values,
        window_query,
        state_output,
        window_output,
        norm_gain.reshape(1, -1),
        state_step,
        state_rate,
        jumps,
        state_gain.reshape(1, -1),
        filter_value,
        filter_keys,
        filter_query,
        window_sink,
    )


def solution(mesh):
    placed = (
        P(("fs", "sp"), None),
        P(),
        P("sp", "tp"),
        P("sp", "tp"),
        P("sp", "tp"),
        P("sp", "tp"),
        P(),
        P("tp"),
        P(("fs", "sp"), "tp"),
        P("tp"),
        P(None, "tp"),
        P(None, "tp"),
        P(None, "tp"),
        P("sp", "tp"),
        P("sp", "tp"),
        P("sp", "tp"),
        P("tp"),
        P("tp", "sp"),
        P("tp", "sp"),
    )
    def plan(*args):
        return (fused_shards if fits(*args) else shards)(*args)

    return jax.shard_map(
        plan, mesh=mesh, in_specs=placed, out_specs=P(("fs", "sp", "tp"), None), check_vma=False
    )
```

```python
import functools
import math

import jax
import jax.numpy as jnp
from jax import lax
from jax.experimental import pallas as pl
from jax.experimental.pallas import tpu as pltpu
from jax.sharding import PartitionSpec as P

STATE_SIZE = 128
HEAD_DIM = 128
WINDOW = 128
BLOCK = 128
GRID_WIDTH = 64


def extended(cells, sides, width):
    for axis, dim in sides:
        count = lax.axis_size(axis)
        ends = count - 1
        head = lax.slice_in_dim(cells, 0, width, axis=dim)
        tail = lax.slice_in_dim(cells, cells.shape[dim] - width, cells.shape[dim], axis=dim)
        cells = jnp.concatenate(
            [
                lax.ppermute(tail, axis, [(i, (i + 1) % count) for i in range(ends)]),
                cells,
                lax.ppermute(head, axis, [((i + 1) % count, i) for i in range(ends)]),
            ],
            axis=dim,
        )
    return cells


def rotate_grid(vectors, positions, grid_width):
    head_dim = vectors.shape[-1]
    quarter = head_dim // 4
    half_dim = head_dim // 2
    inverse = 10000.0 ** (-jnp.arange(quarter, dtype=jnp.float32) / quarter)
    grid_row = (positions // grid_width).astype(jnp.float32)
    grid_col = (positions % grid_width).astype(jnp.float32)
    angle_row = grid_row[:, None] * inverse[None, :]
    angle_col = grid_col[:, None] * inverse[None, :]
    angles = jnp.concatenate([angle_row, angle_row, angle_col, angle_col], axis=-1)[:, None, :]
    first_half = vectors[..., :half_dim]
    second = vectors[..., half_dim:]
    turned = jnp.concatenate(
        [
            -first_half[..., quarter:],
            first_half[..., :quarter],
            -second[..., quarter:],
            second[..., :quarter],
        ],
        axis=-1,
    )
    return (
        vectors.astype(jnp.float32) * jnp.cos(angles) + turned.astype(jnp.float32) * jnp.sin(angles)
    ).astype(jnp.bfloat16)


def window_attend(query_rows, keys_pad, values_pad, sink_logits, key_start, total_len, window):
    row_count, query_heads, head_dim = query_rows.shape
    kv_heads = keys_pad.shape[1]
    group_size = query_heads // kv_heads
    block_count = row_count // window
    query_blocks = query_rows.reshape(block_count, window, kv_heads, group_size, head_dim)
    key_split = keys_pad.reshape(block_count + 2, window, kv_heads, head_dim)
    value_split = values_pad.reshape(block_count + 2, window, kv_heads, head_dim)
    key_band = jnp.concatenate([key_split[:-2], key_split[1:-1], key_split[2:]], axis=1)
    value_band = jnp.concatenate([value_split[:-2], value_split[1:-1], value_split[2:]], axis=1)
    scores = jnp.einsum(
        "kihgd,kjhd->khgij", query_blocks, key_band, preferred_element_type=jnp.float32
    ) * head_dim ** (-0.5)
    query_pos = jnp.arange(window)[:, None]
    band_pos = jnp.arange(3 * window)[None, :]
    within = jnp.abs(band_pos - window - query_pos) <= window
    key_pos = (
        key_start + jnp.arange(block_count)[:, None] * window + jnp.arange(3 * window)[None, :]
    )
    inside = (key_pos >= 0) & (key_pos < total_len)
    valid_pair = (within[None] & inside[:, None, :])[:, None, None]
    sink_logit = sink_logits.reshape(kv_heads, group_size)[None, :, :, None, None]
    masked = jnp.where(valid_pair, scores, -1e30)
    ceiling = jnp.maximum(jnp.max(masked, axis=-1, keepdims=True), sink_logit)
    weights = jnp.where(valid_pair, jnp.exp(masked - ceiling), 0.0)
    denominator = jnp.exp(sink_logit - ceiling) + jnp.sum(weights, axis=-1, keepdims=True)
    weights_bf = (weights / denominator).astype(jnp.bfloat16)
    mixed_rows = jnp.einsum(
        "khgij,kjhd->kihgd", weights_bf, value_band, preferred_element_type=jnp.float32
    )
    return mixed_rows.reshape(row_count, query_heads * head_dim).astype(jnp.bfloat16)


def block_terms(query_rows, key_rows, value_rows, log_rows, block_len):
    row_count, group_count, state_size = query_rows.shape
    head_ratio, head_dim = (value_rows.shape[2], value_rows.shape[3])
    block_count = row_count // block_len
    query_blocks = query_rows.reshape(block_count, block_len, group_count, state_size)
    key_blocks = key_rows.reshape(block_count, block_len, group_count, state_size)
    value_blocks = value_rows.reshape(block_count, block_len, group_count, head_ratio, head_dim)
    decay_cum = jnp.cumsum(
        log_rows.reshape(block_count, block_len, group_count, head_ratio), axis=1
    )
    decay_total = decay_cum[:, -1]
    gram_block = jnp.einsum(
        "kign,kjgn->kgij", query_blocks, key_blocks, preferred_element_type=jnp.float32
    )
    cum_heads = jnp.moveaxis(decay_cum, 1, 3)
    distance = jnp.abs(cum_heads[..., :, None] - cum_heads[..., None, :])
    pair_weight = (gram_block[:, :, None] * jnp.exp(-distance)).astype(jnp.bfloat16)
    near_terms = jnp.einsum(
        "kgrij,kjgrp->kigrp", pair_weight, value_blocks, preferred_element_type=jnp.float32
    )
    keys_after = (
        key_blocks[:, :, :, None, :] * jnp.exp(decay_total[:, None] - decay_cum)[..., None]
    ).astype(jnp.bfloat16)
    keys_before = (key_blocks[:, :, :, None, :] * jnp.exp(decay_cum)[..., None]).astype(
        jnp.bfloat16
    )
    state_after = jnp.einsum(
        "kjgrn,kjgrp->kgrnp", keys_after, value_blocks, preferred_element_type=jnp.float32
    )
    state_before = jnp.einsum(
        "kjgrn,kjgrp->kgrnp", keys_before, value_blocks, preferred_element_type=jnp.float32
    )
    before = jnp.cumsum(decay_total, axis=0) - decay_total
    overall = jnp.sum(decay_total, axis=0)
    after_sum = overall[None] - before - decay_total
    block_order = jnp.arange(block_count)
    earlier_mask = (block_order[None, :] < block_order[:, None])[:, :, None, None]
    later_mask = (block_order[None, :] > block_order[:, None])[:, :, None, None]
    gap_fwd = before[:, None] - before[None, :] - decay_total[None, :]
    gap_bwd = before[None, :] - before[:, None] - decay_total[:, None]
    weight_fwd = jnp.where(earlier_mask, jnp.exp(jnp.minimum(gap_fwd, 0.0)), 0.0)
    weight_bwd = jnp.where(later_mask, jnp.exp(jnp.minimum(gap_bwd, 0.0)), 0.0)
    carried_fwd = jnp.einsum(
        "abgr,bgrnp->agrnp", weight_fwd, state_after, precision=lax.Precision.HIGHEST
    )
    carried_bwd = jnp.einsum(
        "abgr,bgrnp->agrnp", weight_bwd, state_before, precision=lax.Precision.HIGHEST
    )
    summary_fwd = jnp.einsum(
        "agr,agrnp->grnp", jnp.exp(after_sum), state_after, precision=lax.Precision.HIGHEST
    )
    summary_bwd = jnp.einsum(
        "agr,agrnp->grnp", jnp.exp(before), state_before, precision=lax.Precision.HIGHEST
    )
    pieces = (
        near_terms,
        carried_fwd,
        carried_bwd,
        decay_cum,
        decay_total,
        before,
        after_sum,
        query_blocks,
    )
    return (pieces, (summary_fwd, summary_bwd, overall))


def finish_terms(pieces, incoming_fwd, incoming_bwd):
    (
        near_terms,
        carried_fwd,
        carried_bwd,
        decay_cum,
        decay_total,
        before,
        after_sum,
        query_blocks,
    ) = pieces
    total_fwd = carried_fwd + jnp.exp(before)[..., None, None] * incoming_fwd[None]
    total_bwd = carried_bwd + jnp.exp(after_sum)[..., None, None] * incoming_bwd[None]
    query_wide = query_blocks.astype(jnp.float32)
    read_fwd = jnp.einsum(
        "kign,kgrnp->kigrp", query_wide, total_fwd, precision=lax.Precision.HIGHEST
    )
    read_bwd = jnp.einsum(
        "kign,kgrnp->kigrp", query_wide, total_bwd, precision=lax.Precision.HIGHEST
    )
    combined = (
        near_terms
        + jnp.exp(decay_cum)[..., None] * read_fwd
        + jnp.exp(decay_total[:, None] - decay_cum)[..., None] * read_bwd
    )
    block_count, block_len, group_count, head_ratio, head_dim = combined.shape
    return combined.reshape(block_count * block_len, group_count, head_ratio, head_dim)


def combine_all(gathered_states, own_index):
    after_all, before_all, logs_all = gathered_states
    device_count = logs_all.shape[0]
    cum_incl = jnp.cumsum(logs_all, axis=0)
    cum_excl = cum_incl - logs_all
    device_order = jnp.arange(device_count)
    picker = (device_order == own_index).astype(jnp.float32)[:, None, None]
    own_incl = jnp.sum(picker * cum_incl, axis=0)
    own_excl = jnp.sum(picker * cum_excl, axis=0)
    lower_mask = (device_order < own_index)[:, None, None]
    higher_mask = (device_order > own_index)[:, None, None]
    weight_fwd = jnp.where(lower_mask, jnp.exp(jnp.minimum(own_excl[None] - cum_incl, 0.0)), 0.0)
    weight_bwd = jnp.where(higher_mask, jnp.exp(jnp.minimum(cum_excl - own_incl[None], 0.0)), 0.0)
    incoming_fwd = jnp.einsum(
        "dgr,dgrnp->grnp", weight_fwd, after_all, precision=lax.Precision.HIGHEST
    )
    incoming_bwd = jnp.einsum(
        "dgr,dgrnp->grnp", weight_bwd, before_all, precision=lax.Precision.HIGHEST
    )
    return (incoming_fwd, incoming_bwd)


def shards(
    tokens,
    norm_gain,
    state_gate,
    state_value,
    state_keys,
    state_query,
    state_step,
    state_rate,
    state_jumps,
    state_gain,
    filter_value,
    filter_keys,
    filter_query,
    window_query,
    window_keys,
    window_values,
    window_sink,
    state_output,
    window_output,
):
    row_count = tokens.shape[0]
    rows_wide = tokens.astype(jnp.float32)
    normed = (
        rows_wide
        * lax.rsqrt(jnp.mean(rows_wide * rows_wide, axis=-1, keepdims=True) + 1e-06)
        * norm_gain
    ).astype(jnp.bfloat16)
    gathered = (
        lax.all_gather(state_gate, "sp", axis=0, tiled=True),
        lax.all_gather(state_value, "sp", axis=0, tiled=True),
        lax.all_gather(state_keys, "sp", axis=0, tiled=True),
        lax.all_gather(state_query, "sp", axis=0, tiled=True),
        lax.all_gather(window_query, "sp", axis=0, tiled=True),
        lax.all_gather(window_keys, "sp", axis=0, tiled=True),
        lax.all_gather(window_values, "sp", axis=0, tiled=True),
        lax.all_gather(state_output, "sp", axis=1, tiled=True),
        lax.all_gather(window_output, "sp", axis=1, tiled=True),
    )
    projected = [
        jnp.dot(normed, matrix, preferred_element_type=jnp.float32) for matrix in gathered[:7]
    ]
    out_state = gathered[7]
    out_window = gathered[8]
    gate_rows, value_pre, keys_pre, query_pre, query_raw, keys_raw, values_rows = [
        result.astype(jnp.bfloat16) for result in projected
    ]
    head_local = state_rate.shape[0]
    group_local = keys_pre.shape[1] // STATE_SIZE
    head_dim = value_pre.shape[1] // head_local
    head_ratio = head_local // group_local
    step_cols = lax.dynamic_slice_in_dim(
        state_step, lax.axis_index("tp") * head_local, head_local, 1
    )
    step_rows = jax.nn.softplus(jnp.dot(normed, step_cols, preferred_element_type=jnp.float32))
    log_decay = -state_rate[None, :] * step_rows + state_jumps
    half_width = filter_value.shape[0] // 2
    stacked = jnp.concatenate([value_pre, keys_pre, query_pre], axis=-1)
    padded = extended(stacked, (("sp", 0),), half_width)
    filters = jnp.concatenate([filter_value, filter_keys, filter_query], axis=-1).astype(
        jnp.float32
    )
    filtered = jnp.zeros(stacked.shape, jnp.float32)
    for offset in range(filters.shape[0]):
        filtered = (
            filtered + padded[offset : offset + row_count].astype(jnp.float32) * filters[offset]
        )
    value_cols = value_pre.shape[1]
    key_cols = keys_pre.shape[1]
    inner_rows = (
        jax.nn.silu(filtered[:, :value_cols]).reshape(row_count, head_local, head_dim)
        * step_rows[..., None]
    )
    scan_values = inner_rows.astype(jnp.bfloat16).reshape(
        row_count, group_local, head_ratio, head_dim
    )
    scan_keys = (
        filtered[:, value_cols : value_cols + key_cols]
        .astype(jnp.bfloat16)
        .reshape(row_count, group_local, STATE_SIZE)
    )
    scan_query = (
        filtered[:, value_cols + key_cols :]
        .astype(jnp.bfloat16)
        .reshape(row_count, group_local, STATE_SIZE)
    )
    pieces, summaries = block_terms(
        scan_query,
        scan_keys,
        scan_values,
        log_decay.reshape(row_count, group_local, head_ratio),
        BLOCK,
    )
    summary_fwd, summary_bwd, overall = summaries
    gathered_states = (
        lax.all_gather(summary_fwd[None].astype(jnp.bfloat16), "sp", axis=0, tiled=True).astype(
            jnp.float32
        ),
        lax.all_gather(summary_bwd[None].astype(jnp.bfloat16), "sp", axis=0, tiled=True).astype(
            jnp.float32
        ),
        lax.all_gather(overall[None].astype(jnp.bfloat16), "sp", axis=0, tiled=True).astype(
            jnp.float32
        ),
    )
    incoming_fwd, incoming_bwd = combine_all(gathered_states, lax.axis_index("sp"))
    scan_out = finish_terms(pieces, incoming_fwd, incoming_bwd).reshape(
        row_count, head_local * head_dim
    )
    gated_rows = scan_out * jax.nn.silu(gate_rows.astype(jnp.float32))
    per_head = gated_rows.reshape(row_count, head_local, head_dim)
    state_mix = (
        (
            per_head
            * lax.rsqrt(jnp.mean(per_head * per_head, axis=-1, keepdims=True) + 1e-06)
            * state_gain.reshape(head_local, head_dim)
        )
        .astype(jnp.bfloat16)
        .reshape(row_count, head_local * head_dim)
    )
    query_heads = window_sink.shape[0]
    kv_heads = keys_raw.shape[1] // HEAD_DIM
    kv_width = kv_heads * HEAD_DIM
    positions = lax.axis_index("sp") * row_count + jnp.arange(row_count, dtype=jnp.int32)
    query_rot = rotate_grid(
        query_raw.reshape(row_count, query_heads, HEAD_DIM), positions, GRID_WIDTH
    )
    keys_rot = rotate_grid(keys_raw.reshape(row_count, kv_heads, HEAD_DIM), positions, GRID_WIDTH)
    pair_rows = jnp.concatenate([keys_rot.reshape(row_count, kv_width), values_rows], axis=-1)
    padded_pair = extended(pair_rows, (("sp", 0),), WINDOW)
    keys_pad = padded_pair[:, :kv_width].reshape(-1, kv_heads, HEAD_DIM)
    values_pad = padded_pair[:, kv_width:].reshape(-1, kv_heads, HEAD_DIM)
    window_mix = window_attend(
        query_rot,
        keys_pad,
        values_pad,
        window_sink,
        lax.axis_index("sp") * row_count - WINDOW,
        lax.axis_size("sp") * row_count,
        WINDOW,
    )
    return lax.psum_scatter(
        (
            jnp.dot(state_mix, out_state, preferred_element_type=jnp.float32)
            + jnp.dot(window_mix, out_window, preferred_element_type=jnp.float32)
        ).astype(jnp.bfloat16),
        "tp",
        scatter_dimension=0,
        tiled=True,
    )


def fits(*args):
    tokens, state_value, state_keys, state_rate = args[0], args[3], args[4], args[7]
    window_query, window_keys, window_sink = args[13], args[14], args[16]
    parts = lax.axis_size("fs")
    heads = state_rate.shape[0]
    return (
        parts == 4
        and lax.axis_size("tp") == 2
        and lax.axis_size("sp") > 1
        and tokens.shape[0] % (4 * BLOCK) == 0
        and state_keys.shape[1] == parts * STATE_SIZE
        and state_value.shape[1] == parts * STATE_SIZE
        and heads == 2 * parts
        and window_keys.shape[1] == parts * HEAD_DIM
        and window_query.shape[1] == 2 * parts * HEAD_DIM
        and window_sink.shape[0] == 2 * parts
    )


def fused_kernel(
    count,
    tokens,
    w_value,
    w_keys,
    w_query,
    w_gate,
    w_wkeys,
    w_wvalues,
    w_wquery,
    w_sout,
    w_wout,
    norm_gain,
    step_w,
    rate,
    jumps,
    gain,
    tap_value,
    tap_keys,
    tap_query,
    sink,
    out,
    tbuf,
    xbuf,
    wbuf,
    wob,
    stepw,
    stepx,
    cos_t,
    sin_t,
    jbuf,
    bias,
    acc,
    oacc,
    cbuf,
    gbuf,
    stbuf,
    nbuf,
    sabuf,
    sbbuf,
    cumbuf,
    edge,
    sqbuf,
    fin,
    gin,
    fout,
    gout,
    kvbuf,
    qbuf,
    mixs,
    mixr,
    psend,
    pown,
    precv,
    sums,
    loc_sem,
    z_send,
    z_recv,
    x_send,
    x_recv,
    d_send,
    d_recv,
    j_send,
    j_recv,
    h_send,
    h_recv,
    m_send,
    m_recv,
    o_send,
    o_recv,
    p_send,
    p_recv,
):
    f32, bf16 = jnp.float32, jnp.bfloat16
    me, fs, tp = lax.axis_index("sp"), lax.axis_index("fs"), lax.axis_index("tp")
    rows, width = tokens.shape
    depth = w_value.shape[0]
    half = rows // 2
    quarter = half // 2
    blocks = rows // BLOCK
    lanes = STATE_SIZE
    has = [me > 0, me < count - 1]
    beside = [jnp.maximum(me - 1, 0), jnp.minimum(me + 1, count - 1)]
    peers = [fs, fs + 1 - 2 * (fs % 2), fs + 2 - 4 * (fs // 2), 3 - fs]
    other = 1 - tp

    def to(ref_src, ref_dst, send, recv, axis, index):
        return pltpu.make_async_remote_copy(
            src_ref=ref_src,
            dst_ref=ref_dst,
            send_sem=send,
            recv_sem=recv,
            device_id={axis: index},
            device_id_type=pl.DeviceIdType.MESH,
        )

    own_rows = pl.ds(pl.multiple_of(me * depth, depth), depth)
    loads = [pltpu.make_async_copy(tokens, tbuf, loc_sem.at[0])]
    col = 0
    weight_loads = []
    for index, matrix in enumerate(
        (w_value, w_keys, w_query, w_gate, w_wkeys, w_wvalues, w_wquery)
    ):
        size = matrix.shape[1] // 4
        weight_loads.append(
            pltpu.make_async_copy(
                matrix.at[:, pl.ds(pl.multiple_of(fs * size, size), size)],
                wbuf.at[own_rows, pl.ds(col, size)],
                loc_sem.at[1 + index],
            )
        )
        col += size
    out_loads = []
    first_rows = w_sout.shape[0] // 4
    second_rows = w_wout.shape[0] // 4
    out_rows = first_rows + second_rows
    for part in range(4):
        out_loads.append(
            pltpu.make_async_copy(
                w_sout.at[pl.ds(part * first_rows, first_rows)],
                wob.at[me, part, pl.ds(0, first_rows)],
                loc_sem.at[8 + 2 * part],
            )
        )
        out_loads.append(
            pltpu.make_async_copy(
                w_wout.at[pl.ds(part * second_rows, second_rows)],
                wob.at[me, part, pl.ds(first_rows, second_rows)],
                loc_sem.at[9 + 2 * part],
            )
        )
    step_load = pltpu.make_async_copy(step_w, stepw, loc_sem.at[16])
    for load in weight_loads + loads + [step_load]:
        load.start()

    barrier = pltpu.get_barrier_semaphore()
    for side in range(2):
        pl.when(has[side])(
            lambda side=side: pl.semaphore_signal(
                barrier,
                inc=1,
                device_id={"sp": beside[side]},
                device_id_type=pl.DeviceIdType.MESH,
            )
        )
    for k in range(1, 4):
        pl.semaphore_signal(
            barrier, inc=1, device_id={"fs": peers[k]}, device_id_type=pl.DeviceIdType.MESH
        )
    pl.semaphore_signal(
        barrier, inc=1, device_id={"tp": other}, device_id_type=pl.DeviceIdType.MESH
    )
    pl.semaphore_wait(barrier, 4 + jnp.minimum(me, 1) + jnp.minimum(count - 1 - me, 1))

    spans = {
        0: (0, 4 * lanes),
        1: (4 * lanes, 2 * lanes),
        2: (6 * lanes, lanes),
        4: (7 * lanes, lanes),
    }
    pieces = 5

    def line(piece, hop, side):
        origin = me - hop if side == 1 else me + hop
        origin = jnp.clip(origin, 0, count - 1)
        if piece == 3:
            ref = wob.at[origin, fs]
        else:
            start, size = spans[piece]
            ref = wbuf.at[pl.ds(pl.multiple_of(origin * depth, depth), depth), pl.ds(start, size)]
        slot = (side * pieces + piece) * (count - 1) + hop
        return to(ref, ref, z_send.at[slot], z_recv.at[slot], "sp", beside[side])

    def valid(hop, side):
        return me >= hop if side == 1 else me + hop <= count - 1

    def send_line(piece, hop, where=True):
        for side in range(2):
            pl.when(has[side] & valid(hop, side) & where)(
                lambda side=side: line(piece, hop, side).start()
            )

    def take_line(piece, hop, then=None, mode=None, hold=False):
        for side in range(2):
            wanted = valid(hop, side)
            if mode == "pass":
                wanted = wanted & has[side]
            elif mode == "pass_end":
                wanted = wanted & has[side] & jnp.logical_not(valid(hop + 1, side))
            elif mode == "pass_rest":
                wanted = wanted & has[side] & valid(hop + 1, side)
            elif mode == "keep":
                wanted = wanted & jnp.logical_not(has[side])

            def arrive(side=side):
                line_in(piece, hop, side).wait_recv()
                if hop < count - 1 and not hold:
                    pl.when(has[side])(lambda: line(piece, hop, side).start())
                if then is not None:
                    then(hop, side)

            pl.when(wanted)(arrive)

    def line_in(piece, hop, side):
        origin = me - hop if side == 1 else me + hop
        origin = jnp.clip(origin, 0, count - 1)
        if piece == 3:
            ref = wob.at[origin, fs]
        else:
            start, size = spans[piece]
            ref = wbuf.at[pl.ds(pl.multiple_of(origin * depth, depth), depth), pl.ds(start, size)]
        slot = (side * pieces + piece) * (count - 1) + hop - 1
        return to(ref, ref, z_send.at[slot], z_recv.at[slot], "sp", beside[side])

    for load in weight_loads:
        load.wait()
    send_line(0, 0)
    send_line(1, 0)

    loads[0].wait()
    norm_rows = 32

    def norm(index, base):
        at = pl.ds(pl.multiple_of(base + index * norm_rows, norm_rows), norm_rows)
        wide = tbuf[at, :].astype(f32)
        scale = lax.rsqrt(jnp.mean(wide * wide, axis=-1, keepdims=True) + 1e-06)
        xbuf[fs, at, :] = (wide * scale * norm_gain[...]).astype(bf16)
        return base

    lax.fori_loop(0, half // norm_rows, norm, tp * half)
    lax.fori_loop(0, half // norm_rows, norm, other * half)
    own_half = pl.ds(pl.multiple_of(tp * half, half), half)
    x_own = [
        to(
            xbuf.at[fs, own_half],
            xbuf.at[fs, own_half],
            x_send.at[k - 1],
            x_recv.at[k - 1],
            "fs",
            peers[k],
        )
        for k in (1, 2)
    ]
    for copy in x_own:
        copy.start()
    j_own = [
        to(jumps, jbuf.at[fs], j_send.at[k], j_recv.at[k], "fs", peers[k]) for k in range(1, 4)
    ]
    for copy in j_own:
        copy.start()
    for load in out_loads:
        load.start()
    jbuf[fs, :, :] = jumps[...]

    lane = lax.broadcasted_iota(jnp.int32, (1, lanes), 1)
    low = lane < lanes // 2
    q4 = HEAD_DIM // 4

    def table(index, carry):
        at = pl.ds(pl.multiple_of(index * BLOCK, BLOCK), BLOCK)
        spot = lax.broadcasted_iota(jnp.int32, (BLOCK, lanes), 0) + me * rows + index * BLOCK
        place = jnp.where(low, spot // GRID_WIDTH, spot % GRID_WIDTH).astype(f32)
        inverse = jnp.exp((lane % q4).astype(f32) * (-math.log(10000.0) / q4))
        angle = place * inverse
        cos_t[at, :] = jnp.cos(angle)
        sin_t[at, :] = jnp.where(lane % (2 * q4) < q4, -1.0, 1.0) * jnp.sin(angle)
        return carry

    lax.fori_loop(0, blocks, table, 0)

    def window_bias(index, carry):
        q_id = lax.broadcasted_iota(jnp.int32, (2 * WINDOW, 3 * WINDOW), 0)
        b_id = lax.broadcasted_iota(jnp.int32, (2 * WINDOW, 3 * WINDOW), 1)
        blk = jnp.where(index == 2, blocks - 1, index)
        place = me * rows + (blk - 1) * WINDOW + b_id
        ok = jnp.abs(b_id - WINDOW - q_id % WINDOW) <= WINDOW
        ok = ok & (place >= 0) & (place < count * rows)
        bias[index, :, :] = jnp.where(ok, 0.0, -1e30)
        return carry

    lax.fori_loop(0, 3, window_bias, 0)
    kvbuf[:, :, 2 * HEAD_DIM :] = jnp.ones((4, rows + 2 * WINDOW, HEAD_DIM), bf16)
    heads_all = step_w.shape[0]
    first_head = (tp * 4 + fs) * 2
    pick = (
        lax.broadcasted_iota(jnp.int32, (lanes, heads_all), 1)
        == first_head + lax.broadcasted_iota(jnp.int32, (lanes, heads_all), 0) // (lanes // 2)
    )
    step_load.wait()
    stepx[...] = jnp.dot(
        pick.astype(f32).astype(bf16), stepw[...], preferred_element_type=f32
    ).astype(bf16)

    take_line(0, 1)
    for load in out_loads:
        load.wait()
    send_line(3, 0)

    x_first = pl.ds(pl.multiple_of(tp * half, quarter), quarter)
    x_second = pl.ds(pl.multiple_of(tp * half + quarter, quarter), quarter)

    def x_in(k, at, slot):
        return to(xbuf.at[peers[k], at], xbuf.at[peers[k], at], x_send.at[slot], x_recv.at[slot], "fs", peers[k])

    relay = [
        to(xbuf.at[peers[1], x_first], xbuf.at[peers[1], x_first], x_send.at[2], x_recv.at[2], "fs", peers[2]),
        to(xbuf.at[peers[2], x_second], xbuf.at[peers[2], x_second], x_send.at[3], x_recv.at[3], "fs", peers[1]),
    ]
    across = [
        to(xbuf.at[peers[k], own_half], xbuf.at[peers[k], own_half], d_send.at[k - 1], d_recv.at[k - 1], "tp", other)
        for k in range(1, 4)
    ]
    for k in (1, 2):
        x_in(k, own_half, k - 1).wait_recv()
        relay[k - 1].start()
        across[k - 1].start()
    if count > 2:
        take_line(0, 2)
    take_line(1, 1)
    inner = has[0] & has[1]

    out_half = out_rows // 2

    def plane(origin, k, at, slot, target):
        ref = wob.at[origin, peers[k]] if at is None else wob.at[origin, peers[k], at]
        slot = origin * 4 + slot
        return to(ref, ref, o_send.at[slot], o_recv.at[slot], "fs", peers[target])

    halves = (pl.ds(0, out_half), pl.ds(out_half, out_half))

    def spread(hop, side):
        origin = jnp.clip(me - hop if side == 1 else me + hop, 0, count - 1)
        plane(origin, 0, None, 1, 1).start()
        plane(origin, 0, None, 2, 2).start()

    def relay_out(hop):
        for side in range(2):

            def work(side=side):
                origin = jnp.clip(me - hop if side == 1 else me + hop, 0, count - 1)
                plane(origin, 1, None, 1, 1).wait_recv()
                plane(origin, 1, halves[0], 3, 2).start()
                plane(origin, 2, None, 2, 2).wait_recv()
                plane(origin, 2, halves[1], 0, 1).start()

            pl.when(valid(hop, side))(work)

    at_top = jnp.where(me == count - 1, 1, 0)
    most = (count - 1) * depth
    most_at = pl.ds(pl.multiple_of(at_top * depth, depth), most)
    last_at = pl.ds(pl.multiple_of((1 - at_top) * most, depth), depth)
    other_half = pl.ds(pl.multiple_of(other * half, half), half)

    def sequence(step):
        return jnp.where(
            step == 0,
            peers[0],
            jnp.where(step == 1, peers[1], jnp.where(step == 2, peers[2], peers[3])),
        )

    def project_most(index, start):
        seq, at = sequence(index // 2), pl.ds(pl.multiple_of((index % 2) * half, half), half)
        acc[seq, at, :] = jnp.dot(
            xbuf[seq, at, most_at], wbuf[most_at, : 4 * lanes], preferred_element_type=f32
        )
        z = lax.dot_general(
            xbuf[seq, at, :], stepx[...], (((1,), (1,)), ((), ())), preferred_element_type=f32
        )
        stbuf[seq, at, :] = jnp.maximum(z, 0.0) + jnp.log1p(jnp.exp(-jnp.abs(z)))
        return start

    def half_in(k):
        ref = xbuf.at[peers[k], other_half]
        to(ref, ref, d_send.at[k - 1], d_recv.at[k - 1], "tp", other).wait_recv()

    half_in(1)
    half_in(2)
    lax.fori_loop(0, 6, project_most, 0)
    x_in(3, x_first, 2).wait_recv()
    x_in(3, x_second, 3).wait_recv()
    across[2].start()
    take_line(3, 1, spread, hold=True)
    half_in(3)
    lax.fori_loop(6, 8, project_most, 0)
    for hop in range(3, count):
        take_line(0, hop)

    def project_state(index, carry):
        seq, at = index // 2, pl.ds(pl.multiple_of((index % 2) * half, half), half)
        y = acc[seq, at, :] + jnp.dot(
            xbuf[seq, at, last_at], wbuf[last_at, : 4 * lanes], preferred_element_type=f32
        )
        to_at = pl.ds(pl.multiple_of((index % 2) * half + 8, 8), half)
        cbuf[seq, to_at, :] = y[:, : 3 * lanes].astype(bf16).astype(f32)
        gbuf[seq, at, :] = y[:, 3 * lanes :].astype(bf16)
        return carry

    lax.fori_loop(0, 8, project_state, 0)
    low_edge, high_edge = pl.ds(0, 8), pl.ds(rows + 8, 8)
    halo = [
        to(cbuf.at[:, pl.ds(8, 8)], cbuf.at[:, high_edge], h_send.at[0], h_recv.at[0], "sp", beside[0]),
        to(cbuf.at[:, pl.ds(rows, 8)], cbuf.at[:, low_edge], h_send.at[1], h_recv.at[1], "sp", beside[1]),
    ]
    halo_in = [
        to(cbuf.at[:, low_edge], cbuf.at[:, low_edge], h_send.at[1], h_recv.at[1], "sp", beside[0]),
        to(cbuf.at[:, high_edge], cbuf.at[:, high_edge], h_send.at[0], h_recv.at[0], "sp", beside[1]),
    ]
    for side in range(2):
        pl.when(has[side])(lambda side=side: halo[side].start())
    edges = (low_edge, high_edge)
    for side in range(2):

        def clear(side=side):
            cbuf[:, edges[side], :] = jnp.zeros((4, 8, 3 * lanes), f32)

        pl.when(jnp.logical_not(has[side]))(clear)
    if count > 2:
        send_line(3, 1)
    for hop in range(2, count - 1):
        take_line(1, hop, mode="pass")
    send_line(2, 0, jnp.logical_not(inner))
    send_line(4, 0, jnp.logical_not(inner))
    for copy in j_own:
        copy.wait_send()
    for k in range(1, 4):
        to(jumps, jbuf.at[peers[k]], j_send.at[k], j_recv.at[k], "fs", peers[k]).wait_recv()
    for side in range(2):
        pl.when(has[side])(lambda side=side: halo_in[side].wait_recv())

    own_cols = pl.ds(pl.multiple_of(fs * lanes, lanes), lanes)
    taps = jnp.concatenate(
        [ref[:, own_cols].astype(f32) for ref in (tap_value, tap_keys, tap_query)], axis=1
    )
    rate_lane = jnp.where(low, rate[2 * fs], rate[2 * fs + 1])
    row_id = lax.broadcasted_iota(jnp.int32, (BLOCK, lanes), 0)
    col_id = lax.broadcasted_iota(jnp.int32, (BLOCK, lanes), 1)
    lower = (col_id <= row_id).astype(f32)
    left = col_id < lanes // 2
    tap_count = taps.shape[0]
    reach = tap_count // 2
    tall = BLOCK + 16
    high = lax.Precision.HIGHEST

    def scan_block(index):
        seq, blk = index // blocks, index % blocks
        at = pl.ds(pl.multiple_of(blk * BLOCK, BLOCK), BLOCK)
        pre = cbuf[seq, pl.ds(pl.multiple_of(blk * BLOCK, BLOCK), tall), :]
        filt = jnp.zeros((BLOCK, 3 * lanes), f32)
        for tap in range(tap_count):
            moved = pre if tap == reach else pltpu.roll(pre, (reach - tap) % tall, 0)
            filt = filt + moved[8 : 8 + BLOCK] * taps[tap : tap + 1, :]
        fv, fk, fq = filt[:, :lanes], filt[:, lanes : 2 * lanes], filt[:, 2 * lanes :]
        step = stbuf[seq, at, :]
        sv = (fv * jax.nn.sigmoid(fv) * step).astype(bf16)
        sk, sq = fk.astype(bf16), fq.astype(bf16)
        jrows = jbuf[seq, :, at]
        jrow_id = lax.broadcasted_iota(jnp.int32, jrows.shape, 0)
        jrow = [
            jnp.sum(jnp.where(jrow_id == 2 * fs + r, jrows, 0.0), axis=0, keepdims=True)
            for r in range(2)
        ]
        jump = jnp.where(row_id < lanes // 2, jrow[0], jrow[1]).T
        logs = jump - rate_lane * step
        cum = jnp.dot(lower, logs, preferred_element_type=f32, precision=high)
        cum_t = cum.T
        gram = lax.dot_general(sq, sk, (((1,), (1,)), ((), ())), preferred_element_type=f32)
        key_t = sk.astype(f32).T
        near, after, before = [], [], []
        for r in range(2):
            spot = r * (lanes // 2)
            down = cum[:, spot : spot + 1]
            across_row = cum_t[spot : spot + 1, :]
            pair = (gram * jnp.exp(-jnp.abs(down - across_row))).astype(bf16)
            near.append(jnp.dot(pair, sv, preferred_element_type=f32))
            last = across_row[:, BLOCK - 1 : BLOCK]
            k_after = (key_t * jnp.exp(last - across_row)).astype(bf16)
            after.append(jnp.dot(k_after, sv, preferred_element_type=f32))
            k_before = (key_t * jnp.exp(across_row)).astype(bf16)
            before.append(jnp.dot(k_before, sv, preferred_element_type=f32))

        def store():
            sqbuf[seq, at, :] = sq
            cumbuf[seq, at, :] = cum
            nbuf[seq, at, :] = jnp.where(left, near[0], near[1])
            sabuf[index, :, :] = jnp.where(left, after[0], after[1])
            sbbuf[index, :, :] = jnp.where(left, before[0], before[1])

        return store

    def pairs_of(block):
        def body(index, carry):
            for store in [block(2 * index + k) for k in range(2)]:
                store()
            return carry

        return body

    lax.fori_loop(0, 2 * blocks, pairs_of(scan_block), 0)

    relay_out(1)
    for hop in range(2, count - 1):
        take_line(3, hop, spread)
    if count > 2:
        take_line(2, 1, mode="pass_end")
        take_line(4, 1, mode="pass_end")

    zero_state = jnp.zeros((STATE_SIZE, lanes), f32)

    def total_of(seq, blk):
        return cumbuf[seq, blk * BLOCK + BLOCK - 8 : blk * BLOCK + BLOCK, :][7:8, :]

    def carry_states(seq, carry):
        state, so_far = zero_state, jnp.zeros((1, lanes), f32)
        for blk in range(blocks):
            added = sabuf[seq * blocks + blk, :, :]
            sabuf[seq * blocks + blk, :, :] = state
            edge[seq * blocks + blk, 0:1, :] = so_far
            total = total_of(seq, blk)
            state = state * jnp.exp(total) + added
            so_far = so_far + total
        fout[seq, :, :] = state.astype(bf16)
        edge[4 * blocks + seq, 0:1, :] = so_far
        state, so_far = zero_state, jnp.zeros((1, lanes), f32)
        for blk in range(blocks - 1, -1, -1):
            added = sbbuf[seq * blocks + blk, :, :]
            sbbuf[seq * blocks + blk, :, :] = state
            edge[seq * blocks + blk, 1:2, :] = so_far
            total = total_of(seq, blk)
            state = state * jnp.exp(total) + added
            so_far = so_far + total
        gout[seq, :, :] = state.astype(bf16)
        return carry

    lax.fori_loop(0, 4, carry_states, 0)
    chain = [
        to(gout, gin, h_send.at[2], h_recv.at[2], "sp", beside[0]),
        to(fout, fin, h_send.at[3], h_recv.at[3], "sp", beside[1]),
    ]

    def clear_forward():
        fin[...] = jnp.zeros(fin.shape, bf16)

    def clear_backward():
        gin[...] = jnp.zeros(gin.shape, bf16)

    pl.when(me == 0)(clear_forward)
    pl.when(me == count - 1)(clear_backward)
    pl.when(me == 0)(lambda: chain[1].start())
    pl.when(me == count - 1)(lambda: chain[0].start())

    def rotated(vectors):
        lane_full = lax.broadcasted_iota(jnp.int32, vectors.shape, 1)
        turned = jnp.where(
            lane_full % (2 * q4) < q4,
            pltpu.roll(vectors, HEAD_DIM - q4, 1),
            pltpu.roll(vectors, q4, 1),
        )
        return (vectors * cos_t[...] + turned * sin_t[...]).astype(bf16)

    for hop in range(2, count):
        take_line(1, hop, mode="keep")

    def project_pair(seq, carry):
        y = jnp.dot(
            xbuf[seq, :, :], wbuf[:, 4 * lanes : 6 * lanes], preferred_element_type=f32
        ).astype(bf16)
        kvbuf[seq, WINDOW : WINDOW + rows, :HEAD_DIM] = rotated(y[:, :HEAD_DIM].astype(f32))
        kvbuf[seq, WINDOW : WINDOW + rows, HEAD_DIM : 2 * HEAD_DIM] = y[:, HEAD_DIM:]
        return carry

    lax.fori_loop(0, 4, project_pair, 0)
    bottom, top = pl.ds(0, WINDOW), pl.ds(rows + WINDOW, WINDOW)
    pair_cols = pl.ds(0, 2 * HEAD_DIM)

    def kv(at):
        return kvbuf.at[:, at, pair_cols]

    low_rows, high_rows = pl.ds(WINDOW, WINDOW), pl.ds(rows, WINDOW)
    kv_edge = [
        to(kv(low_rows), kv(top), h_send.at[4], h_recv.at[4], "sp", beside[0]),
        to(kv(high_rows), kv(bottom), h_send.at[5], h_recv.at[5], "sp", beside[1]),
    ]
    kv_in = [
        to(kv(bottom), kv(bottom), h_send.at[5], h_recv.at[5], "sp", beside[0]),
        to(kv(top), kv(top), h_send.at[4], h_recv.at[4], "sp", beside[1]),
    ]
    bands = (bottom, top)
    for side in range(2):

        def clear_band(side=side):
            kvbuf[:, bands[side], : 2 * HEAD_DIM] = jnp.zeros((4, WINDOW, 2 * HEAD_DIM), bf16)

        pl.when(jnp.logical_not(has[side]))(clear_band)

    def forward_step():
        to(fin, fin, h_send.at[3], h_recv.at[3], "sp", beside[0]).wait_recv()

        def add(seq, carry):
            passed = jnp.exp(edge[4 * blocks + seq, 0:1, :])
            fout[seq, :, :] = (
                fout[seq, :, :].astype(f32) + passed * fin[seq, :, :].astype(f32)
            ).astype(bf16)
            return carry

        def pass_on():
            lax.fori_loop(0, 4, add, 0)
            chain[1].start()

        pl.when(has[1])(pass_on)

    def backward_step():
        to(gin, gin, h_send.at[2], h_recv.at[2], "sp", beside[1]).wait_recv()

        def add(seq, carry):
            passed = jnp.exp(edge[4 * blocks + seq, 0:1, :])
            gout[seq, :, :] = (
                gout[seq, :, :].astype(f32) + passed * gin[seq, :, :].astype(f32)
            ).astype(bf16)
            return carry

        def pass_on():
            lax.fori_loop(0, 4, add, 0)
            chain[0].start()

        pl.when(has[0])(pass_on)

    near_first = 2 * me < count
    pl.when(inner & near_first)(forward_step)
    pl.when(inner)(backward_step)
    pl.when(inner & jnp.logical_not(near_first))(forward_step)
    send_line(2, 0, inner)
    if count > 2:
        take_line(2, 1, mode="pass_rest")
    send_line(4, 0, inner)
    for hop in range(2, count - 1):
        take_line(2, hop, mode="pass")
    if count > 2:
        take_line(4, 1, mode="pass_rest")
    for hop in range(2, count - 1):
        take_line(4, hop, mode="pass")
    for side in range(2):
        pl.when(has[side])(lambda side=side: kv_edge[side].start())
    for hop in range(2, count - 1):
        relay_out(hop)
    if count > 2:
        take_line(3, count - 1, spread)

    inner_rows = pl.ds(BLOCK, rows - 2 * BLOCK)
    parts = (
        (pl.ds(0, rows), pl.ds(0, lanes)),
        (inner_rows, pl.ds(lanes, HEAD_DIM)),
        (inner_rows, pl.ds(lanes + HEAD_DIM, HEAD_DIM)),
        (pl.ds(0, BLOCK), pl.ds(lanes, 2 * HEAD_DIM)),
        (pl.ds(rows - BLOCK, BLOCK), pl.ds(lanes, 2 * HEAD_DIM)),
    )

    def swap(k, part):
        slot = part * 4 + k
        return to(
            mixs.at[(peers[k], *parts[part])],
            mixr.at[(fs, *parts[part])],
            m_send.at[slot],
            m_recv.at[slot],
            "fs",
            peers[k],
        )

    def swap_in(k, part):
        ref, slot = mixr.at[(peers[k], *parts[part])], part * 4 + k
        return to(ref, ref, m_send.at[slot], m_recv.at[slot], "fs", peers[k])

    pl.when(has[0] & jnp.logical_not(has[1]))(forward_step)
    pl.when(has[1] & jnp.logical_not(has[0]))(backward_step)
    gain_row = gain[:, own_cols]

    def split_dot(a, b):
        top_bits = b.astype(bf16)
        rest = (b - top_bits.astype(f32)).astype(bf16)
        return jnp.dot(a, top_bits, preferred_element_type=f32) + jnp.dot(
            a, rest, preferred_element_type=f32
        )

    def finish_block(index):
        seq, blk = index // blocks, index % blocks
        at = pl.ds(pl.multiple_of(blk * BLOCK, BLOCK), BLOCK)
        ahead = sabuf[index, :, :] + jnp.exp(edge[index, 0:1, :]) * fin[seq, :, :].astype(f32)
        behind = sbbuf[index, :, :] + jnp.exp(edge[index, 1:2, :]) * gin[seq, :, :].astype(f32)
        sq = sqbuf[seq, at, :]
        cum = cumbuf[seq, at, :]
        total = cum[BLOCK - 1 : BLOCK, :]
        mixed = (
            nbuf[seq, at, :]
            + jnp.exp(cum) * split_dot(sq, ahead)
            + jnp.exp(total - cum) * split_dot(sq, behind)
        )
        g = gbuf[seq, at, :].astype(f32)
        gated = mixed * (g * jax.nn.sigmoid(g))
        square = gated * gated
        first = jnp.sum(jnp.where(left, square, 0.0), axis=-1, keepdims=True)
        second = jnp.sum(jnp.where(left, 0.0, square), axis=-1, keepdims=True)
        mean = jnp.where(left, first, second) * (2.0 / lanes)
        mix = (gated * lax.rsqrt(mean + 1e-06) * gain_row).astype(bf16)

        def store():
            mixs[seq, at, :lanes] = mix

        return store

    lax.fori_loop(0, 2 * blocks, pairs_of(finish_block), 0)
    for k in (3, 1, 2):
        swap(k, 0).start()


    def query_cols(r):
        return slice((6 + r) * lanes, (7 + r) * lanes)

    def head_cols(r):
        return slice(r * HEAD_DIM, (r + 1) * HEAD_DIM)

    near_count = max(1, count // 2)
    near_at = pl.ds(
        pl.multiple_of(at_top * (count - near_count) * depth, depth), near_count * depth
    )
    far_at = pl.ds(
        pl.multiple_of((1 - at_top) * near_count * depth, depth), (count - near_count) * depth
    )
    query_parts = ((most_at, last_at), (near_at, far_at))

    def query_first(r):
        at = query_parts[r][0]

        def body(seq, carry):
            acc[seq, :, head_cols(r)] = jnp.dot(
                xbuf[seq, :, at], wbuf[at, query_cols(r)], preferred_element_type=f32
            )
            return carry

        lax.fori_loop(0, 4, body, 0)

    def query_rest(r):
        at = query_parts[r][1]

        def body(seq, carry):
            y = acc[seq, :, head_cols(r)] + jnp.dot(
                xbuf[seq, :, at], wbuf[at, query_cols(r)], preferred_element_type=f32
            )
            qbuf[seq, :, head_cols(r)] = rotated(y.astype(bf16).astype(f32))
            return carry

        lax.fori_loop(0, 4, body, 0)

    for hop in range(1, count - 1):
        take_line(2, hop, mode="keep")
    query_first(0)
    take_line(2, count - 1, mode="keep")
    query_rest(0)
    band = 3 * WINDOW
    log2e = math.log2(math.e)
    def sink_rows(heads):
        row = lax.broadcasted_iota(jnp.int32, (len(heads) * WINDOW, 1), 0)
        first = sink[2 * fs + heads[0]]
        return log2e * jnp.where(row < WINDOW, first, sink[2 * fs + heads[-1]])

    floors = {heads: sink_rows(heads) for heads in ((0,), (1,), (0, 1))}

    def attend_block(seq, blk, heads):
        at = pl.ds(pl.multiple_of(blk * WINDOW, WINDOW), WINDOW)
        wide = pl.ds(pl.multiple_of(blk * WINDOW, WINDOW), band)
        q = jnp.concatenate([qbuf[seq, at, head_cols(r)] for r in heads], axis=0)
        s = lax.dot_general(
            q,
            kvbuf[seq, wide, :HEAD_DIM],
            (((1,), (1,)), ((), ())),
            preferred_element_type=f32,
        )
        kind = jnp.where(blk == 0, 0, jnp.where(blk == blocks - 1, 2, 1))
        floor = floors[heads]
        s = s * (HEAD_DIM ** (-0.5) * log2e) + bias[kind, : len(heads) * WINDOW, :]
        m = jnp.maximum(jnp.max(s, axis=-1, keepdims=True), floor)
        w = jnp.exp2(s - m).astype(bf16)
        y = jnp.dot(w, kvbuf[seq, wide, HEAD_DIM:], preferred_element_type=f32)
        total = jnp.exp2(floor - m) + y[:, HEAD_DIM:]
        o = (y[:, :HEAD_DIM] / total).astype(bf16)

        def store():
            for index, r in enumerate(heads):
                mixs[seq, at, lanes + r * HEAD_DIM : lanes + (r + 1) * HEAD_DIM] = o[
                    index * WINDOW : (index + 1) * WINDOW
                ]

        return store

    def far_first(step):
        return jnp.where(
            step == 0,
            peers[3],
            jnp.where(step == 1, peers[1], jnp.where(step == 2, peers[2], peers[0])),
        )

    def attend_inner(r):
        def each(step, carry):
            seq = far_first(step)

            def body(index, carry):
                for store in [attend_block(seq, 1 + 2 * index + k, (r,)) for k in range(2)]:
                    store()
                return carry

            lax.fori_loop(0, blocks // 2 - 1, body, 0)
            for index, k in enumerate((3, 1, 2)):
                pl.when(step == index)(lambda k=k: swap(k, 1 + r).start())
            return carry

        lax.fori_loop(0, 4, each, 0)

    attend_inner(0)
    for hop in range(1, near_count):
        take_line(4, hop, mode="keep")
    query_first(1)
    if count > 2:
        relay_out(count - 1)
    for hop in range(near_count, count):
        take_line(4, hop, mode="keep")
    query_rest(1)
    attend_inner(1)
    for side in range(2):
        pl.when(has[side])(lambda side=side: kv_in[side].wait_recv())

    def attend_edges(step, carry):
        seq = far_first(step)
        for store in [attend_block(seq, blk, (0, 1)) for blk in (0, blocks - 1)]:
            store()
        for index, k in enumerate((3, 1, 2)):

            def send(k=k):
                swap(k, 3).start()
                swap(k, 4).start()

            pl.when(step == index)(send)
        return carry

    lax.fori_loop(0, 4, attend_edges, 0)

    cols = w_sout.shape[1]

    def out_in(origin):
        def work():
            plane(origin, 3, halves[0], 3, 2).wait_recv()
            plane(origin, 3, halves[1], 0, 1).wait_recv()

        pl.when(origin != me)(work)

    def trade(origin):
        return to(
            psend.at[origin], precv.at[origin], p_send.at[origin], p_recv.at[origin], "tp", other
        )

    def hand_over(origin, totals):
        psend[origin, :, :] = totals[0].astype(bf16)
        trade(origin).start()
        pown[origin, :, :] = totals[1].astype(bf16)

    row_halves = (other_half, own_half)

    def first_product(origin, carry):
        out_in(origin)
        weights = jnp.concatenate(
            [wob[origin, fs, :, :]] + [wob[origin, peers[k], :lanes, :] for k in range(1, 4)], axis=0
        )
        for at in row_halves:
            mix = jnp.concatenate(
                [mixs[fs, at, :]] + [mixr[peers[k], at, :lanes] for k in range(1, 4)], axis=1
            )
            oacc[origin, at, :] = jnp.dot(mix, weights, preferred_element_type=f32)
        return carry

    def add_parts(ks, last):
        def body(origin, carry):
            weights = jnp.concatenate([wob[origin, peers[k], lanes:, :] for k in ks], axis=0)
            totals = [
                oacc[origin, at, :]
                + jnp.dot(
                    jnp.concatenate([mixr[peers[k], at, lanes:] for k in ks], axis=1),
                    weights,
                    preferred_element_type=f32,
                )
                for at in row_halves
            ]
            if last:
                hand_over(origin, totals)
            else:
                for total, at in zip(totals, row_halves):
                    oacc[origin, at, :] = total
            return carry

        lax.fori_loop(0, count, body, 0)

    def store_out(origin):
        return pltpu.make_async_copy(
            sums.at[origin],
            out.at[:, pl.ds(pl.multiple_of(origin * cols, cols), cols)],
            loc_sem.at[17 + origin],
        )

    def finish_out(origin):
        trade(origin).wait_recv()
        sums[origin, :, :] = (
            pown[origin, :, :].astype(f32) + precv[origin, :, :].astype(f32)
        ).astype(bf16)
        store_out(origin).start()

    for k in (3, 1, 2):
        swap_in(k, 0).wait_recv()
    lax.fori_loop(0, count, first_product, 0)
    for ks in ((3,), (1, 2)):
        for k in ks:
            for part in range(1, 5):
                swap_in(k, part).wait_recv()
        add_parts(ks, 2 in ks)

    def finish_each(origin, carry):
        finish_out(origin)
        return carry

    lax.fori_loop(0, count, finish_each, 0)
    for origin in range(count):
        store_out(origin).wait()

    for piece in range(pieces):
        for hop in range(count - 1):
            for side in range(2):
                pl.when(has[side] & valid(hop, side))(
                    lambda piece=piece, hop=hop, side=side: line(piece, hop, side).wait_send()
                )
    for copy in x_own + relay + across:
        copy.wait_send()
    for side in range(2):
        pl.when(has[side])(lambda side=side: halo[side].wait_send())
        pl.when(has[side])(lambda side=side: chain[side].wait_send())
        pl.when(has[side])(lambda side=side: kv_edge[side].wait_send())
    for k in range(1, 4):
        for part in range(5):
            swap(k, part).wait_send()

    def left_plane(origin, carry):
        def work():
            plane(origin, 0, None, 1, 1).wait_send()
            plane(origin, 0, None, 2, 2).wait_send()
            plane(origin, 1, halves[0], 3, 2).wait_send()
            plane(origin, 2, halves[1], 0, 1).wait_send()

        pl.when(origin != me)(work)
        return carry

    lax.fori_loop(0, count, left_plane, 0)
    for origin in range(count):
        trade(origin).wait_send()


def fused_shards(
    tokens,
    norm_gain,
    state_gate,
    state_value,
    state_keys,
    state_query,
    state_step,
    state_rate,
    state_jumps,
    state_gain,
    filter_value,
    filter_keys,
    filter_query,
    window_query,
    window_keys,
    window_values,
    window_sink,
    state_output,
    window_output,
):
    count = lax.axis_size("sp")
    rows, width = tokens.shape
    lanes = STATE_SIZE
    blocks = rows // BLOCK
    depth = state_value.shape[0]
    cols = state_output.shape[1]
    out_rows = (state_output.shape[0] + window_output.shape[0]) // 4
    f32, bf16 = jnp.float32, jnp.bfloat16
    vmem = pltpu.VMEM
    dma = pltpu.SemaphoreType.DMA
    hbm = pl.BlockSpec(memory_space=pl.ANY)
    chip = pl.BlockSpec(memory_space=pltpu.VMEM)
    scalar = pl.BlockSpec(memory_space=pltpu.SMEM)
    jumps = state_jumps.T
    half = rows // 2
    return pl.pallas_call(
        functools.partial(fused_kernel, count),
        out_shape=jax.ShapeDtypeStruct((half, width), bf16),
        in_specs=[hbm] * 10
        + [chip, hbm, scalar, chip, chip, chip, chip, chip, scalar],
        out_specs=hbm,
        scratch_shapes=[
            vmem((rows, width), bf16),
            vmem((4, rows, width), bf16),
            vmem((count * depth, 8 * lanes), bf16),
            vmem((count, 4, out_rows, cols), bf16),
            vmem(state_step.shape[::-1], bf16),
            vmem((lanes, width), bf16),
            vmem((rows, lanes), f32),
            vmem((rows, lanes), f32),
            vmem((4,) + jumps.shape, f32),
            vmem((3, 2 * WINDOW, 3 * WINDOW), f32),
            vmem((4, rows, 4 * lanes), f32),
            vmem((count, rows, cols), f32),
            vmem((4, rows + 16, 3 * lanes), f32),
            vmem((4, rows, lanes), bf16),
            vmem((4, rows, lanes), f32),
            vmem((4, rows, lanes), f32),
            vmem((4 * blocks, STATE_SIZE, lanes), f32),
            vmem((4 * blocks, STATE_SIZE, lanes), f32),
            vmem((4, rows, lanes), f32),
            vmem((4 * blocks + 4, 8, lanes), f32),
            vmem((4, rows, lanes), bf16),
            vmem((4, STATE_SIZE, lanes), bf16),
            vmem((4, STATE_SIZE, lanes), bf16),
            vmem((4, STATE_SIZE, lanes), bf16),
            vmem((4, STATE_SIZE, lanes), bf16),
            vmem((4, rows + 2 * WINDOW, 3 * HEAD_DIM), bf16),
            vmem((4, rows, 2 * HEAD_DIM), bf16),
            vmem((4, rows, 3 * lanes), bf16),
            vmem((4, rows, 3 * lanes), bf16),
            vmem((count, half, cols), bf16),
            vmem((count, half, cols), bf16),
            vmem((count, half, cols), bf16),
            vmem((count, half, cols), bf16),
            dma((17 + count,)),
            dma((10 * (count - 1),)),
            dma((10 * (count - 1),)),
            dma((4,)),
            dma((4,)),
            dma((3,)),
            dma((3,)),
            dma((4,)),
            dma((4,)),
            dma((6,)),
            dma((6,)),
            dma((20,)),
            dma((20,)),
            dma((4 * count,)),
            dma((4 * count,)),
            dma((count,)),
            dma((count,)),
        ],
        compiler_params=pltpu.CompilerParams(
            collective_id=0, has_side_effects=True, vmem_limit_bytes=62 * 1024 * 1024
        ),
        name="fused_layer",
    )(
        tokens,
        state_value,
        state_keys,
        state_query,
        state_gate,
        window_keys,
        window_values,
        window_query,
        state_output,
        window_output,
        norm_gain.reshape(1, -1),
        state_step.T,
        state_rate,
        jumps,
        state_gain.reshape(1, -1),
        filter_value,
        filter_keys,
        filter_query,
        window_sink,
    )


def solution(mesh):
    placed = (
        P(("fs", "sp"), None),
        P(),
        P("sp", "tp"),
        P("sp", "tp"),
        P("sp", "tp"),
        P("sp", "tp"),
        P(),
        P("tp"),
        P(("fs", "sp"), "tp"),
        P("tp"),
        P(None, "tp"),
        P(None, "tp"),
        P(None, "tp"),
        P("sp", "tp"),
        P("sp", "tp"),
        P("sp", "tp"),
        P("tp"),
        P("tp", "sp"),
        P("tp", "sp"),
    )
    def plan(*args):
        return (fused_shards if fits(*args) else shards)(*args)

    return jax.shard_map(
        plan, mesh=mesh, in_specs=placed, out_specs=P(("fs", "sp", "tp"), None), check_vma=False
    )
```

```python
import functools
import math

import jax
import jax.numpy as jnp
from jax import lax
from jax.experimental import pallas as pl
from jax.experimental.pallas import tpu as pltpu
from jax.sharding import PartitionSpec as P

STATE_SIZE = 128
HEAD_DIM = 128
WINDOW = 128
BLOCK = 128
GRID_WIDTH = 64


def extended(cells, sides, width):
    for axis, dim in sides:
        count = lax.axis_size(axis)
        ends = count - 1
        head = lax.slice_in_dim(cells, 0, width, axis=dim)
        tail = lax.slice_in_dim(cells, cells.shape[dim] - width, cells.shape[dim], axis=dim)
        cells = jnp.concatenate(
            [
                lax.ppermute(tail, axis, [(i, (i + 1) % count) for i in range(ends)]),
                cells,
                lax.ppermute(head, axis, [((i + 1) % count, i) for i in range(ends)]),
            ],
            axis=dim,
        )
    return cells


def rotate_grid(vectors, positions, grid_width):
    head_dim = vectors.shape[-1]
    quarter = head_dim // 4
    half_dim = head_dim // 2
    inverse = 10000.0 ** (-jnp.arange(quarter, dtype=jnp.float32) / quarter)
    grid_row = (positions // grid_width).astype(jnp.float32)
    grid_col = (positions % grid_width).astype(jnp.float32)
    angle_row = grid_row[:, None] * inverse[None, :]
    angle_col = grid_col[:, None] * inverse[None, :]
    angles = jnp.concatenate([angle_row, angle_row, angle_col, angle_col], axis=-1)[:, None, :]
    first_half = vectors[..., :half_dim]
    second = vectors[..., half_dim:]
    turned = jnp.concatenate(
        [
            -first_half[..., quarter:],
            first_half[..., :quarter],
            -second[..., quarter:],
            second[..., :quarter],
        ],
        axis=-1,
    )
    return (
        vectors.astype(jnp.float32) * jnp.cos(angles) + turned.astype(jnp.float32) * jnp.sin(angles)
    ).astype(jnp.bfloat16)


def window_attend(query_rows, keys_pad, values_pad, sink_logits, key_start, total_len, window):
    row_count, query_heads, head_dim = query_rows.shape
    kv_heads = keys_pad.shape[1]
    group_size = query_heads // kv_heads
    block_count = row_count // window
    query_blocks = query_rows.reshape(block_count, window, kv_heads, group_size, head_dim)
    key_split = keys_pad.reshape(block_count + 2, window, kv_heads, head_dim)
    value_split = values_pad.reshape(block_count + 2, window, kv_heads, head_dim)
    key_band = jnp.concatenate([key_split[:-2], key_split[1:-1], key_split[2:]], axis=1)
    value_band = jnp.concatenate([value_split[:-2], value_split[1:-1], value_split[2:]], axis=1)
    scores = jnp.einsum(
        "kihgd,kjhd->khgij", query_blocks, key_band, preferred_element_type=jnp.float32
    ) * head_dim ** (-0.5)
    query_pos = jnp.arange(window)[:, None]
    band_pos = jnp.arange(3 * window)[None, :]
    within = jnp.abs(band_pos - window - query_pos) <= window
    key_pos = (
        key_start + jnp.arange(block_count)[:, None] * window + jnp.arange(3 * window)[None, :]
    )
    inside = (key_pos >= 0) & (key_pos < total_len)
    valid_pair = (within[None] & inside[:, None, :])[:, None, None]
    sink_logit = sink_logits.reshape(kv_heads, group_size)[None, :, :, None, None]
    masked = jnp.where(valid_pair, scores, -1e30)
    ceiling = jnp.maximum(jnp.max(masked, axis=-1, keepdims=True), sink_logit)
    weights = jnp.where(valid_pair, jnp.exp(masked - ceiling), 0.0)
    denominator = jnp.exp(sink_logit - ceiling) + jnp.sum(weights, axis=-1, keepdims=True)
    weights_bf = (weights / denominator).astype(jnp.bfloat16)
    mixed_rows = jnp.einsum(
        "khgij,kjhd->kihgd", weights_bf, value_band, preferred_element_type=jnp.float32
    )
    return mixed_rows.reshape(row_count, query_heads * head_dim).astype(jnp.bfloat16)


def block_terms(query_rows, key_rows, value_rows, log_rows, block_len):
    row_count, group_count, state_size = query_rows.shape
    head_ratio, head_dim = (value_rows.shape[2], value_rows.shape[3])
    block_count = row_count // block_len
    query_blocks = query_rows.reshape(block_count, block_len, group_count, state_size)
    key_blocks = key_rows.reshape(block_count, block_len, group_count, state_size)
    value_blocks = value_rows.reshape(block_count, block_len, group_count, head_ratio, head_dim)
    decay_cum = jnp.cumsum(
        log_rows.reshape(block_count, block_len, group_count, head_ratio), axis=1
    )
    decay_total = decay_cum[:, -1]
    gram_block = jnp.einsum(
        "kign,kjgn->kgij", query_blocks, key_blocks, preferred_element_type=jnp.float32
    )
    cum_heads = jnp.moveaxis(decay_cum, 1, 3)
    distance = jnp.abs(cum_heads[..., :, None] - cum_heads[..., None, :])
    pair_weight = (gram_block[:, :, None] * jnp.exp(-distance)).astype(jnp.bfloat16)
    near_terms = jnp.einsum(
        "kgrij,kjgrp->kigrp", pair_weight, value_blocks, preferred_element_type=jnp.float32
    )
    keys_after = (
        key_blocks[:, :, :, None, :] * jnp.exp(decay_total[:, None] - decay_cum)[..., None]
    ).astype(jnp.bfloat16)
    keys_before = (key_blocks[:, :, :, None, :] * jnp.exp(decay_cum)[..., None]).astype(
        jnp.bfloat16
    )
    state_after = jnp.einsum(
        "kjgrn,kjgrp->kgrnp", keys_after, value_blocks, preferred_element_type=jnp.float32
    )
    state_before = jnp.einsum(
        "kjgrn,kjgrp->kgrnp", keys_before, value_blocks, preferred_element_type=jnp.float32
    )
    before = jnp.cumsum(decay_total, axis=0) - decay_total
    overall = jnp.sum(decay_total, axis=0)
    after_sum = overall[None] - before - decay_total
    block_order = jnp.arange(block_count)
    earlier_mask = (block_order[None, :] < block_order[:, None])[:, :, None, None]
    later_mask = (block_order[None, :] > block_order[:, None])[:, :, None, None]
    gap_fwd = before[:, None] - before[None, :] - decay_total[None, :]
    gap_bwd = before[None, :] - before[:, None] - decay_total[:, None]
    weight_fwd = jnp.where(earlier_mask, jnp.exp(jnp.minimum(gap_fwd, 0.0)), 0.0)
    weight_bwd = jnp.where(later_mask, jnp.exp(jnp.minimum(gap_bwd, 0.0)), 0.0)
    carried_fwd = jnp.einsum(
        "abgr,bgrnp->agrnp", weight_fwd, state_after, precision=lax.Precision.HIGHEST
    )
    carried_bwd = jnp.einsum(
        "abgr,bgrnp->agrnp", weight_bwd, state_before, precision=lax.Precision.HIGHEST
    )
    summary_fwd = jnp.einsum(
        "agr,agrnp->grnp", jnp.exp(after_sum), state_after, precision=lax.Precision.HIGHEST
    )
    summary_bwd = jnp.einsum(
        "agr,agrnp->grnp", jnp.exp(before), state_before, precision=lax.Precision.HIGHEST
    )
    pieces = (
        near_terms,
        carried_fwd,
        carried_bwd,
        decay_cum,
        decay_total,
        before,
        after_sum,
        query_blocks,
    )
    return (pieces, (summary_fwd, summary_bwd, overall))


def finish_terms(pieces, incoming_fwd, incoming_bwd):
    (
        near_terms,
        carried_fwd,
        carried_bwd,
        decay_cum,
        decay_total,
        before,
        after_sum,
        query_blocks,
    ) = pieces
    total_fwd = carried_fwd + jnp.exp(before)[..., None, None] * incoming_fwd[None]
    total_bwd = carried_bwd + jnp.exp(after_sum)[..., None, None] * incoming_bwd[None]
    query_wide = query_blocks.astype(jnp.float32)
    read_fwd = jnp.einsum(
        "kign,kgrnp->kigrp", query_wide, total_fwd, precision=lax.Precision.HIGHEST
    )
    read_bwd = jnp.einsum(
        "kign,kgrnp->kigrp", query_wide, total_bwd, precision=lax.Precision.HIGHEST
    )
    combined = (
        near_terms
        + jnp.exp(decay_cum)[..., None] * read_fwd
        + jnp.exp(decay_total[:, None] - decay_cum)[..., None] * read_bwd
    )
    block_count, block_len, group_count, head_ratio, head_dim = combined.shape
    return combined.reshape(block_count * block_len, group_count, head_ratio, head_dim)


def combine_all(gathered_states, own_index):
    after_all, before_all, logs_all = gathered_states
    device_count = logs_all.shape[0]
    cum_incl = jnp.cumsum(logs_all, axis=0)
    cum_excl = cum_incl - logs_all
    device_order = jnp.arange(device_count)
    picker = (device_order == own_index).astype(jnp.float32)[:, None, None]
    own_incl = jnp.sum(picker * cum_incl, axis=0)
    own_excl = jnp.sum(picker * cum_excl, axis=0)
    lower_mask = (device_order < own_index)[:, None, None]
    higher_mask = (device_order > own_index)[:, None, None]
    weight_fwd = jnp.where(lower_mask, jnp.exp(jnp.minimum(own_excl[None] - cum_incl, 0.0)), 0.0)
    weight_bwd = jnp.where(higher_mask, jnp.exp(jnp.minimum(cum_excl - own_incl[None], 0.0)), 0.0)
    incoming_fwd = jnp.einsum(
        "dgr,dgrnp->grnp", weight_fwd, after_all, precision=lax.Precision.HIGHEST
    )
    incoming_bwd = jnp.einsum(
        "dgr,dgrnp->grnp", weight_bwd, before_all, precision=lax.Precision.HIGHEST
    )
    return (incoming_fwd, incoming_bwd)


def shards(
    tokens,
    norm_gain,
    state_gate,
    state_value,
    state_keys,
    state_query,
    state_step,
    state_rate,
    state_jumps,
    state_gain,
    filter_value,
    filter_keys,
    filter_query,
    window_query,
    window_keys,
    window_values,
    window_sink,
    state_output,
    window_output,
):
    row_count = tokens.shape[0]
    rows_wide = tokens.astype(jnp.float32)
    normed = (
        rows_wide
        * lax.rsqrt(jnp.mean(rows_wide * rows_wide, axis=-1, keepdims=True) + 1e-06)
        * norm_gain
    ).astype(jnp.bfloat16)
    gathered = (
        lax.all_gather(state_gate, "sp", axis=0, tiled=True),
        lax.all_gather(state_value, "sp", axis=0, tiled=True),
        lax.all_gather(state_keys, "sp", axis=0, tiled=True),
        lax.all_gather(state_query, "sp", axis=0, tiled=True),
        lax.all_gather(window_query, "sp", axis=0, tiled=True),
        lax.all_gather(window_keys, "sp", axis=0, tiled=True),
        lax.all_gather(window_values, "sp", axis=0, tiled=True),
        lax.all_gather(state_output, "sp", axis=1, tiled=True),
        lax.all_gather(window_output, "sp", axis=1, tiled=True),
    )
    projected = [
        jnp.dot(normed, matrix, preferred_element_type=jnp.float32) for matrix in gathered[:7]
    ]
    out_state = gathered[7]
    out_window = gathered[8]
    gate_rows, value_pre, keys_pre, query_pre, query_raw, keys_raw, values_rows = [
        result.astype(jnp.bfloat16) for result in projected
    ]
    head_local = state_rate.shape[0]
    group_local = keys_pre.shape[1] // STATE_SIZE
    head_dim = value_pre.shape[1] // head_local
    head_ratio = head_local // group_local
    step_cols = lax.dynamic_slice_in_dim(
        state_step, lax.axis_index("tp") * head_local, head_local, 1
    )
    step_rows = jax.nn.softplus(jnp.dot(normed, step_cols, preferred_element_type=jnp.float32))
    log_decay = -state_rate[None, :] * step_rows + state_jumps
    half_width = filter_value.shape[0] // 2
    stacked = jnp.concatenate([value_pre, keys_pre, query_pre], axis=-1)
    padded = extended(stacked, (("sp", 0),), half_width)
    filters = jnp.concatenate([filter_value, filter_keys, filter_query], axis=-1).astype(
        jnp.float32
    )
    filtered = jnp.zeros(stacked.shape, jnp.float32)
    for offset in range(filters.shape[0]):
        filtered = (
            filtered + padded[offset : offset + row_count].astype(jnp.float32) * filters[offset]
        )
    value_cols = value_pre.shape[1]
    key_cols = keys_pre.shape[1]
    inner_rows = (
        jax.nn.silu(filtered[:, :value_cols]).reshape(row_count, head_local, head_dim)
        * step_rows[..., None]
    )
    scan_values = inner_rows.astype(jnp.bfloat16).reshape(
        row_count, group_local, head_ratio, head_dim
    )
    scan_keys = (
        filtered[:, value_cols : value_cols + key_cols]
        .astype(jnp.bfloat16)
        .reshape(row_count, group_local, STATE_SIZE)
    )
    scan_query = (
        filtered[:, value_cols + key_cols :]
        .astype(jnp.bfloat16)
        .reshape(row_count, group_local, STATE_SIZE)
    )
    pieces, summaries = block_terms(
        scan_query,
        scan_keys,
        scan_values,
        log_decay.reshape(row_count, group_local, head_ratio),
        BLOCK,
    )
    summary_fwd, summary_bwd, overall = summaries
    gathered_states = (
        lax.all_gather(summary_fwd[None].astype(jnp.bfloat16), "sp", axis=0, tiled=True).astype(
            jnp.float32
        ),
        lax.all_gather(summary_bwd[None].astype(jnp.bfloat16), "sp", axis=0, tiled=True).astype(
            jnp.float32
        ),
        lax.all_gather(overall[None].astype(jnp.bfloat16), "sp", axis=0, tiled=True).astype(
            jnp.float32
        ),
    )
    incoming_fwd, incoming_bwd = combine_all(gathered_states, lax.axis_index("sp"))
    scan_out = finish_terms(pieces, incoming_fwd, incoming_bwd).reshape(
        row_count, head_local * head_dim
    )
    gated_rows = scan_out * jax.nn.silu(gate_rows.astype(jnp.float32))
    per_head = gated_rows.reshape(row_count, head_local, head_dim)
    state_mix = (
        (
            per_head
            * lax.rsqrt(jnp.mean(per_head * per_head, axis=-1, keepdims=True) + 1e-06)
            * state_gain.reshape(head_local, head_dim)
        )
        .astype(jnp.bfloat16)
        .reshape(row_count, head_local * head_dim)
    )
    query_heads = window_sink.shape[0]
    kv_heads = keys_raw.shape[1] // HEAD_DIM
    kv_width = kv_heads * HEAD_DIM
    positions = lax.axis_index("sp") * row_count + jnp.arange(row_count, dtype=jnp.int32)
    query_rot = rotate_grid(
        query_raw.reshape(row_count, query_heads, HEAD_DIM), positions, GRID_WIDTH
    )
    keys_rot = rotate_grid(keys_raw.reshape(row_count, kv_heads, HEAD_DIM), positions, GRID_WIDTH)
    pair_rows = jnp.concatenate([keys_rot.reshape(row_count, kv_width), values_rows], axis=-1)
    padded_pair = extended(pair_rows, (("sp", 0),), WINDOW)
    keys_pad = padded_pair[:, :kv_width].reshape(-1, kv_heads, HEAD_DIM)
    values_pad = padded_pair[:, kv_width:].reshape(-1, kv_heads, HEAD_DIM)
    window_mix = window_attend(
        query_rot,
        keys_pad,
        values_pad,
        window_sink,
        lax.axis_index("sp") * row_count - WINDOW,
        lax.axis_size("sp") * row_count,
        WINDOW,
    )
    return lax.psum_scatter(
        (
            jnp.dot(state_mix, out_state, preferred_element_type=jnp.float32)
            + jnp.dot(window_mix, out_window, preferred_element_type=jnp.float32)
        ).astype(jnp.bfloat16),
        "tp",
        scatter_dimension=0,
        tiled=True,
    )


def fits(*args):
    tokens, state_value, state_keys, state_rate = args[0], args[3], args[4], args[7]
    window_query, window_keys, window_sink = args[13], args[14], args[16]
    parts = lax.axis_size("fs")
    heads = state_rate.shape[0]
    return (
        parts == 4
        and lax.axis_size("tp") == 2
        and lax.axis_size("sp") > 1
        and tokens.shape[0] % (4 * BLOCK) == 0
        and state_keys.shape[1] == parts * STATE_SIZE
        and state_value.shape[1] == parts * STATE_SIZE
        and heads == 2 * parts
        and window_keys.shape[1] == parts * HEAD_DIM
        and window_query.shape[1] == 2 * parts * HEAD_DIM
        and window_sink.shape[0] == 2 * parts
    )


def fused_kernel(
    count,
    tokens,
    w_value,
    w_keys,
    w_query,
    w_gate,
    w_wkeys,
    w_wvalues,
    w_wquery,
    w_sout,
    w_wout,
    norm_gain_in,
    step_w,
    rate,
    jumps_in,
    gain_in,
    tap_value_in,
    tap_keys_in,
    tap_query_in,
    sink,
    out_own,
    out_other,
    norm_gain,
    jumps,
    gain,
    tap_value,
    tap_keys,
    tap_query,
    tbuf,
    xbuf,
    wbuf,
    wob,
    stepw,
    stepx,
    cos_t,
    sin_t,
    jbuf,
    bias,
    acc,
    oacc,
    cbuf,
    gbuf,
    stbuf,
    nbuf,
    sabuf,
    sbbuf,
    cumbuf,
    edge,
    sqbuf,
    fin,
    gin,
    fout,
    gout,
    kvbuf,
    qbuf,
    mixs,
    mixr,
    psend,
    pown,
    loc_sem,
    z_send,
    z_recv,
    x_send,
    x_recv,
    d_send,
    d_recv,
    j_send,
    j_recv,
    h_send,
    h_recv,
    m_send,
    m_recv,
    o_send,
    o_recv,
    p_send,
    p_recv,
):
    f32, bf16 = jnp.float32, jnp.bfloat16
    me, fs, tp = lax.axis_index("sp"), lax.axis_index("fs"), lax.axis_index("tp")
    rows, width = tokens.shape
    depth = w_value.shape[0]
    half = rows // 2
    quarter = half // 2
    blocks = rows // BLOCK
    lanes = STATE_SIZE
    has = [me > 0, me < count - 1]
    beside = [jnp.maximum(me - 1, 0), jnp.minimum(me + 1, count - 1)]
    peers = [fs, fs + 1 - 2 * (fs % 2), fs + 2 - 4 * (fs // 2), 3 - fs]
    other = 1 - tp

    def to(ref_src, ref_dst, send, recv, axis, index):
        return pltpu.make_async_remote_copy(
            src_ref=ref_src,
            dst_ref=ref_dst,
            send_sem=send,
            recv_sem=recv,
            device_id={axis: index},
            device_id_type=pl.DeviceIdType.MESH,
        )

    own_rows = pl.ds(pl.multiple_of(me * depth, depth), depth)
    loads = [pltpu.make_async_copy(tokens, tbuf, loc_sem.at[0])]
    col = 0
    weight_loads = []
    for index, matrix in enumerate(
        (w_value, w_keys, w_query, w_gate, w_wkeys, w_wvalues, w_wquery)
    ):
        size = matrix.shape[1] // 4
        weight_loads.append(
            pltpu.make_async_copy(
                matrix.at[:, pl.ds(pl.multiple_of(fs * size, size), size)],
                wbuf.at[own_rows, pl.ds(col, size)],
                loc_sem.at[1 + index],
            )
        )
        col += size
    out_loads = []
    first_rows = w_sout.shape[0] // 4
    second_rows = w_wout.shape[0] // 4
    out_rows = first_rows + second_rows
    for part in range(4):
        out_loads.append(
            pltpu.make_async_copy(
                w_sout.at[pl.ds(part * first_rows, first_rows)],
                wob.at[me, part, pl.ds(0, first_rows)],
                loc_sem.at[8 + 2 * part],
            )
        )
        out_loads.append(
            pltpu.make_async_copy(
                w_wout.at[pl.ds(part * second_rows, second_rows)],
                wob.at[me, part, pl.ds(first_rows, second_rows)],
                loc_sem.at[9 + 2 * part],
            )
        )
    step_load = pltpu.make_async_copy(step_w, stepw, loc_sem.at[16])
    small = (
        (norm_gain_in, norm_gain),
        (jumps_in, jumps),
        (gain_in, gain),
        (tap_value_in, tap_value),
        (tap_keys_in, tap_keys),
        (tap_query_in, tap_query),
    )
    small_loads = [
        pltpu.make_async_copy(source, target, loc_sem.at[17 + count + index])
        for index, (source, target) in enumerate(small)
    ]

    barrier = pltpu.get_barrier_semaphore()
    for side in range(2):
        pl.when(has[side])(
            lambda side=side: pl.semaphore_signal(
                barrier,
                inc=1,
                device_id={"sp": beside[side]},
                device_id_type=pl.DeviceIdType.MESH,
            )
        )
    for k in range(1, 4):
        pl.semaphore_signal(
            barrier, inc=1, device_id={"fs": peers[k]}, device_id_type=pl.DeviceIdType.MESH
        )
    pl.semaphore_signal(
        barrier, inc=1, device_id={"tp": other}, device_id_type=pl.DeviceIdType.MESH
    )
    for load in weight_loads + loads + small_loads + [step_load]:
        load.start()
    pl.semaphore_wait(barrier, 4 + jnp.minimum(me, 1) + jnp.minimum(count - 1 - me, 1))

    spans = {
        0: (0, 4 * lanes),
        1: (4 * lanes, 2 * lanes),
        2: (6 * lanes, lanes),
        4: (7 * lanes, lanes),
    }
    pieces = 5

    def line(piece, hop, side):
        origin = me - hop if side == 1 else me + hop
        origin = jnp.clip(origin, 0, count - 1)
        if piece == 3:
            ref = wob.at[origin, fs]
        else:
            start, size = spans[piece]
            ref = wbuf.at[pl.ds(pl.multiple_of(origin * depth, depth), depth), pl.ds(start, size)]
        slot = (side * pieces + piece) * (count - 1) + hop
        return to(ref, ref, z_send.at[slot], z_recv.at[slot], "sp", beside[side])

    def valid(hop, side):
        return me >= hop if side == 1 else me + hop <= count - 1

    def send_line(piece, hop, where=True):
        for side in range(2):
            pl.when(has[side] & valid(hop, side) & where)(
                lambda side=side: line(piece, hop, side).start()
            )

    def take_line(piece, hop, then=None, mode=None, hold=False):
        for side in range(2):
            wanted = valid(hop, side)
            if mode == "pass":
                wanted = wanted & has[side]
            elif mode == "pass_end":
                wanted = wanted & has[side] & jnp.logical_not(valid(hop + 1, side))
            elif mode == "pass_rest":
                wanted = wanted & has[side] & valid(hop + 1, side)
            elif mode == "keep":
                wanted = wanted & jnp.logical_not(has[side])

            def arrive(side=side):
                line_in(piece, hop, side).wait_recv()
                if hop < count - 1 and not hold:
                    pl.when(has[side])(lambda: line(piece, hop, side).start())
                if then is not None:
                    then(hop, side)

            pl.when(wanted)(arrive)

    def line_in(piece, hop, side):
        origin = me - hop if side == 1 else me + hop
        origin = jnp.clip(origin, 0, count - 1)
        if piece == 3:
            ref = wob.at[origin, fs]
        else:
            start, size = spans[piece]
            ref = wbuf.at[pl.ds(pl.multiple_of(origin * depth, depth), depth), pl.ds(start, size)]
        slot = (side * pieces + piece) * (count - 1) + hop - 1
        return to(ref, ref, z_send.at[slot], z_recv.at[slot], "sp", beside[side])

    for load in weight_loads:
        load.wait()
    send_line(0, 0)
    send_line(1, 0)

    for load in loads + small_loads:
        load.wait()
    norm_rows = 32

    def norm(index, base):
        at = pl.ds(pl.multiple_of(base + index * norm_rows, norm_rows), norm_rows)
        wide = tbuf[at, :].astype(f32)
        scale = lax.rsqrt(jnp.mean(wide * wide, axis=-1, keepdims=True) + 1e-06)
        xbuf[fs, at, :] = (wide * scale * norm_gain[...]).astype(bf16)
        return base

    lax.fori_loop(0, half // norm_rows, norm, tp * half)
    lax.fori_loop(0, half // norm_rows, norm, other * half)
    own_half = pl.ds(pl.multiple_of(tp * half, half), half)
    x_own = [
        to(
            xbuf.at[fs, own_half],
            xbuf.at[fs, own_half],
            x_send.at[k - 1],
            x_recv.at[k - 1],
            "fs",
            peers[k],
        )
        for k in (1, 2)
    ]
    for copy in x_own:
        copy.start()
    j_own = [
        to(jumps, jbuf.at[fs], j_send.at[k], j_recv.at[k], "fs", peers[k]) for k in range(1, 4)
    ]
    for copy in j_own:
        copy.start()
    for load in out_loads:
        load.start()
    jbuf[fs, :, :] = jumps[...]

    lane = lax.broadcasted_iota(jnp.int32, (1, lanes), 1)
    low = lane < lanes // 2
    q4 = HEAD_DIM // 4

    def table(index, carry):
        at = pl.ds(pl.multiple_of(index * BLOCK, BLOCK), BLOCK)
        spot = lax.broadcasted_iota(jnp.int32, (BLOCK, lanes), 0) + me * rows + index * BLOCK
        place = jnp.where(low, spot // GRID_WIDTH, spot % GRID_WIDTH).astype(f32)
        inverse = jnp.exp((lane % q4).astype(f32) * (-math.log(10000.0) / q4))
        angle = place * inverse
        cos_t[at, :] = jnp.cos(angle)
        sin_t[at, :] = jnp.where(lane % (2 * q4) < q4, -1.0, 1.0) * jnp.sin(angle)
        return carry

    lax.fori_loop(0, blocks, table, 0)

    def window_bias(index, carry):
        q_id = lax.broadcasted_iota(jnp.int32, (2 * WINDOW, 3 * WINDOW), 0)
        b_id = lax.broadcasted_iota(jnp.int32, (2 * WINDOW, 3 * WINDOW), 1)
        blk = jnp.where(index == 2, blocks - 1, index)
        place = me * rows + (blk - 1) * WINDOW + b_id
        ok = jnp.abs(b_id - WINDOW - q_id % WINDOW) <= WINDOW
        ok = ok & (place >= 0) & (place < count * rows)
        bias[index, :, :] = jnp.where(ok, 0.0, -1e30)
        return carry

    lax.fori_loop(0, 3, window_bias, 0)
    kvbuf[:, :, 2 * HEAD_DIM :] = jnp.ones((4, rows + 2 * WINDOW, HEAD_DIM), bf16)
    heads_all = step_w.shape[0]
    first_head = (tp * 4 + fs) * 2
    pick = (
        lax.broadcasted_iota(jnp.int32, (lanes, heads_all), 1)
        == first_head + lax.broadcasted_iota(jnp.int32, (lanes, heads_all), 0) // (lanes // 2)
    )
    step_load.wait()
    stepx[...] = jnp.dot(
        pick.astype(f32).astype(bf16), stepw[...], preferred_element_type=f32
    ).astype(bf16)

    take_line(0, 1)
    for load in out_loads:
        load.wait()
    send_line(3, 0)

    x_first = pl.ds(pl.multiple_of(tp * half, quarter), quarter)
    x_second = pl.ds(pl.multiple_of(tp * half + quarter, quarter), quarter)

    def x_in(k, at, slot):
        return to(xbuf.at[peers[k], at], xbuf.at[peers[k], at], x_send.at[slot], x_recv.at[slot], "fs", peers[k])

    relay = [
        to(xbuf.at[peers[1], x_first], xbuf.at[peers[1], x_first], x_send.at[2], x_recv.at[2], "fs", peers[2]),
        to(xbuf.at[peers[2], x_second], xbuf.at[peers[2], x_second], x_send.at[3], x_recv.at[3], "fs", peers[1]),
    ]
    across = [
        to(xbuf.at[peers[k], own_half], xbuf.at[peers[k], own_half], d_send.at[k - 1], d_recv.at[k - 1], "tp", other)
        for k in range(1, 4)
    ]
    for k in (1, 2):
        x_in(k, own_half, k - 1).wait_recv()
        relay[k - 1].start()
        across[k - 1].start()
    if count > 2:
        take_line(0, 2)
    inner = has[0] & has[1]

    out_half = out_rows // 2

    def plane(origin, k, at, slot, target):
        ref = wob.at[origin, peers[k]] if at is None else wob.at[origin, peers[k], at]
        slot = origin * 4 + slot
        return to(ref, ref, o_send.at[slot], o_recv.at[slot], "fs", peers[target])

    halves = (pl.ds(0, out_half), pl.ds(out_half, out_half))

    def spread(hop, side):
        origin = jnp.clip(me - hop if side == 1 else me + hop, 0, count - 1)
        plane(origin, 0, None, 1, 1).start()
        plane(origin, 0, None, 2, 2).start()

    def relay_out(hop, where=True):
        for side in range(2):

            def work(side=side):
                origin = jnp.clip(me - hop if side == 1 else me + hop, 0, count - 1)
                plane(origin, 1, None, 1, 1).wait_recv()
                plane(origin, 1, halves[0], 3, 2).start()
                plane(origin, 2, None, 2, 2).wait_recv()
                plane(origin, 2, halves[1], 0, 1).start()

            pl.when(valid(hop, side) & where)(work)

    at_top = jnp.where(me == count - 1, 1, 0)
    most = (count - 1) * depth
    most_at = pl.ds(pl.multiple_of(at_top * depth, depth), most)
    last_at = pl.ds(pl.multiple_of((1 - at_top) * most, depth), depth)
    other_half = pl.ds(pl.multiple_of(other * half, half), half)

    def sequence(step):
        return jnp.where(
            step == 0,
            peers[0],
            jnp.where(step == 1, peers[1], jnp.where(step == 2, peers[2], peers[3])),
        )

    def project_most(index, start):
        seq, at = sequence(index // 2), pl.ds(pl.multiple_of((index % 2) * half, half), half)
        acc[seq, at, :] = jnp.dot(
            xbuf[seq, at, most_at], wbuf[most_at, : 4 * lanes], preferred_element_type=f32
        )
        z = lax.dot_general(
            xbuf[seq, at, :], stepx[...], (((1,), (1,)), ((), ())), preferred_element_type=f32
        )
        stbuf[seq, at, :] = jnp.maximum(z, 0.0) + jnp.log1p(jnp.exp(-jnp.abs(z)))
        return start

    def half_in(k):
        ref = xbuf.at[peers[k], other_half]
        to(ref, ref, d_send.at[k - 1], d_recv.at[k - 1], "tp", other).wait_recv()

    half_in(1)
    half_in(2)
    lax.fori_loop(0, 6, project_most, 0)
    x_in(3, x_first, 2).wait_recv()
    x_in(3, x_second, 3).wait_recv()
    across[2].start()
    take_line(3, 1, spread, hold=True)
    half_in(3)
    lax.fori_loop(6, 8, project_most, 0)
    for hop in range(3, count):
        take_line(0, hop)

    def project_state(index, carry):
        seq, at = index // 2, pl.ds(pl.multiple_of((index % 2) * half, half), half)
        y = acc[seq, at, :] + jnp.dot(
            xbuf[seq, at, last_at], wbuf[last_at, : 4 * lanes], preferred_element_type=f32
        )
        to_at = pl.ds(pl.multiple_of((index % 2) * half + 8, 8), half)
        cbuf[seq, to_at, :] = y[:, : 3 * lanes].astype(bf16).astype(f32)
        gbuf[seq, at, :] = y[:, 3 * lanes :].astype(bf16)
        return carry

    lax.fori_loop(0, 8, project_state, 0)
    low_edge, high_edge = pl.ds(0, 8), pl.ds(rows + 8, 8)
    halo = [
        to(cbuf.at[:, pl.ds(8, 8)], cbuf.at[:, high_edge], h_send.at[0], h_recv.at[0], "sp", beside[0]),
        to(cbuf.at[:, pl.ds(rows, 8)], cbuf.at[:, low_edge], h_send.at[1], h_recv.at[1], "sp", beside[1]),
    ]
    halo_in = [
        to(cbuf.at[:, low_edge], cbuf.at[:, low_edge], h_send.at[1], h_recv.at[1], "sp", beside[0]),
        to(cbuf.at[:, high_edge], cbuf.at[:, high_edge], h_send.at[0], h_recv.at[0], "sp", beside[1]),
    ]
    for side in range(2):
        pl.when(has[side])(lambda side=side: halo[side].start())
    edges = (low_edge, high_edge)
    for side in range(2):

        def clear(side=side):
            cbuf[:, edges[side], :] = jnp.zeros((4, 8, 3 * lanes), f32)

        pl.when(jnp.logical_not(has[side]))(clear)
    if count > 2:
        send_line(3, 1)
    take_line(1, 1)
    send_line(2, 0, jnp.logical_not(inner))
    send_line(4, 0, jnp.logical_not(inner))
    for copy in j_own:
        copy.wait_send()
    for k in range(1, 4):
        to(jumps, jbuf.at[peers[k]], j_send.at[k], j_recv.at[k], "fs", peers[k]).wait_recv()
    for side in range(2):
        pl.when(has[side])(lambda side=side: halo_in[side].wait_recv())

    own_cols = pl.ds(pl.multiple_of(fs * lanes, lanes), lanes)
    taps = jnp.concatenate(
        [ref[:, own_cols].astype(f32) for ref in (tap_value, tap_keys, tap_query)], axis=1
    )
    rate_lane = jnp.where(low, rate[2 * fs], rate[2 * fs + 1])
    row_id = lax.broadcasted_iota(jnp.int32, (BLOCK, lanes), 0)
    col_id = lax.broadcasted_iota(jnp.int32, (BLOCK, lanes), 1)
    lower = (col_id <= row_id).astype(f32)
    left = col_id < lanes // 2
    tap_count = taps.shape[0]
    reach = tap_count // 2
    tall = BLOCK + 16
    high = lax.Precision.HIGHEST

    def scan_block(index):
        seq, blk = index // blocks, index % blocks
        at = pl.ds(pl.multiple_of(blk * BLOCK, BLOCK), BLOCK)
        pre = cbuf[seq, pl.ds(pl.multiple_of(blk * BLOCK, BLOCK), tall), :]
        filt = jnp.zeros((BLOCK, 3 * lanes), f32)
        for tap in range(tap_count):
            moved = pre if tap == reach else pltpu.roll(pre, (reach - tap) % tall, 0)
            filt = filt + moved[8 : 8 + BLOCK] * taps[tap : tap + 1, :]
        fv, fk, fq = filt[:, :lanes], filt[:, lanes : 2 * lanes], filt[:, 2 * lanes :]
        step = stbuf[seq, at, :]
        sv = (fv * jax.nn.sigmoid(fv) * step).astype(bf16)
        sk, sq = fk.astype(bf16), fq.astype(bf16)
        jrows = jbuf[seq, :, at]
        jrow_id = lax.broadcasted_iota(jnp.int32, jrows.shape, 0)
        jrow = [
            jnp.sum(jnp.where(jrow_id == 2 * fs + r, jrows, 0.0), axis=0, keepdims=True)
            for r in range(2)
        ]
        jump = jnp.where(row_id < lanes // 2, jrow[0], jrow[1]).T
        logs = jump - rate_lane * step
        cum = jnp.dot(lower, logs, preferred_element_type=f32, precision=high)
        cum_t = cum.T
        gram = lax.dot_general(sq, sk, (((1,), (1,)), ((), ())), preferred_element_type=f32)
        key_t = sk.astype(f32).T
        near, after, before = [], [], []
        for r in range(2):
            spot = r * (lanes // 2)
            down = cum[:, spot : spot + 1]
            across_row = cum_t[spot : spot + 1, :]
            pair = (gram * jnp.exp(-jnp.abs(down - across_row))).astype(bf16)
            near.append(jnp.dot(pair, sv, preferred_element_type=f32))
            last = across_row[:, BLOCK - 1 : BLOCK]
            k_after = (key_t * jnp.exp(last - across_row)).astype(bf16)
            after.append(jnp.dot(k_after, sv, preferred_element_type=f32))
            k_before = (key_t * jnp.exp(across_row)).astype(bf16)
            before.append(jnp.dot(k_before, sv, preferred_element_type=f32))

        def store():
            sqbuf[seq, at, :] = sq
            cumbuf[seq, at, :] = cum
            nbuf[seq, at, :] = jnp.where(left, near[0], near[1])
            sabuf[index, :, :] = jnp.where(left, after[0], after[1])
            sbbuf[index, :, :] = jnp.where(left, before[0], before[1])

        return store

    def pairs_of(block):
        def body(index, carry):
            for store in [block(2 * index + k) for k in range(2)]:
                store()
            return carry

        return body

    relay_out(1, jnp.logical_not(inner))
    lax.fori_loop(0, blocks, pairs_of(scan_block), 0)
    for hop in range(2, count - 1):
        take_line(1, hop, mode="pass")
    relay_out(1, inner)
    for hop in range(2, count - 1):
        take_line(3, hop, spread)
    lax.fori_loop(blocks, 2 * blocks, pairs_of(scan_block), 0)

    if count > 2:
        take_line(2, 1, mode="pass_end")
        take_line(4, 1, mode="pass_end")

    zero_state = jnp.zeros((STATE_SIZE, lanes), f32)

    def total_of(seq, blk):
        return cumbuf[seq, blk * BLOCK + BLOCK - 8 : blk * BLOCK + BLOCK, :][7:8, :]

    def carry_states(seq, carry):
        state, so_far = zero_state, jnp.zeros((1, lanes), f32)
        for blk in range(blocks):
            added = sabuf[seq * blocks + blk, :, :]
            sabuf[seq * blocks + blk, :, :] = state
            edge[seq * blocks + blk, 0:1, :] = so_far
            total = total_of(seq, blk)
            state = state * jnp.exp(total) + added
            so_far = so_far + total
        fout[seq, :, :] = state.astype(bf16)
        edge[4 * blocks + seq, 0:1, :] = so_far
        state, so_far = zero_state, jnp.zeros((1, lanes), f32)
        for blk in range(blocks - 1, -1, -1):
            added = sbbuf[seq * blocks + blk, :, :]
            sbbuf[seq * blocks + blk, :, :] = state
            edge[seq * blocks + blk, 1:2, :] = so_far
            total = total_of(seq, blk)
            state = state * jnp.exp(total) + added
            so_far = so_far + total
        gout[seq, :, :] = state.astype(bf16)
        return carry

    lax.fori_loop(0, 4, carry_states, 0)
    chain = [
        to(gout, gin, h_send.at[2], h_recv.at[2], "sp", beside[0]),
        to(fout, fin, h_send.at[3], h_recv.at[3], "sp", beside[1]),
    ]

    def clear_forward():
        fin[...] = jnp.zeros(fin.shape, bf16)

    def clear_backward():
        gin[...] = jnp.zeros(gin.shape, bf16)

    pl.when(me == 0)(clear_forward)
    pl.when(me == count - 1)(clear_backward)
    pl.when(me == 0)(lambda: chain[1].start())
    pl.when(me == count - 1)(lambda: chain[0].start())

    def rotated(vectors):
        lane_full = lax.broadcasted_iota(jnp.int32, vectors.shape, 1)
        turned = jnp.where(
            lane_full % (2 * q4) < q4,
            pltpu.roll(vectors, HEAD_DIM - q4, 1),
            pltpu.roll(vectors, q4, 1),
        )
        return (vectors * cos_t[...] + turned * sin_t[...]).astype(bf16)

    for hop in range(2, count):
        take_line(1, hop, mode="keep")

    def project_pair(seq, carry):
        y = jnp.dot(
            xbuf[seq, :, :], wbuf[:, 4 * lanes : 6 * lanes], preferred_element_type=f32
        ).astype(bf16)
        kvbuf[seq, WINDOW : WINDOW + rows, :HEAD_DIM] = rotated(y[:, :HEAD_DIM].astype(f32))
        kvbuf[seq, WINDOW : WINDOW + rows, HEAD_DIM : 2 * HEAD_DIM] = y[:, HEAD_DIM:]
        return carry

    lax.fori_loop(0, 4, project_pair, 0)
    bottom, top = pl.ds(0, WINDOW), pl.ds(rows + WINDOW, WINDOW)
    pair_cols = pl.ds(0, 2 * HEAD_DIM)

    def kv(at):
        return kvbuf.at[:, at, pair_cols]

    low_rows, high_rows = pl.ds(WINDOW, WINDOW), pl.ds(rows, WINDOW)
    kv_edge = [
        to(kv(low_rows), kv(top), h_send.at[4], h_recv.at[4], "sp", beside[0]),
        to(kv(high_rows), kv(bottom), h_send.at[5], h_recv.at[5], "sp", beside[1]),
    ]
    kv_in = [
        to(kv(bottom), kv(bottom), h_send.at[5], h_recv.at[5], "sp", beside[0]),
        to(kv(top), kv(top), h_send.at[4], h_recv.at[4], "sp", beside[1]),
    ]
    bands = (bottom, top)
    for side in range(2):

        def clear_band(side=side):
            kvbuf[:, bands[side], : 2 * HEAD_DIM] = jnp.zeros((4, WINDOW, 2 * HEAD_DIM), bf16)

        pl.when(jnp.logical_not(has[side]))(clear_band)

    def forward_step():
        to(fin, fin, h_send.at[3], h_recv.at[3], "sp", beside[0]).wait_recv()

        def add(seq, carry):
            passed = jnp.exp(edge[4 * blocks + seq, 0:1, :])
            fout[seq, :, :] = (
                fout[seq, :, :].astype(f32) + passed * fin[seq, :, :].astype(f32)
            ).astype(bf16)
            return carry

        def pass_on():
            lax.fori_loop(0, 4, add, 0)
            chain[1].start()

        pl.when(has[1])(pass_on)

    def backward_step():
        to(gin, gin, h_send.at[2], h_recv.at[2], "sp", beside[1]).wait_recv()

        def add(seq, carry):
            passed = jnp.exp(edge[4 * blocks + seq, 0:1, :])
            gout[seq, :, :] = (
                gout[seq, :, :].astype(f32) + passed * gin[seq, :, :].astype(f32)
            ).astype(bf16)
            return carry

        def pass_on():
            lax.fori_loop(0, 4, add, 0)
            chain[0].start()

        pl.when(has[0])(pass_on)

    near_first = 2 * me < count
    pl.when(inner & near_first)(forward_step)
    pl.when(inner)(backward_step)
    pl.when(inner & jnp.logical_not(near_first))(forward_step)
    send_line(2, 0, inner)
    if count > 2:
        take_line(2, 1, mode="pass_rest")
    send_line(4, 0, inner)
    for hop in range(2, count - 1):
        take_line(2, hop, mode="pass")
    if count > 2:
        take_line(4, 1, mode="pass_rest")
    for hop in range(2, count - 1):
        take_line(4, hop, mode="pass")
    for side in range(2):
        pl.when(has[side])(lambda side=side: kv_edge[side].start())
    for hop in range(2, count - 1):
        relay_out(hop)
    if count > 2:
        take_line(3, count - 1, spread)

    inner_rows = pl.ds(BLOCK, rows - 2 * BLOCK)

    def edge_block(second):
        return jnp.where(at_top == 1 - second, blocks - 1, 0)

    def edge_rows(second):
        return pl.ds(pl.multiple_of(edge_block(second) * BLOCK, BLOCK), BLOCK)

    parts = (
        (pl.ds(0, rows), pl.ds(0, lanes)),
        (inner_rows, pl.ds(lanes, HEAD_DIM)),
        (inner_rows, pl.ds(lanes + HEAD_DIM, HEAD_DIM)),
        (edge_rows(0), pl.ds(lanes, 2 * HEAD_DIM)),
        (edge_rows(1), pl.ds(lanes, 2 * HEAD_DIM)),
    )

    def swap(k, part):
        slot = part * 4 + k
        return to(
            mixs.at[(peers[k], *parts[part])],
            mixr.at[(fs, *parts[part])],
            m_send.at[slot],
            m_recv.at[slot],
            "fs",
            peers[k],
        )

    def swap_in(k, part):
        ref, slot = mixr.at[(peers[k], *parts[part])], part * 4 + k
        return to(ref, ref, m_send.at[slot], m_recv.at[slot], "fs", peers[k])

    pl.when(has[0] & jnp.logical_not(has[1]))(forward_step)
    pl.when(has[1] & jnp.logical_not(has[0]))(backward_step)
    gain_row = gain[:, own_cols]

    def split_dot(a, b):
        top_bits = b.astype(bf16)
        rest = (b - top_bits.astype(f32)).astype(bf16)
        return jnp.dot(a, top_bits, preferred_element_type=f32) + jnp.dot(
            a, rest, preferred_element_type=f32
        )

    def finish_block(index):
        seq, blk = index // blocks, index % blocks
        at = pl.ds(pl.multiple_of(blk * BLOCK, BLOCK), BLOCK)
        ahead = sabuf[index, :, :] + jnp.exp(edge[index, 0:1, :]) * fin[seq, :, :].astype(f32)
        behind = sbbuf[index, :, :] + jnp.exp(edge[index, 1:2, :]) * gin[seq, :, :].astype(f32)
        sq = sqbuf[seq, at, :]
        cum = cumbuf[seq, at, :]
        total = cum[BLOCK - 1 : BLOCK, :]
        mixed = (
            nbuf[seq, at, :]
            + jnp.exp(cum) * split_dot(sq, ahead)
            + jnp.exp(total - cum) * split_dot(sq, behind)
        )
        g = gbuf[seq, at, :].astype(f32)
        gated = mixed * (g * jax.nn.sigmoid(g))
        square = gated * gated
        first = jnp.sum(jnp.where(left, square, 0.0), axis=-1, keepdims=True)
        second = jnp.sum(jnp.where(left, 0.0, square), axis=-1, keepdims=True)
        mean = jnp.where(left, first, second) * (2.0 / lanes)
        mix = (gated * lax.rsqrt(mean + 1e-06) * gain_row).astype(bf16)

        def store():
            mixs[seq, at, :lanes] = mix

        return store

    lax.fori_loop(0, 2 * blocks, pairs_of(finish_block), 0)
    for k in (3, 1, 2):
        swap(k, 0).start()


    def query_cols(r):
        return slice((6 + r) * lanes, (7 + r) * lanes)

    def head_cols(r):
        return slice(r * HEAD_DIM, (r + 1) * HEAD_DIM)

    near_count = max(1, count // 2)
    near_at = pl.ds(
        pl.multiple_of(at_top * (count - near_count) * depth, depth), near_count * depth
    )
    far_at = pl.ds(
        pl.multiple_of((1 - at_top) * near_count * depth, depth), (count - near_count) * depth
    )
    query_parts = ((most_at, last_at), (near_at, far_at))

    def query_first(r):
        at = query_parts[r][0]

        def body(seq, carry):
            acc[seq, :, head_cols(r)] = jnp.dot(
                xbuf[seq, :, at], wbuf[at, query_cols(r)], preferred_element_type=f32
            )
            return carry

        lax.fori_loop(0, 4, body, 0)

    def query_rest(r):
        at = query_parts[r][1]

        def body(seq, carry):
            y = acc[seq, :, head_cols(r)] + jnp.dot(
                xbuf[seq, :, at], wbuf[at, query_cols(r)], preferred_element_type=f32
            )
            qbuf[seq, :, head_cols(r)] = rotated(y.astype(bf16).astype(f32))
            return carry

        lax.fori_loop(0, 4, body, 0)

    for hop in range(1, count - 1):
        take_line(2, hop, mode="keep")
    query_first(0)
    if count > 2:
        relay_out(count - 1, tp == 1)
    take_line(2, count - 1, mode="keep")
    query_rest(0)
    band = 3 * WINDOW
    log2e = math.log2(math.e)
    def sink_rows(heads):
        row = lax.broadcasted_iota(jnp.int32, (len(heads) * WINDOW, 1), 0)
        first = sink[2 * fs + heads[0]]
        return log2e * jnp.where(row < WINDOW, first, sink[2 * fs + heads[-1]])

    floors = {heads: sink_rows(heads) for heads in ((0,), (1,), (0, 1))}

    def attend_block(seq, blk, heads):
        at = pl.ds(pl.multiple_of(blk * WINDOW, WINDOW), WINDOW)
        wide = pl.ds(pl.multiple_of(blk * WINDOW, WINDOW), band)
        q = jnp.concatenate([qbuf[seq, at, head_cols(r)] for r in heads], axis=0)
        s = lax.dot_general(
            q,
            kvbuf[seq, wide, :HEAD_DIM],
            (((1,), (1,)), ((), ())),
            preferred_element_type=f32,
        )
        kind = jnp.where(blk == 0, 0, jnp.where(blk == blocks - 1, 2, 1))
        floor = floors[heads]
        s = s * (HEAD_DIM ** (-0.5) * log2e) + bias[kind, : len(heads) * WINDOW, :]
        m = jnp.maximum(jnp.max(s, axis=-1, keepdims=True), floor)
        w = jnp.exp2(s - m).astype(bf16)
        y = jnp.dot(w, kvbuf[seq, wide, HEAD_DIM:], preferred_element_type=f32)
        total = jnp.exp2(floor - m) + y[:, HEAD_DIM:]
        o = (y[:, :HEAD_DIM] / total).astype(bf16)

        def store():
            for index, r in enumerate(heads):
                mixs[seq, at, lanes + r * HEAD_DIM : lanes + (r + 1) * HEAD_DIM] = o[
                    index * WINDOW : (index + 1) * WINDOW
                ]

        return store

    def far_first(step):
        return jnp.where(
            step == 0,
            peers[3],
            jnp.where(step == 1, peers[1], jnp.where(step == 2, peers[2], peers[0])),
        )

    def attend_inner(r):
        def each(step, carry):
            seq = far_first(step)

            def body(index, carry):
                for store in [attend_block(seq, 1 + 2 * index + k, (r,)) for k in range(2)]:
                    store()
                return carry

            lax.fori_loop(0, blocks // 2 - 1, body, 0)
            for index, k in enumerate((3, 1, 2)):
                pl.when(step == index)(lambda k=k: swap(k, 1 + r).start())
            return carry

        lax.fori_loop(0, 4, each, 0)

    attend_inner(0)
    if count > 2:
        relay_out(count - 1, tp == 0)
    for hop in range(1, near_count):
        take_line(4, hop, mode="keep")
    query_first(1)
    for hop in range(near_count, count):
        take_line(4, hop, mode="keep")
    query_rest(1)
    attend_inner(1)
    def edges_in(where):
        for side in range(2):
            pl.when(has[side] & where)(lambda side=side: kv_in[side].wait_recv())

    def attend_edges(second):
        def body(index, carry):
            steps = [2 * index + k for k in range(2)]
            seqs = [far_first(step) for step in steps]
            for store in [attend_block(seq, edge_block(second), (0, 1)) for seq in seqs]:
                store()
            for step, k in enumerate((3, 1, 2)):
                pl.when(index == step // 2)(lambda k=k: swap(k, 3 + second).start())
            return carry

        lax.fori_loop(0, 2, body, 0)

    edges_in(inner)
    attend_edges(0)
    edges_in(jnp.logical_not(inner))
    attend_edges(1)

    cols = w_sout.shape[1]

    def out_in(origin):
        def work():
            plane(origin, 3, halves[0], 3, 2).wait_recv()
            plane(origin, 3, halves[1], 0, 1).wait_recv()

        pl.when(origin != me)(work)

    def columns(origin):
        return pl.ds(pl.multiple_of(origin * cols, cols), cols)

    def trade(origin):
        return to(
            psend.at[origin],
            out_other.at[:, columns(origin)],
            p_send.at[origin],
            p_recv.at[origin],
            "tp",
            other,
        )

    def store_own(origin):
        return pltpu.make_async_copy(
            pown.at[origin], out_own.at[:, columns(origin)], loc_sem.at[17 + origin]
        )

    def hand_over(origin, totals):
        psend[origin, :, :] = totals[0].astype(bf16)
        trade(origin).start()
        pown[origin, :, :] = totals[1].astype(bf16)
        store_own(origin).start()

    row_halves = (other_half, own_half)

    def first_product(origin, carry):
        out_in(origin)
        weights = jnp.concatenate(
            [wob[origin, fs, :, :]] + [wob[origin, peers[k], :lanes, :] for k in range(1, 4)], axis=0
        )
        for at in row_halves:
            mix = jnp.concatenate(
                [mixs[fs, at, :]] + [mixr[peers[k], at, :lanes] for k in range(1, 4)], axis=1
            )
            oacc[origin, at, :] = jnp.dot(mix, weights, preferred_element_type=f32)
        return carry

    def add_parts(ks, last):
        def body(origin, carry):
            weights = jnp.concatenate([wob[origin, peers[k], lanes:, :] for k in ks], axis=0)
            totals = [
                oacc[origin, at, :]
                + jnp.dot(
                    jnp.concatenate([mixr[peers[k], at, lanes:] for k in ks], axis=1),
                    weights,
                    preferred_element_type=f32,
                )
                for at in row_halves
            ]
            if last:
                hand_over(origin, totals)
            else:
                for total, at in zip(totals, row_halves):
                    oacc[origin, at, :] = total
            return carry

        lax.fori_loop(0, count, body, 0)

    for k in (3, 1, 2):
        swap_in(k, 0).wait_recv()
    lax.fori_loop(0, count, first_product, 0)
    for ks in ((3,), (1, 2)):
        for k in ks:
            for part in range(1, 5):
                swap_in(k, part).wait_recv()
        add_parts(ks, 2 in ks)

    for origin in range(count):
        trade(origin).wait_recv()
        store_own(origin).wait()

    for piece in range(pieces):
        for hop in range(count - 1):
            for side in range(2):
                pl.when(has[side] & valid(hop, side))(
                    lambda piece=piece, hop=hop, side=side: line(piece, hop, side).wait_send()
                )
    for copy in x_own + relay + across:
        copy.wait_send()
    for side in range(2):
        pl.when(has[side])(lambda side=side: halo[side].wait_send())
        pl.when(has[side])(lambda side=side: chain[side].wait_send())
        pl.when(has[side])(lambda side=side: kv_edge[side].wait_send())
    for k in range(1, 4):
        for part in range(5):
            swap(k, part).wait_send()

    def left_plane(origin, carry):
        def work():
            plane(origin, 0, None, 1, 1).wait_send()
            plane(origin, 0, None, 2, 2).wait_send()
            plane(origin, 1, halves[0], 3, 2).wait_send()
            plane(origin, 2, halves[1], 0, 1).wait_send()

        pl.when(origin != me)(work)
        return carry

    lax.fori_loop(0, count, left_plane, 0)
    for origin in range(count):
        trade(origin).wait_send()


def fused_shards(
    tokens,
    norm_gain,
    state_gate,
    state_value,
    state_keys,
    state_query,
    state_step,
    state_rate,
    state_jumps,
    state_gain,
    filter_value,
    filter_keys,
    filter_query,
    window_query,
    window_keys,
    window_values,
    window_sink,
    state_output,
    window_output,
):
    count = lax.axis_size("sp")
    rows, width = tokens.shape
    lanes = STATE_SIZE
    blocks = rows // BLOCK
    depth = state_value.shape[0]
    cols = state_output.shape[1]
    out_rows = (state_output.shape[0] + window_output.shape[0]) // 4
    f32, bf16 = jnp.float32, jnp.bfloat16
    vmem = pltpu.VMEM
    dma = pltpu.SemaphoreType.DMA
    hbm = pl.BlockSpec(memory_space=pl.ANY)
    scalar = pl.BlockSpec(memory_space=pltpu.SMEM)
    jumps = state_jumps.T
    half = rows // 2
    own, others = pl.pallas_call(
        functools.partial(fused_kernel, count),
        out_shape=[jax.ShapeDtypeStruct((half, width), bf16)] * 2,
        in_specs=[hbm] * 10
        + [hbm, hbm, scalar, hbm, hbm, hbm, hbm, hbm, scalar],
        out_specs=[hbm, hbm],
        scratch_shapes=[
            vmem((1, width), f32),
            vmem(jumps.shape, f32),
            vmem((1,) + state_gain.shape, f32),
            vmem(filter_value.shape, bf16),
            vmem(filter_keys.shape, bf16),
            vmem(filter_query.shape, bf16),
            vmem((rows, width), bf16),
            vmem((4, rows, width), bf16),
            vmem((count * depth, 8 * lanes), bf16),
            vmem((count, 4, out_rows, cols), bf16),
            vmem(state_step.shape[::-1], bf16),
            vmem((lanes, width), bf16),
            vmem((rows, lanes), f32),
            vmem((rows, lanes), f32),
            vmem((4,) + jumps.shape, f32),
            vmem((3, 2 * WINDOW, 3 * WINDOW), f32),
            vmem((4, rows, 4 * lanes), f32),
            vmem((count, rows, cols), f32),
            vmem((4, rows + 16, 3 * lanes), f32),
            vmem((4, rows, lanes), bf16),
            vmem((4, rows, lanes), f32),
            vmem((4, rows, lanes), f32),
            vmem((4 * blocks, STATE_SIZE, lanes), f32),
            vmem((4 * blocks, STATE_SIZE, lanes), f32),
            vmem((4, rows, lanes), f32),
            vmem((4 * blocks + 4, 8, lanes), f32),
            vmem((4, rows, lanes), bf16),
            vmem((4, STATE_SIZE, lanes), bf16),
            vmem((4, STATE_SIZE, lanes), bf16),
            vmem((4, STATE_SIZE, lanes), bf16),
            vmem((4, STATE_SIZE, lanes), bf16),
            vmem((4, rows + 2 * WINDOW, 3 * HEAD_DIM), bf16),
            vmem((4, rows, 2 * HEAD_DIM), bf16),
            vmem((4, rows, 3 * lanes), bf16),
            vmem((4, rows, 3 * lanes), bf16),
            vmem((count, half, cols), bf16),
            vmem((count, half, cols), bf16),
            dma((23 + count,)),
            dma((10 * (count - 1),)),
            dma((10 * (count - 1),)),
            dma((4,)),
            dma((4,)),
            dma((3,)),
            dma((3,)),
            dma((4,)),
            dma((4,)),
            dma((6,)),
            dma((6,)),
            dma((20,)),
            dma((20,)),
            dma((4 * count,)),
            dma((4 * count,)),
            dma((count,)),
            dma((count,)),
        ],
        compiler_params=pltpu.CompilerParams(
            collective_id=0, has_side_effects=True, vmem_limit_bytes=62 * 1024 * 1024
        ),
        name="fused_layer",
    )(
        tokens,
        state_value,
        state_keys,
        state_query,
        state_gate,
        window_keys,
        window_values,
        window_query,
        state_output,
        window_output,
        norm_gain.reshape(1, -1),
        state_step.T,
        state_rate,
        jumps,
        state_gain.reshape(1, -1),
        filter_value,
        filter_keys,
        filter_query,
        window_sink,
    )
    return (own.astype(f32) + others.astype(f32)).astype(bf16)


def solution(mesh):
    placed = (
        P(("fs", "sp"), None),
        P(),
        P("sp", "tp"),
        P("sp", "tp"),
        P("sp", "tp"),
        P("sp", "tp"),
        P(),
        P("tp"),
        P(("fs", "sp"), "tp"),
        P("tp"),
        P(None, "tp"),
        P(None, "tp"),
        P(None, "tp"),
        P("sp", "tp"),
        P("sp", "tp"),
        P("sp", "tp"),
        P("tp"),
        P("tp", "sp"),
        P("tp", "sp"),
    )
    def plan(*args):
        return (fused_shards if fits(*args) else shards)(*args)

    return jax.shard_map(
        plan, mesh=mesh, in_specs=placed, out_specs=P(("fs", "sp", "tp"), None), check_vma=False
    )
```

```python
import functools
import math

import jax
import jax.numpy as jnp
from jax import lax
from jax.experimental import pallas as pl
from jax.experimental.pallas import tpu as pltpu
from jax.sharding import PartitionSpec as P

STATE_SIZE = 128
HEAD_DIM = 128
WINDOW = 128
BLOCK = 128
GRID_WIDTH = 64


def extended(cells, sides, width):
    for axis, dim in sides:
        count = lax.axis_size(axis)
        ends = count - 1
        head = lax.slice_in_dim(cells, 0, width, axis=dim)
        tail = lax.slice_in_dim(cells, cells.shape[dim] - width, cells.shape[dim], axis=dim)
        cells = jnp.concatenate(
            [
                lax.ppermute(tail, axis, [(i, (i + 1) % count) for i in range(ends)]),
                cells,
                lax.ppermute(head, axis, [((i + 1) % count, i) for i in range(ends)]),
            ],
            axis=dim,
        )
    return cells


def rotate_grid(vectors, positions, grid_width):
    head_dim = vectors.shape[-1]
    quarter = head_dim // 4
    half_dim = head_dim // 2
    inverse = 10000.0 ** (-jnp.arange(quarter, dtype=jnp.float32) / quarter)
    grid_row = (positions // grid_width).astype(jnp.float32)
    grid_col = (positions % grid_width).astype(jnp.float32)
    angle_row = grid_row[:, None] * inverse[None, :]
    angle_col = grid_col[:, None] * inverse[None, :]
    angles = jnp.concatenate([angle_row, angle_row, angle_col, angle_col], axis=-1)[:, None, :]
    first_half = vectors[..., :half_dim]
    second = vectors[..., half_dim:]
    turned = jnp.concatenate(
        [
            -first_half[..., quarter:],
            first_half[..., :quarter],
            -second[..., quarter:],
            second[..., :quarter],
        ],
        axis=-1,
    )
    return (
        vectors.astype(jnp.float32) * jnp.cos(angles) + turned.astype(jnp.float32) * jnp.sin(angles)
    ).astype(jnp.bfloat16)


def window_attend(query_rows, keys_pad, values_pad, sink_logits, key_start, total_len, window):
    row_count, query_heads, head_dim = query_rows.shape
    kv_heads = keys_pad.shape[1]
    group_size = query_heads // kv_heads
    block_count = row_count // window
    query_blocks = query_rows.reshape(block_count, window, kv_heads, group_size, head_dim)
    key_split = keys_pad.reshape(block_count + 2, window, kv_heads, head_dim)
    value_split = values_pad.reshape(block_count + 2, window, kv_heads, head_dim)
    key_band = jnp.concatenate([key_split[:-2], key_split[1:-1], key_split[2:]], axis=1)
    value_band = jnp.concatenate([value_split[:-2], value_split[1:-1], value_split[2:]], axis=1)
    scores = jnp.einsum(
        "kihgd,kjhd->khgij", query_blocks, key_band, preferred_element_type=jnp.float32
    ) * head_dim ** (-0.5)
    query_pos = jnp.arange(window)[:, None]
    band_pos = jnp.arange(3 * window)[None, :]
    within = jnp.abs(band_pos - window - query_pos) <= window
    key_pos = (
        key_start + jnp.arange(block_count)[:, None] * window + jnp.arange(3 * window)[None, :]
    )
    inside = (key_pos >= 0) & (key_pos < total_len)
    valid_pair = (within[None] & inside[:, None, :])[:, None, None]
    sink_logit = sink_logits.reshape(kv_heads, group_size)[None, :, :, None, None]
    masked = jnp.where(valid_pair, scores, -1e30)
    ceiling = jnp.maximum(jnp.max(masked, axis=-1, keepdims=True), sink_logit)
    weights = jnp.where(valid_pair, jnp.exp(masked - ceiling), 0.0)
    denominator = jnp.exp(sink_logit - ceiling) + jnp.sum(weights, axis=-1, keepdims=True)
    weights_bf = (weights / denominator).astype(jnp.bfloat16)
    mixed_rows = jnp.einsum(
        "khgij,kjhd->kihgd", weights_bf, value_band, preferred_element_type=jnp.float32
    )
    return mixed_rows.reshape(row_count, query_heads * head_dim).astype(jnp.bfloat16)


def block_terms(query_rows, key_rows, value_rows, log_rows, block_len):
    row_count, group_count, state_size = query_rows.shape
    head_ratio, head_dim = (value_rows.shape[2], value_rows.shape[3])
    block_count = row_count // block_len
    query_blocks = query_rows.reshape(block_count, block_len, group_count, state_size)
    key_blocks = key_rows.reshape(block_count, block_len, group_count, state_size)
    value_blocks = value_rows.reshape(block_count, block_len, group_count, head_ratio, head_dim)
    decay_cum = jnp.cumsum(
        log_rows.reshape(block_count, block_len, group_count, head_ratio), axis=1
    )
    decay_total = decay_cum[:, -1]
    gram_block = jnp.einsum(
        "kign,kjgn->kgij", query_blocks, key_blocks, preferred_element_type=jnp.float32
    )
    cum_heads = jnp.moveaxis(decay_cum, 1, 3)
    distance = jnp.abs(cum_heads[..., :, None] - cum_heads[..., None, :])
    pair_weight = (gram_block[:, :, None] * jnp.exp(-distance)).astype(jnp.bfloat16)
    near_terms = jnp.einsum(
        "kgrij,kjgrp->kigrp", pair_weight, value_blocks, preferred_element_type=jnp.float32
    )
    keys_after = (
        key_blocks[:, :, :, None, :] * jnp.exp(decay_total[:, None] - decay_cum)[..., None]
    ).astype(jnp.bfloat16)
    keys_before = (key_blocks[:, :, :, None, :] * jnp.exp(decay_cum)[..., None]).astype(
        jnp.bfloat16
    )
    state_after = jnp.einsum(
        "kjgrn,kjgrp->kgrnp", keys_after, value_blocks, preferred_element_type=jnp.float32
    )
    state_before = jnp.einsum(
        "kjgrn,kjgrp->kgrnp", keys_before, value_blocks, preferred_element_type=jnp.float32
    )
    before = jnp.cumsum(decay_total, axis=0) - decay_total
    overall = jnp.sum(decay_total, axis=0)
    after_sum = overall[None] - before - decay_total
    block_order = jnp.arange(block_count)
    earlier_mask = (block_order[None, :] < block_order[:, None])[:, :, None, None]
    later_mask = (block_order[None, :] > block_order[:, None])[:, :, None, None]
    gap_fwd = before[:, None] - before[None, :] - decay_total[None, :]
    gap_bwd = before[None, :] - before[:, None] - decay_total[:, None]
    weight_fwd = jnp.where(earlier_mask, jnp.exp(jnp.minimum(gap_fwd, 0.0)), 0.0)
    weight_bwd = jnp.where(later_mask, jnp.exp(jnp.minimum(gap_bwd, 0.0)), 0.0)
    carried_fwd = jnp.einsum(
        "abgr,bgrnp->agrnp", weight_fwd, state_after, precision=lax.Precision.HIGHEST
    )
    carried_bwd = jnp.einsum(
        "abgr,bgrnp->agrnp", weight_bwd, state_before, precision=lax.Precision.HIGHEST
    )
    summary_fwd = jnp.einsum(
        "agr,agrnp->grnp", jnp.exp(after_sum), state_after, precision=lax.Precision.HIGHEST
    )
    summary_bwd = jnp.einsum(
        "agr,agrnp->grnp", jnp.exp(before), state_before, precision=lax.Precision.HIGHEST
    )
    pieces = (
        near_terms,
        carried_fwd,
        carried_bwd,
        decay_cum,
        decay_total,
        before,
        after_sum,
        query_blocks,
    )
    return (pieces, (summary_fwd, summary_bwd, overall))


def finish_terms(pieces, incoming_fwd, incoming_bwd):
    (
        near_terms,
        carried_fwd,
        carried_bwd,
        decay_cum,
        decay_total,
        before,
        after_sum,
        query_blocks,
    ) = pieces
    total_fwd = carried_fwd + jnp.exp(before)[..., None, None] * incoming_fwd[None]
    total_bwd = carried_bwd + jnp.exp(after_sum)[..., None, None] * incoming_bwd[None]
    query_wide = query_blocks.astype(jnp.float32)
    read_fwd = jnp.einsum(
        "kign,kgrnp->kigrp", query_wide, total_fwd, precision=lax.Precision.HIGHEST
    )
    read_bwd = jnp.einsum(
        "kign,kgrnp->kigrp", query_wide, total_bwd, precision=lax.Precision.HIGHEST
    )
    combined = (
        near_terms
        + jnp.exp(decay_cum)[..., None] * read_fwd
        + jnp.exp(decay_total[:, None] - decay_cum)[..., None] * read_bwd
    )
    block_count, block_len, group_count, head_ratio, head_dim = combined.shape
    return combined.reshape(block_count * block_len, group_count, head_ratio, head_dim)


def combine_all(gathered_states, own_index):
    after_all, before_all, logs_all = gathered_states
    device_count = logs_all.shape[0]
    cum_incl = jnp.cumsum(logs_all, axis=0)
    cum_excl = cum_incl - logs_all
    device_order = jnp.arange(device_count)
    picker = (device_order == own_index).astype(jnp.float32)[:, None, None]
    own_incl = jnp.sum(picker * cum_incl, axis=0)
    own_excl = jnp.sum(picker * cum_excl, axis=0)
    lower_mask = (device_order < own_index)[:, None, None]
    higher_mask = (device_order > own_index)[:, None, None]
    weight_fwd = jnp.where(lower_mask, jnp.exp(jnp.minimum(own_excl[None] - cum_incl, 0.0)), 0.0)
    weight_bwd = jnp.where(higher_mask, jnp.exp(jnp.minimum(cum_excl - own_incl[None], 0.0)), 0.0)
    incoming_fwd = jnp.einsum(
        "dgr,dgrnp->grnp", weight_fwd, after_all, precision=lax.Precision.HIGHEST
    )
    incoming_bwd = jnp.einsum(
        "dgr,dgrnp->grnp", weight_bwd, before_all, precision=lax.Precision.HIGHEST
    )
    return (incoming_fwd, incoming_bwd)


def shards(
    tokens,
    norm_gain,
    state_gate,
    state_value,
    state_keys,
    state_query,
    state_step,
    state_rate,
    state_jumps,
    state_gain,
    filter_value,
    filter_keys,
    filter_query,
    window_query,
    window_keys,
    window_values,
    window_sink,
    state_output,
    window_output,
):
    row_count = tokens.shape[0]
    rows_wide = tokens.astype(jnp.float32)
    normed = (
        rows_wide
        * lax.rsqrt(jnp.mean(rows_wide * rows_wide, axis=-1, keepdims=True) + 1e-06)
        * norm_gain
    ).astype(jnp.bfloat16)
    gathered = (
        lax.all_gather(state_gate, "sp", axis=0, tiled=True),
        lax.all_gather(state_value, "sp", axis=0, tiled=True),
        lax.all_gather(state_keys, "sp", axis=0, tiled=True),
        lax.all_gather(state_query, "sp", axis=0, tiled=True),
        lax.all_gather(window_query, "sp", axis=0, tiled=True),
        lax.all_gather(window_keys, "sp", axis=0, tiled=True),
        lax.all_gather(window_values, "sp", axis=0, tiled=True),
        lax.all_gather(state_output, "sp", axis=1, tiled=True),
        lax.all_gather(window_output, "sp", axis=1, tiled=True),
    )
    projected = [
        jnp.dot(normed, matrix, preferred_element_type=jnp.float32) for matrix in gathered[:7]
    ]
    out_state = gathered[7]
    out_window = gathered[8]
    gate_rows, value_pre, keys_pre, query_pre, query_raw, keys_raw, values_rows = [
        result.astype(jnp.bfloat16) for result in projected
    ]
    head_local = state_rate.shape[0]
    group_local = keys_pre.shape[1] // STATE_SIZE
    head_dim = value_pre.shape[1] // head_local
    head_ratio = head_local // group_local
    step_cols = lax.dynamic_slice_in_dim(
        state_step, lax.axis_index("tp") * head_local, head_local, 1
    )
    step_rows = jax.nn.softplus(jnp.dot(normed, step_cols, preferred_element_type=jnp.float32))
    log_decay = -state_rate[None, :] * step_rows + state_jumps
    half_width = filter_value.shape[0] // 2
    stacked = jnp.concatenate([value_pre, keys_pre, query_pre], axis=-1)
    padded = extended(stacked, (("sp", 0),), half_width)
    filters = jnp.concatenate([filter_value, filter_keys, filter_query], axis=-1).astype(
        jnp.float32
    )
    filtered = jnp.zeros(stacked.shape, jnp.float32)
    for offset in range(filters.shape[0]):
        filtered = (
            filtered + padded[offset : offset + row_count].astype(jnp.float32) * filters[offset]
        )
    value_cols = value_pre.shape[1]
    key_cols = keys_pre.shape[1]
    inner_rows = (
        jax.nn.silu(filtered[:, :value_cols]).reshape(row_count, head_local, head_dim)
        * step_rows[..., None]
    )
    scan_values = inner_rows.astype(jnp.bfloat16).reshape(
        row_count, group_local, head_ratio, head_dim
    )
    scan_keys = (
        filtered[:, value_cols : value_cols + key_cols]
        .astype(jnp.bfloat16)
        .reshape(row_count, group_local, STATE_SIZE)
    )
    scan_query = (
        filtered[:, value_cols + key_cols :]
        .astype(jnp.bfloat16)
        .reshape(row_count, group_local, STATE_SIZE)
    )
    pieces, summaries = block_terms(
        scan_query,
        scan_keys,
        scan_values,
        log_decay.reshape(row_count, group_local, head_ratio),
        BLOCK,
    )
    summary_fwd, summary_bwd, overall = summaries
    gathered_states = (
        lax.all_gather(summary_fwd[None].astype(jnp.bfloat16), "sp", axis=0, tiled=True).astype(
            jnp.float32
        ),
        lax.all_gather(summary_bwd[None].astype(jnp.bfloat16), "sp", axis=0, tiled=True).astype(
            jnp.float32
        ),
        lax.all_gather(overall[None].astype(jnp.bfloat16), "sp", axis=0, tiled=True).astype(
            jnp.float32
        ),
    )
    incoming_fwd, incoming_bwd = combine_all(gathered_states, lax.axis_index("sp"))
    scan_out = finish_terms(pieces, incoming_fwd, incoming_bwd).reshape(
        row_count, head_local * head_dim
    )
    gated_rows = scan_out * jax.nn.silu(gate_rows.astype(jnp.float32))
    per_head = gated_rows.reshape(row_count, head_local, head_dim)
    state_mix = (
        (
            per_head
            * lax.rsqrt(jnp.mean(per_head * per_head, axis=-1, keepdims=True) + 1e-06)
            * state_gain.reshape(head_local, head_dim)
        )
        .astype(jnp.bfloat16)
        .reshape(row_count, head_local * head_dim)
    )
    query_heads = window_sink.shape[0]
    kv_heads = keys_raw.shape[1] // HEAD_DIM
    kv_width = kv_heads * HEAD_DIM
    positions = lax.axis_index("sp") * row_count + jnp.arange(row_count, dtype=jnp.int32)
    query_rot = rotate_grid(
        query_raw.reshape(row_count, query_heads, HEAD_DIM), positions, GRID_WIDTH
    )
    keys_rot = rotate_grid(keys_raw.reshape(row_count, kv_heads, HEAD_DIM), positions, GRID_WIDTH)
    pair_rows = jnp.concatenate([keys_rot.reshape(row_count, kv_width), values_rows], axis=-1)
    padded_pair = extended(pair_rows, (("sp", 0),), WINDOW)
    keys_pad = padded_pair[:, :kv_width].reshape(-1, kv_heads, HEAD_DIM)
    values_pad = padded_pair[:, kv_width:].reshape(-1, kv_heads, HEAD_DIM)
    window_mix = window_attend(
        query_rot,
        keys_pad,
        values_pad,
        window_sink,
        lax.axis_index("sp") * row_count - WINDOW,
        lax.axis_size("sp") * row_count,
        WINDOW,
    )
    return lax.psum_scatter(
        (
            jnp.dot(state_mix, out_state, preferred_element_type=jnp.float32)
            + jnp.dot(window_mix, out_window, preferred_element_type=jnp.float32)
        ).astype(jnp.bfloat16),
        "tp",
        scatter_dimension=0,
        tiled=True,
    )


def fits(*args):
    tokens, state_value, state_keys, state_rate = args[0], args[3], args[4], args[7]
    window_query, window_keys, window_sink = args[13], args[14], args[16]
    parts = lax.axis_size("fs")
    heads = state_rate.shape[0]
    return (
        parts == 4
        and lax.axis_size("tp") == 2
        and lax.axis_size("sp") > 1
        and tokens.shape[0] % (4 * BLOCK) == 0
        and state_keys.shape[1] == parts * STATE_SIZE
        and state_value.shape[1] == parts * STATE_SIZE
        and heads == 2 * parts
        and window_keys.shape[1] == parts * HEAD_DIM
        and window_query.shape[1] == 2 * parts * HEAD_DIM
        and window_sink.shape[0] == 2 * parts
    )


def fused_kernel(
    count,
    tokens,
    w_value,
    w_keys,
    w_query,
    w_gate,
    w_wkeys,
    w_wvalues,
    w_wquery,
    w_sout,
    w_wout,
    norm_gain_in,
    step_w,
    rate,
    jumps_in,
    gain_in,
    tap_value_in,
    tap_keys_in,
    tap_query_in,
    sink,
    out_own,
    out_other,
    norm_gain,
    jumps,
    gain,
    tap_value,
    tap_keys,
    tap_query,
    tbuf,
    xbuf,
    wbuf,
    wob,
    stepw,
    stepx,
    cos_t,
    sin_t,
    jbuf,
    bias,
    acc,
    oacc,
    cbuf,
    gbuf,
    stbuf,
    nbuf,
    sabuf,
    sbbuf,
    cumbuf,
    edge,
    sqbuf,
    fin,
    gin,
    fout,
    gout,
    kvbuf,
    qbuf,
    mixs,
    mixr,
    psend,
    pown,
    loc_sem,
    z_send,
    z_recv,
    x_send,
    x_recv,
    d_send,
    d_recv,
    j_send,
    j_recv,
    h_send,
    h_recv,
    m_send,
    m_recv,
    o_send,
    o_recv,
    p_send,
    p_recv,
):
    f32, bf16 = jnp.float32, jnp.bfloat16
    me, fs, tp = lax.axis_index("sp"), lax.axis_index("fs"), lax.axis_index("tp")
    rows, width = tokens.shape
    depth = w_value.shape[0]
    half = rows // 2
    quarter = half // 2
    blocks = rows // BLOCK
    lanes = STATE_SIZE
    has = [me > 0, me < count - 1]
    beside = [jnp.maximum(me - 1, 0), jnp.minimum(me + 1, count - 1)]
    peers = [fs, fs + 1 - 2 * (fs % 2), fs + 2 - 4 * (fs // 2), 3 - fs]
    other = 1 - tp

    def to(ref_src, ref_dst, send, recv, axis, index):
        return pltpu.make_async_remote_copy(
            src_ref=ref_src,
            dst_ref=ref_dst,
            send_sem=send,
            recv_sem=recv,
            device_id={axis: index},
            device_id_type=pl.DeviceIdType.MESH,
        )

    own_rows = pl.ds(pl.multiple_of(me * depth, depth), depth)
    loads = [pltpu.make_async_copy(tokens, tbuf, loc_sem.at[0])]
    col = 0
    weight_loads = []
    for index, matrix in enumerate(
        (w_value, w_keys, w_query, w_gate, w_wkeys, w_wvalues, w_wquery)
    ):
        size = matrix.shape[1] // 4
        weight_loads.append(
            pltpu.make_async_copy(
                matrix.at[:, pl.ds(pl.multiple_of(fs * size, size), size)],
                wbuf.at[own_rows, pl.ds(col, size)],
                loc_sem.at[1 + index],
            )
        )
        col += size
    out_loads = []
    first_rows = w_sout.shape[0] // 4
    second_rows = w_wout.shape[0] // 4
    out_rows = first_rows + second_rows
    for part in range(4):
        out_loads.append(
            pltpu.make_async_copy(
                w_sout.at[pl.ds(part * first_rows, first_rows)],
                wob.at[me, part, pl.ds(0, first_rows)],
                loc_sem.at[8 + 2 * part],
            )
        )
        out_loads.append(
            pltpu.make_async_copy(
                w_wout.at[pl.ds(part * second_rows, second_rows)],
                wob.at[me, part, pl.ds(first_rows, second_rows)],
                loc_sem.at[9 + 2 * part],
            )
        )
    step_load = pltpu.make_async_copy(step_w, stepw, loc_sem.at[16])
    small = (
        (norm_gain_in, norm_gain),
        (jumps_in, jumps),
        (gain_in, gain),
        (tap_value_in, tap_value),
        (tap_keys_in, tap_keys),
        (tap_query_in, tap_query),
    )
    small_loads = [
        pltpu.make_async_copy(source, target, loc_sem.at[17 + count + index])
        for index, (source, target) in enumerate(small)
    ]

    barrier = pltpu.get_barrier_semaphore()
    for side in range(2):
        pl.when(has[side])(
            lambda side=side: pl.semaphore_signal(
                barrier,
                inc=1,
                device_id={"sp": beside[side]},
                device_id_type=pl.DeviceIdType.MESH,
            )
        )
    for k in range(1, 4):
        pl.semaphore_signal(
            barrier, inc=1, device_id={"fs": peers[k]}, device_id_type=pl.DeviceIdType.MESH
        )
    pl.semaphore_signal(
        barrier, inc=1, device_id={"tp": other}, device_id_type=pl.DeviceIdType.MESH
    )
    for load in weight_loads + loads + small_loads + [step_load]:
        load.start()
    pl.semaphore_wait(barrier, 4 + jnp.minimum(me, 1) + jnp.minimum(count - 1 - me, 1))

    spans = {
        0: (0, 4 * lanes),
        1: (4 * lanes, 2 * lanes),
        2: (6 * lanes, lanes),
        4: (7 * lanes, lanes),
    }
    pieces = 5

    def line(piece, hop, side):
        origin = me - hop if side == 1 else me + hop
        origin = jnp.clip(origin, 0, count - 1)
        if piece == 3:
            ref = wob.at[origin, fs]
        else:
            start, size = spans[piece]
            ref = wbuf.at[pl.ds(pl.multiple_of(origin * depth, depth), depth), pl.ds(start, size)]
        slot = (side * pieces + piece) * (count - 1) + hop
        return to(ref, ref, z_send.at[slot], z_recv.at[slot], "sp", beside[side])

    def valid(hop, side):
        return me >= hop if side == 1 else me + hop <= count - 1

    def send_line(piece, hop, where=True):
        for side in range(2):
            pl.when(has[side] & valid(hop, side) & where)(
                lambda side=side: line(piece, hop, side).start()
            )

    def take_line(piece, hop, then=None, mode=None, hold=False):
        for side in range(2):
            wanted = valid(hop, side)
            if mode == "pass":
                wanted = wanted & has[side]
            elif mode == "pass_end":
                wanted = wanted & has[side] & jnp.logical_not(valid(hop + 1, side))
            elif mode == "pass_rest":
                wanted = wanted & has[side] & valid(hop + 1, side)
            elif mode == "keep":
                wanted = wanted & jnp.logical_not(has[side])

            def arrive(side=side):
                line_in(piece, hop, side).wait_recv()
                if hop < count - 1 and not hold:
                    pl.when(has[side])(lambda: line(piece, hop, side).start())
                if then is not None:
                    then(hop, side)

            pl.when(wanted)(arrive)

    def line_in(piece, hop, side):
        origin = me - hop if side == 1 else me + hop
        origin = jnp.clip(origin, 0, count - 1)
        if piece == 3:
            ref = wob.at[origin, fs]
        else:
            start, size = spans[piece]
            ref = wbuf.at[pl.ds(pl.multiple_of(origin * depth, depth), depth), pl.ds(start, size)]
        slot = (side * pieces + piece) * (count - 1) + hop - 1
        return to(ref, ref, z_send.at[slot], z_recv.at[slot], "sp", beside[side])

    for load in weight_loads:
        load.wait()
    send_line(0, 0)
    send_line(1, 0)

    for load in loads + small_loads:
        load.wait()
    norm_rows = 32

    def norm(index, base):
        at = pl.ds(pl.multiple_of(base + index * norm_rows, norm_rows), norm_rows)
        wide = tbuf[at, :].astype(f32)
        scale = lax.rsqrt(jnp.mean(wide * wide, axis=-1, keepdims=True) + 1e-06)
        xbuf[fs, at, :] = (wide * scale * norm_gain[...]).astype(bf16)
        return base

    lax.fori_loop(0, half // norm_rows, norm, tp * half)
    lax.fori_loop(0, half // norm_rows, norm, other * half)
    own_half = pl.ds(pl.multiple_of(tp * half, half), half)
    x_own = [
        to(
            xbuf.at[fs, own_half],
            xbuf.at[fs, own_half],
            x_send.at[k - 1],
            x_recv.at[k - 1],
            "fs",
            peers[k],
        )
        for k in (1, 2)
    ]
    for copy in x_own:
        copy.start()
    j_own = [
        to(jumps, jbuf.at[fs], j_send.at[k], j_recv.at[k], "fs", peers[k]) for k in range(1, 4)
    ]
    for copy in j_own:
        copy.start()
    for load in out_loads:
        load.start()
    jbuf[fs, :, :] = jumps[...]

    lane = lax.broadcasted_iota(jnp.int32, (1, lanes), 1)
    low = lane < lanes // 2
    q4 = HEAD_DIM // 4

    def table(index, carry):
        at = pl.ds(pl.multiple_of(index * BLOCK, BLOCK), BLOCK)
        spot = lax.broadcasted_iota(jnp.int32, (BLOCK, lanes), 0) + me * rows + index * BLOCK
        place = jnp.where(low, spot // GRID_WIDTH, spot % GRID_WIDTH).astype(f32)
        inverse = jnp.exp((lane % q4).astype(f32) * (-math.log(10000.0) / q4))
        angle = place * inverse
        cos_t[at, :] = jnp.cos(angle)
        sin_t[at, :] = jnp.where(lane % (2 * q4) < q4, -1.0, 1.0) * jnp.sin(angle)
        return carry

    lax.fori_loop(0, blocks, table, 0)

    def window_bias(index, carry):
        q_id = lax.broadcasted_iota(jnp.int32, (2 * WINDOW, 3 * WINDOW), 0)
        b_id = lax.broadcasted_iota(jnp.int32, (2 * WINDOW, 3 * WINDOW), 1)
        blk = jnp.where(index == 2, blocks - 1, index)
        place = me * rows + (blk - 1) * WINDOW + b_id
        ok = jnp.abs(b_id - WINDOW - q_id % WINDOW) <= WINDOW
        ok = ok & (place >= 0) & (place < count * rows)
        bias[index, :, :] = jnp.where(ok, 0.0, -1e30)
        return carry

    lax.fori_loop(0, 3, window_bias, 0)
    kvbuf[:, :, 2 * HEAD_DIM :] = jnp.ones((4, rows + 2 * WINDOW, HEAD_DIM), bf16)
    heads_all = step_w.shape[0]
    first_head = (tp * 4 + fs) * 2
    pick = (
        lax.broadcasted_iota(jnp.int32, (lanes, heads_all), 1)
        == first_head + lax.broadcasted_iota(jnp.int32, (lanes, heads_all), 0) // (lanes // 2)
    )
    step_load.wait()
    stepx[...] = jnp.dot(
        pick.astype(f32).astype(bf16), stepw[...], preferred_element_type=f32
    ).astype(bf16)

    take_line(0, 1)
    for load in out_loads:
        load.wait()
    send_line(3, 0)

    x_first = pl.ds(pl.multiple_of(tp * half, quarter), quarter)
    x_second = pl.ds(pl.multiple_of(tp * half + quarter, quarter), quarter)

    def x_in(k, at, slot):
        return to(xbuf.at[peers[k], at], xbuf.at[peers[k], at], x_send.at[slot], x_recv.at[slot], "fs", peers[k])

    relay = [
        to(xbuf.at[peers[1], x_first], xbuf.at[peers[1], x_first], x_send.at[2], x_recv.at[2], "fs", peers[2]),
        to(xbuf.at[peers[2], x_second], xbuf.at[peers[2], x_second], x_send.at[3], x_recv.at[3], "fs", peers[1]),
    ]
    across = [
        to(xbuf.at[peers[k], own_half], xbuf.at[peers[k], own_half], d_send.at[k - 1], d_recv.at[k - 1], "tp", other)
        for k in range(1, 4)
    ]
    for k in (1, 2):
        x_in(k, own_half, k - 1).wait_recv()
        relay[k - 1].start()
        across[k - 1].start()
    if count > 2:
        take_line(0, 2)
    inner = has[0] & has[1]

    out_half = out_rows // 2

    def plane(origin, k, at, slot, target):
        ref = wob.at[origin, peers[k]] if at is None else wob.at[origin, peers[k], at]
        slot = origin * 4 + slot
        return to(ref, ref, o_send.at[slot], o_recv.at[slot], "fs", peers[target])

    halves = (pl.ds(0, out_half), pl.ds(out_half, out_half))

    def spread(hop, side):
        origin = jnp.clip(me - hop if side == 1 else me + hop, 0, count - 1)
        plane(origin, 0, None, 1, 1).start()
        plane(origin, 0, None, 2, 2).start()

    def relay_out(hop, where=True):
        for side in range(2):

            def work(side=side):
                origin = jnp.clip(me - hop if side == 1 else me + hop, 0, count - 1)
                plane(origin, 1, None, 1, 1).wait_recv()
                plane(origin, 1, halves[0], 3, 2).start()
                plane(origin, 2, None, 2, 2).wait_recv()
                plane(origin, 2, halves[1], 0, 1).start()

            pl.when(valid(hop, side) & where)(work)

    at_top = jnp.where(me == count - 1, 1, 0)
    most = (count - 1) * depth
    most_at = pl.ds(pl.multiple_of(at_top * depth, depth), most)
    last_at = pl.ds(pl.multiple_of((1 - at_top) * most, depth), depth)
    other_half = pl.ds(pl.multiple_of(other * half, half), half)

    def sequence(step):
        return jnp.where(
            step == 0,
            peers[0],
            jnp.where(step == 1, peers[1], jnp.where(step == 2, peers[2], peers[3])),
        )

    def project_most(index, start):
        seq, at = sequence(index // 2), pl.ds(pl.multiple_of((index % 2) * half, half), half)
        acc[seq, at, :] = jnp.dot(
            xbuf[seq, at, most_at], wbuf[most_at, : 4 * lanes], preferred_element_type=f32
        )
        z = lax.dot_general(
            xbuf[seq, at, :], stepx[...], (((1,), (1,)), ((), ())), preferred_element_type=f32
        )
        stbuf[seq, at, :] = jnp.maximum(z, 0.0) + jnp.log1p(jnp.exp(-jnp.abs(z)))
        return start

    def half_in(k):
        ref = xbuf.at[peers[k], other_half]
        to(ref, ref, d_send.at[k - 1], d_recv.at[k - 1], "tp", other).wait_recv()

    half_in(1)
    half_in(2)
    lax.fori_loop(0, 6, project_most, 0)
    x_in(3, x_first, 2).wait_recv()
    x_in(3, x_second, 3).wait_recv()
    across[2].start()
    take_line(3, 1, spread, hold=True)
    half_in(3)
    lax.fori_loop(6, 8, project_most, 0)
    for hop in range(3, count):
        take_line(0, hop)

    def project_state(index, carry):
        seq, at = index // 2, pl.ds(pl.multiple_of((index % 2) * half, half), half)
        y = acc[seq, at, :] + jnp.dot(
            xbuf[seq, at, last_at], wbuf[last_at, : 4 * lanes], preferred_element_type=f32
        )
        to_at = pl.ds(pl.multiple_of((index % 2) * half + 8, 8), half)
        cbuf[seq, to_at, :] = y[:, : 3 * lanes].astype(bf16).astype(f32)
        gbuf[seq, at, :] = y[:, 3 * lanes :].astype(bf16)
        return carry

    lax.fori_loop(0, 8, project_state, 0)
    low_edge, high_edge = pl.ds(0, 8), pl.ds(rows + 8, 8)
    halo = [
        to(cbuf.at[:, pl.ds(8, 8)], cbuf.at[:, high_edge], h_send.at[0], h_recv.at[0], "sp", beside[0]),
        to(cbuf.at[:, pl.ds(rows, 8)], cbuf.at[:, low_edge], h_send.at[1], h_recv.at[1], "sp", beside[1]),
    ]
    halo_in = [
        to(cbuf.at[:, low_edge], cbuf.at[:, low_edge], h_send.at[1], h_recv.at[1], "sp", beside[0]),
        to(cbuf.at[:, high_edge], cbuf.at[:, high_edge], h_send.at[0], h_recv.at[0], "sp", beside[1]),
    ]
    for side in range(2):
        pl.when(has[side])(lambda side=side: halo[side].start())
    edges = (low_edge, high_edge)
    for side in range(2):

        def clear(side=side):
            cbuf[:, edges[side], :] = jnp.zeros((4, 8, 3 * lanes), f32)

        pl.when(jnp.logical_not(has[side]))(clear)
    if count > 2:
        send_line(3, 1)
    take_line(1, 1)
    send_line(2, 0, jnp.logical_not(inner))
    send_line(4, 0, jnp.logical_not(inner))
    for copy in j_own:
        copy.wait_send()
    for k in range(1, 4):
        to(jumps, jbuf.at[peers[k]], j_send.at[k], j_recv.at[k], "fs", peers[k]).wait_recv()
    for side in range(2):
        pl.when(has[side])(lambda side=side: halo_in[side].wait_recv())

    own_cols = pl.ds(pl.multiple_of(fs * lanes, lanes), lanes)
    taps = jnp.concatenate(
        [ref[:, own_cols].astype(f32) for ref in (tap_value, tap_keys, tap_query)], axis=1
    )
    rate_lane = jnp.where(low, rate[2 * fs], rate[2 * fs + 1])
    row_id = lax.broadcasted_iota(jnp.int32, (BLOCK, lanes), 0)
    col_id = lax.broadcasted_iota(jnp.int32, (BLOCK, lanes), 1)
    lower = (col_id <= row_id).astype(f32)
    left = col_id < lanes // 2
    tap_count = taps.shape[0]
    reach = tap_count // 2
    tall = BLOCK + 16
    high = lax.Precision.HIGHEST

    def scan_block(index):
        seq, blk = index // blocks, index % blocks
        at = pl.ds(pl.multiple_of(blk * BLOCK, BLOCK), BLOCK)
        pre = cbuf[seq, pl.ds(pl.multiple_of(blk * BLOCK, BLOCK), tall), :]
        filt = jnp.zeros((BLOCK, 3 * lanes), f32)
        for tap in range(tap_count):
            moved = pre if tap == reach else pltpu.roll(pre, (reach - tap) % tall, 0)
            filt = filt + moved[8 : 8 + BLOCK] * taps[tap : tap + 1, :]
        fv, fk, fq = filt[:, :lanes], filt[:, lanes : 2 * lanes], filt[:, 2 * lanes :]
        step = stbuf[seq, at, :]
        sv = (fv * jax.nn.sigmoid(fv) * step).astype(bf16)
        sk, sq = fk.astype(bf16), fq.astype(bf16)
        jrows = jbuf[seq, :, at]
        jrow_id = lax.broadcasted_iota(jnp.int32, jrows.shape, 0)
        jrow = [
            jnp.sum(jnp.where(jrow_id == 2 * fs + r, jrows, 0.0), axis=0, keepdims=True)
            for r in range(2)
        ]
        jump = jnp.where(row_id < lanes // 2, jrow[0], jrow[1]).T
        logs = jump - rate_lane * step
        cum = jnp.dot(lower, logs, preferred_element_type=f32, precision=high)
        cum_t = cum.T
        gram = lax.dot_general(sq, sk, (((1,), (1,)), ((), ())), preferred_element_type=f32)
        key_t = sk.astype(f32).T
        near, after, before = [], [], []
        for r in range(2):
            spot = r * (lanes // 2)
            down = cum[:, spot : spot + 1]
            across_row = cum_t[spot : spot + 1, :]
            pair = (gram * jnp.exp(-jnp.abs(down - across_row))).astype(bf16)
            near.append(jnp.dot(pair, sv, preferred_element_type=f32))
            last = across_row[:, BLOCK - 1 : BLOCK]
            k_after = (key_t * jnp.exp(last - across_row)).astype(bf16)
            after.append(jnp.dot(k_after, sv, preferred_element_type=f32))
            k_before = (key_t * jnp.exp(across_row)).astype(bf16)
            before.append(jnp.dot(k_before, sv, preferred_element_type=f32))

        def store():
            sqbuf[seq, at, :] = sq
            cumbuf[seq, at, :] = cum
            nbuf[seq, at, :] = jnp.where(left, near[0], near[1])
            sabuf[index, :, :] = jnp.where(left, after[0], after[1])
            sbbuf[index, :, :] = jnp.where(left, before[0], before[1])

        return store

    def pairs_of(block):
        def body(index, carry):
            for store in [block(2 * index + k) for k in range(2)]:
                store()
            return carry

        return body

    relay_out(1, jnp.logical_not(inner))
    lax.fori_loop(0, blocks, pairs_of(scan_block), 0)
    for hop in range(2, count - 1):
        take_line(1, hop, mode="pass")
    relay_out(1, inner)
    for hop in range(2, count - 1):
        take_line(3, hop, spread)
    lax.fori_loop(blocks, 2 * blocks, pairs_of(scan_block), 0)

    if count > 2:
        take_line(2, 1, mode="pass_end")
        take_line(4, 1, mode="pass_end")

    zero_state = jnp.zeros((STATE_SIZE, lanes), f32)

    def total_of(seq, blk):
        return cumbuf[seq, blk * BLOCK + BLOCK - 8 : blk * BLOCK + BLOCK, :][7:8, :]

    def carry_states(seq, carry):
        state, so_far = zero_state, jnp.zeros((1, lanes), f32)
        for blk in range(blocks):
            added = sabuf[seq * blocks + blk, :, :]
            sabuf[seq * blocks + blk, :, :] = state
            edge[seq * blocks + blk, 0:1, :] = so_far
            total = total_of(seq, blk)
            state = state * jnp.exp(total) + added
            so_far = so_far + total
        fout[seq, :, :] = state.astype(bf16)
        edge[4 * blocks + seq, 0:1, :] = so_far
        state, so_far = zero_state, jnp.zeros((1, lanes), f32)
        for blk in range(blocks - 1, -1, -1):
            added = sbbuf[seq * blocks + blk, :, :]
            sbbuf[seq * blocks + blk, :, :] = state
            edge[seq * blocks + blk, 1:2, :] = so_far
            total = total_of(seq, blk)
            state = state * jnp.exp(total) + added
            so_far = so_far + total
        gout[seq, :, :] = state.astype(bf16)
        return carry

    lax.fori_loop(0, 4, carry_states, 0)
    chain = [
        to(gout, gin, h_send.at[2], h_recv.at[2], "sp", beside[0]),
        to(fout, fin, h_send.at[3], h_recv.at[3], "sp", beside[1]),
    ]

    def clear_forward():
        fin[...] = jnp.zeros(fin.shape, bf16)

    def clear_backward():
        gin[...] = jnp.zeros(gin.shape, bf16)

    pl.when(me == 0)(clear_forward)
    pl.when(me == count - 1)(clear_backward)
    pl.when(me == 0)(lambda: chain[1].start())
    pl.when(me == count - 1)(lambda: chain[0].start())

    def rotated(vectors):
        lane_full = lax.broadcasted_iota(jnp.int32, vectors.shape, 1)
        turned = jnp.where(
            lane_full % (2 * q4) < q4,
            pltpu.roll(vectors, HEAD_DIM - q4, 1),
            pltpu.roll(vectors, q4, 1),
        )
        return (vectors * cos_t[...] + turned * sin_t[...]).astype(bf16)

    for hop in range(2, count):
        take_line(1, hop, mode="keep")

    def project_pair(seq, carry):
        y = jnp.dot(
            xbuf[seq, :, :], wbuf[:, 4 * lanes : 6 * lanes], preferred_element_type=f32
        ).astype(bf16)
        kvbuf[seq, WINDOW : WINDOW + rows, :HEAD_DIM] = rotated(y[:, :HEAD_DIM].astype(f32))
        kvbuf[seq, WINDOW : WINDOW + rows, HEAD_DIM : 2 * HEAD_DIM] = y[:, HEAD_DIM:]
        return carry

    lax.fori_loop(0, 4, project_pair, 0)
    bottom, top = pl.ds(0, WINDOW), pl.ds(rows + WINDOW, WINDOW)
    pair_cols = pl.ds(0, 2 * HEAD_DIM)

    def kv(at):
        return kvbuf.at[:, at, pair_cols]

    low_rows, high_rows = pl.ds(WINDOW, WINDOW), pl.ds(rows, WINDOW)
    kv_edge = [
        to(kv(low_rows), kv(top), h_send.at[4], h_recv.at[4], "sp", beside[0]),
        to(kv(high_rows), kv(bottom), h_send.at[5], h_recv.at[5], "sp", beside[1]),
    ]
    kv_in = [
        to(kv(bottom), kv(bottom), h_send.at[5], h_recv.at[5], "sp", beside[0]),
        to(kv(top), kv(top), h_send.at[4], h_recv.at[4], "sp", beside[1]),
    ]
    bands = (bottom, top)
    for side in range(2):

        def clear_band(side=side):
            kvbuf[:, bands[side], : 2 * HEAD_DIM] = jnp.zeros((4, WINDOW, 2 * HEAD_DIM), bf16)

        pl.when(jnp.logical_not(has[side]))(clear_band)

    def forward_step():
        to(fin, fin, h_send.at[3], h_recv.at[3], "sp", beside[0]).wait_recv()

        def add(seq, carry):
            passed = jnp.exp(edge[4 * blocks + seq, 0:1, :])
            fout[seq, :, :] = (
                fout[seq, :, :].astype(f32) + passed * fin[seq, :, :].astype(f32)
            ).astype(bf16)
            return carry

        def pass_on():
            lax.fori_loop(0, 4, add, 0)
            chain[1].start()

        pl.when(has[1])(pass_on)

    def backward_step():
        to(gin, gin, h_send.at[2], h_recv.at[2], "sp", beside[1]).wait_recv()

        def add(seq, carry):
            passed = jnp.exp(edge[4 * blocks + seq, 0:1, :])
            gout[seq, :, :] = (
                gout[seq, :, :].astype(f32) + passed * gin[seq, :, :].astype(f32)
            ).astype(bf16)
            return carry

        def pass_on():
            lax.fori_loop(0, 4, add, 0)
            chain[0].start()

        pl.when(has[0])(pass_on)

    near_first = 2 * me < count
    pl.when(inner & near_first)(forward_step)
    pl.when(inner)(backward_step)
    pl.when(inner & jnp.logical_not(near_first))(forward_step)
    send_line(2, 0, inner)
    if count > 2:
        take_line(2, 1, mode="pass_rest")
    send_line(4, 0, inner)
    for hop in range(2, count - 1):
        take_line(2, hop, mode="pass")
    if count > 2:
        take_line(4, 1, mode="pass_rest")
    for hop in range(2, count - 1):
        take_line(4, hop, mode="pass")
    for side in range(2):
        pl.when(has[side])(lambda side=side: kv_edge[side].start())
    for hop in range(2, count - 1):
        relay_out(hop)
    if count > 2:
        take_line(3, count - 1, spread)

    inner_rows = pl.ds(BLOCK, rows - 2 * BLOCK)

    def edge_block(second):
        return jnp.where(at_top == 1 - second, blocks - 1, 0)

    def edge_rows(second):
        return pl.ds(pl.multiple_of(edge_block(second) * BLOCK, BLOCK), BLOCK)

    parts = (
        (pl.ds(0, rows), pl.ds(0, lanes)),
        (inner_rows, pl.ds(lanes, HEAD_DIM)),
        (inner_rows, pl.ds(lanes + HEAD_DIM, HEAD_DIM)),
        (edge_rows(0), pl.ds(lanes, 2 * HEAD_DIM)),
        (edge_rows(1), pl.ds(lanes, 2 * HEAD_DIM)),
    )

    def swap(k, part):
        slot = part * 4 + k
        return to(
            mixs.at[(peers[k], *parts[part])],
            mixr.at[(fs, *parts[part])],
            m_send.at[slot],
            m_recv.at[slot],
            "fs",
            peers[k],
        )

    def swap_in(k, part):
        ref, slot = mixr.at[(peers[k], *parts[part])], part * 4 + k
        return to(ref, ref, m_send.at[slot], m_recv.at[slot], "fs", peers[k])

    pl.when(has[0] & jnp.logical_not(has[1]))(forward_step)
    pl.when(has[1] & jnp.logical_not(has[0]))(backward_step)
    gain_row = gain[:, own_cols]

    def split_dot(a, b):
        top_bits = b.astype(bf16)
        rest = (b - top_bits.astype(f32)).astype(bf16)
        return jnp.dot(a, top_bits, preferred_element_type=f32) + jnp.dot(
            a, rest, preferred_element_type=f32
        )

    def finish_block(index):
        seq, blk = index // blocks, index % blocks
        at = pl.ds(pl.multiple_of(blk * BLOCK, BLOCK), BLOCK)
        ahead = sabuf[index, :, :] + jnp.exp(edge[index, 0:1, :]) * fin[seq, :, :].astype(f32)
        behind = sbbuf[index, :, :] + jnp.exp(edge[index, 1:2, :]) * gin[seq, :, :].astype(f32)
        sq = sqbuf[seq, at, :]
        cum = cumbuf[seq, at, :]
        total = cum[BLOCK - 1 : BLOCK, :]
        mixed = (
            nbuf[seq, at, :]
            + jnp.exp(cum) * split_dot(sq, ahead)
            + jnp.exp(total - cum) * split_dot(sq, behind)
        )
        g = gbuf[seq, at, :].astype(f32)
        gated = mixed * (g * jax.nn.sigmoid(g))
        square = gated * gated
        first = jnp.sum(jnp.where(left, square, 0.0), axis=-1, keepdims=True)
        second = jnp.sum(jnp.where(left, 0.0, square), axis=-1, keepdims=True)
        mean = jnp.where(left, first, second) * (2.0 / lanes)
        mix = (gated * lax.rsqrt(mean + 1e-06) * gain_row).astype(bf16)

        def store():
            mixs[seq, at, :lanes] = mix

        return store

    lax.fori_loop(0, 2 * blocks, pairs_of(finish_block), 0)
    for k in (3, 1, 2):
        swap(k, 0).start()


    def query_cols(r):
        return slice((6 + r) * lanes, (7 + r) * lanes)

    def head_cols(r):
        return slice(r * HEAD_DIM, (r + 1) * HEAD_DIM)

    near_count = max(1, count // 2)
    near_at = pl.ds(
        pl.multiple_of(at_top * (count - near_count) * depth, depth), near_count * depth
    )
    far_at = pl.ds(
        pl.multiple_of((1 - at_top) * near_count * depth, depth), (count - near_count) * depth
    )
    query_parts = ((most_at, last_at), (near_at, far_at))

    def query_first(r):
        at = query_parts[r][0]

        def body(seq, carry):
            acc[seq, :, head_cols(r)] = jnp.dot(
                xbuf[seq, :, at], wbuf[at, query_cols(r)], preferred_element_type=f32
            )
            return carry

        lax.fori_loop(0, 4, body, 0)

    def query_rest(r):
        at = query_parts[r][1]

        def body(seq, carry):
            y = acc[seq, :, head_cols(r)] + jnp.dot(
                xbuf[seq, :, at], wbuf[at, query_cols(r)], preferred_element_type=f32
            )
            qbuf[seq, :, head_cols(r)] = rotated(y.astype(bf16).astype(f32))
            return carry

        lax.fori_loop(0, 4, body, 0, unroll=2)

    for hop in range(1, count - 1):
        take_line(2, hop, mode="keep")
    query_first(0)
    if count > 2:
        relay_out(count - 1, tp == 1)
    take_line(2, count - 1, mode="keep")
    query_rest(0)
    band = 3 * WINDOW
    log2e = math.log2(math.e)
    def sink_rows(heads):
        row = lax.broadcasted_iota(jnp.int32, (len(heads) * WINDOW, 1), 0)
        first = sink[2 * fs + heads[0]]
        return log2e * jnp.where(row < WINDOW, first, sink[2 * fs + heads[-1]])

    floors = {heads: sink_rows(heads) for heads in ((0,), (1,), (0, 1))}

    def attend_block(seq, blk, heads):
        at = pl.ds(pl.multiple_of(blk * WINDOW, WINDOW), WINDOW)
        wide = pl.ds(pl.multiple_of(blk * WINDOW, WINDOW), band)
        q = jnp.concatenate([qbuf[seq, at, head_cols(r)] for r in heads], axis=0)
        s = lax.dot_general(
            q,
            kvbuf[seq, wide, :HEAD_DIM],
            (((1,), (1,)), ((), ())),
            preferred_element_type=f32,
        )
        kind = jnp.where(blk == 0, 0, jnp.where(blk == blocks - 1, 2, 1))
        floor = floors[heads]
        s = s * (HEAD_DIM ** (-0.5) * log2e) + bias[kind, : len(heads) * WINDOW, :]
        m = jnp.maximum(jnp.max(s, axis=-1, keepdims=True), floor)
        w = jnp.exp2(s - m).astype(bf16)
        y = jnp.dot(w, kvbuf[seq, wide, HEAD_DIM:], preferred_element_type=f32)
        total = jnp.exp2(floor - m) + y[:, HEAD_DIM:]
        o = (y[:, :HEAD_DIM] / total).astype(bf16)

        def store():
            for index, r in enumerate(heads):
                mixs[seq, at, lanes + r * HEAD_DIM : lanes + (r + 1) * HEAD_DIM] = o[
                    index * WINDOW : (index + 1) * WINDOW
                ]

        return store

    def far_first(step):
        return jnp.where(
            step == 0,
            peers[3],
            jnp.where(step == 1, peers[1], jnp.where(step == 2, peers[2], peers[0])),
        )

    def attend_inner(r):
        def each(step, carry):
            seq = far_first(step)

            def body(index, carry):
                for store in [attend_block(seq, 1 + 2 * index + k, (r,)) for k in range(2)]:
                    store()
                return carry

            lax.fori_loop(0, blocks // 2 - 1, body, 0)
            for index, k in enumerate((3, 1, 2)):
                pl.when(step == index)(lambda k=k: swap(k, 1 + r).start())
            return carry

        lax.fori_loop(0, 4, each, 0)

    attend_inner(0)
    if count > 2:
        relay_out(count - 1, tp == 0)
    for hop in range(1, near_count):
        take_line(4, hop, mode="keep")
    query_first(1)
    for hop in range(near_count, count):
        take_line(4, hop, mode="keep")
    query_rest(1)
    attend_inner(1)
    def edges_in(where):
        for side in range(2):
            pl.when(has[side] & where)(lambda side=side: kv_in[side].wait_recv())

    def attend_edges(second):
        def body(index, carry):
            steps = [2 * index + k for k in range(2)]
            seqs = [far_first(step) for step in steps]
            for store in [attend_block(seq, edge_block(second), (0, 1)) for seq in seqs]:
                store()
            for step, k in enumerate((3, 1, 2)):
                pl.when(index == step // 2)(lambda k=k: swap(k, 3 + second).start())
            return carry

        lax.fori_loop(0, 2, body, 0)

    edges_in(inner)
    attend_edges(0)
    edges_in(jnp.logical_not(inner))
    attend_edges(1)

    cols = w_sout.shape[1]

    def out_in(origin):
        def work():
            plane(origin, 3, halves[0], 3, 2).wait_recv()
            plane(origin, 3, halves[1], 0, 1).wait_recv()

        pl.when(origin != me)(work)

    def columns(origin):
        return pl.ds(pl.multiple_of(origin * cols, cols), cols)

    def trade(origin):
        return to(
            psend.at[origin],
            out_other.at[:, columns(origin)],
            p_send.at[origin],
            p_recv.at[origin],
            "tp",
            other,
        )

    def store_own(origin):
        return pltpu.make_async_copy(
            pown.at[origin], out_own.at[:, columns(origin)], loc_sem.at[17 + origin]
        )

    def hand_over(origin, totals):
        psend[origin, :, :] = totals[0].astype(bf16)
        trade(origin).start()
        pown[origin, :, :] = totals[1].astype(bf16)
        store_own(origin).start()

    row_halves = (other_half, own_half)

    def first_product(origin, carry):
        out_in(origin)
        weights = jnp.concatenate(
            [wob[origin, fs, :, :]] + [wob[origin, peers[k], :lanes, :] for k in range(1, 4)], axis=0
        )
        for at in row_halves:
            mix = jnp.concatenate(
                [mixs[fs, at, :]] + [mixr[peers[k], at, :lanes] for k in range(1, 4)], axis=1
            )
            oacc[origin, at, :] = jnp.dot(mix, weights, preferred_element_type=f32)
        return carry

    def add_parts(ks, last):
        def body(origin, carry):
            weights = jnp.concatenate([wob[origin, peers[k], lanes:, :] for k in ks], axis=0)
            totals = [
                oacc[origin, at, :]
                + jnp.dot(
                    jnp.concatenate([mixr[peers[k], at, lanes:] for k in ks], axis=1),
                    weights,
                    preferred_element_type=f32,
                )
                for at in row_halves
            ]
            if last:
                hand_over(origin, totals)
            else:
                for total, at in zip(totals, row_halves):
                    oacc[origin, at, :] = total
            return carry

        lax.fori_loop(0, count, body, 0, unroll=2)

    for k in (3, 1, 2):
        swap_in(k, 0).wait_recv()
    lax.fori_loop(0, count, first_product, 0, unroll=2)
    for ks in ((3,), (1, 2)):
        for k in ks:
            for part in range(1, 5):
                swap_in(k, part).wait_recv()
        add_parts(ks, 2 in ks)

    for origin in range(count):
        trade(origin).wait_recv()
        store_own(origin).wait()

    for piece in range(pieces):
        for hop in range(count - 1):
            for side in range(2):
                pl.when(has[side] & valid(hop, side))(
                    lambda piece=piece, hop=hop, side=side: line(piece, hop, side).wait_send()
                )
    for copy in x_own + relay + across:
        copy.wait_send()
    for side in range(2):
        pl.when(has[side])(lambda side=side: halo[side].wait_send())
        pl.when(has[side])(lambda side=side: chain[side].wait_send())
        pl.when(has[side])(lambda side=side: kv_edge[side].wait_send())
    for k in range(1, 4):
        for part in range(5):
            swap(k, part).wait_send()

    def left_plane(origin, carry):
        def work():
            plane(origin, 0, None, 1, 1).wait_send()
            plane(origin, 0, None, 2, 2).wait_send()
            plane(origin, 1, halves[0], 3, 2).wait_send()
            plane(origin, 2, halves[1], 0, 1).wait_send()

        pl.when(origin != me)(work)
        return carry

    lax.fori_loop(0, count, left_plane, 0)
    for origin in range(count):
        trade(origin).wait_send()


def fused_shards(
    tokens,
    norm_gain,
    state_gate,
    state_value,
    state_keys,
    state_query,
    state_step,
    state_rate,
    state_jumps,
    state_gain,
    filter_value,
    filter_keys,
    filter_query,
    window_query,
    window_keys,
    window_values,
    window_sink,
    state_output,
    window_output,
):
    count = lax.axis_size("sp")
    rows, width = tokens.shape
    lanes = STATE_SIZE
    blocks = rows // BLOCK
    depth = state_value.shape[0]
    cols = state_output.shape[1]
    out_rows = (state_output.shape[0] + window_output.shape[0]) // 4
    f32, bf16 = jnp.float32, jnp.bfloat16
    vmem = pltpu.VMEM
    dma = pltpu.SemaphoreType.DMA
    hbm = pl.BlockSpec(memory_space=pl.ANY)
    scalar = pl.BlockSpec(memory_space=pltpu.SMEM)
    jumps = state_jumps.T
    half = rows // 2
    own, others = pl.pallas_call(
        functools.partial(fused_kernel, count),
        out_shape=[jax.ShapeDtypeStruct((half, width), bf16)] * 2,
        in_specs=[hbm] * 10
        + [hbm, hbm, scalar, hbm, hbm, hbm, hbm, hbm, scalar],
        out_specs=[hbm, hbm],
        scratch_shapes=[
            vmem((1, width), f32),
            vmem(jumps.shape, f32),
            vmem((1,) + state_gain.shape, f32),
            vmem(filter_value.shape, bf16),
            vmem(filter_keys.shape, bf16),
            vmem(filter_query.shape, bf16),
            vmem((rows, width), bf16),
            vmem((4, rows, width), bf16),
            vmem((count * depth, 8 * lanes), bf16),
            vmem((count, 4, out_rows, cols), bf16),
            vmem(state_step.shape[::-1], bf16),
            vmem((lanes, width), bf16),
            vmem((rows, lanes), f32),
            vmem((rows, lanes), f32),
            vmem((4,) + jumps.shape, f32),
            vmem((3, 2 * WINDOW, 3 * WINDOW), f32),
            vmem((4, rows, 4 * lanes), f32),
            vmem((count, rows, cols), f32),
            vmem((4, rows + 16, 3 * lanes), f32),
            vmem((4, rows, lanes), bf16),
            vmem((4, rows, lanes), f32),
            vmem((4, rows, lanes), f32),
            vmem((4 * blocks, STATE_SIZE, lanes), f32),
            vmem((4 * blocks, STATE_SIZE, lanes), f32),
            vmem((4, rows, lanes), f32),
            vmem((4 * blocks + 4, 8, lanes), f32),
            vmem((4, rows, lanes), bf16),
            vmem((4, STATE_SIZE, lanes), bf16),
            vmem((4, STATE_SIZE, lanes), bf16),
            vmem((4, STATE_SIZE, lanes), bf16),
            vmem((4, STATE_SIZE, lanes), bf16),
            vmem((4, rows + 2 * WINDOW, 3 * HEAD_DIM), bf16),
            vmem((4, rows, 2 * HEAD_DIM), bf16),
            vmem((4, rows, 3 * lanes), bf16),
            vmem((4, rows, 3 * lanes), bf16),
            vmem((count, half, cols), bf16),
            vmem((count, half, cols), bf16),
            dma((23 + count,)),
            dma((10 * (count - 1),)),
            dma((10 * (count - 1),)),
            dma((4,)),
            dma((4,)),
            dma((3,)),
            dma((3,)),
            dma((4,)),
            dma((4,)),
            dma((6,)),
            dma((6,)),
            dma((20,)),
            dma((20,)),
            dma((4 * count,)),
            dma((4 * count,)),
            dma((count,)),
            dma((count,)),
        ],
        compiler_params=pltpu.CompilerParams(
            collective_id=0, has_side_effects=True, vmem_limit_bytes=62 * 1024 * 1024
        ),
        name="fused_layer",
    )(
        tokens,
        state_value,
        state_keys,
        state_query,
        state_gate,
        window_keys,
        window_values,
        window_query,
        state_output,
        window_output,
        norm_gain.reshape(1, -1),
        state_step.T,
        state_rate,
        jumps,
        state_gain.reshape(1, -1),
        filter_value,
        filter_keys,
        filter_query,
        window_sink,
    )
    return (own.astype(f32) + others.astype(f32)).astype(bf16)


def solution(mesh):
    placed = (
        P(("fs", "sp"), None),
        P(),
        P("sp", "tp"),
        P("sp", "tp"),
        P("sp", "tp"),
        P("sp", "tp"),
        P(),
        P("tp"),
        P(("fs", "sp"), "tp"),
        P("tp"),
        P(None, "tp"),
        P(None, "tp"),
        P(None, "tp"),
        P("sp", "tp"),
        P("sp", "tp"),
        P("sp", "tp"),
        P("tp"),
        P("tp", "sp"),
        P("tp", "sp"),
    )
    def plan(*args):
        return (fused_shards if fits(*args) else shards)(*args)

    return jax.shard_map(
        plan, mesh=mesh, in_specs=placed, out_specs=P(("fs", "sp", "tp"), None), check_vma=False
    )
```
